128 devices in a mesh: sp: 32 (over z, y, core), tp: 4 (over x).
Axes of the slice: x: 4, y: 4, z: 4, core: 2. Of those that a mesh axis runs over, the one named last changes fastest.
Arguments:
- residual: bfloat16 [32768, 2048], P('sp'), may hold values from -6 to 6
- small_heads: bfloat16 [32768, 1024], P('sp', 'tp'), may hold values from -6 to 6
- large_heads: bfloat16 [32768, 1024], P('sp', 'tp'), may hold values from -6 to 6
- state_keys: bfloat16 [32768, 8, 128], P('sp', 'tp'), may hold values from -6 to 6
- state_queries: bfloat16 [32768, 8, 128], P('sp', 'tp'), may hold values from -6 to 6
- small_gate: bfloat16 [32768, 1024], P('sp', 'tp'), may hold values from -6 to 6
- large_gate: bfloat16 [32768, 1024], P('sp', 'tp'), may hold values from -6 to 6
- small_step: float32 [32768, 16], P('sp', 'tp'), may hold values from -3 to 2
- large_step: float32 [32768, 8], P('sp', 'tp'), may hold values from -3 to 2
- small_taps: bfloat16 [4, 1024], P(None, 'tp'), may hold values from -3 to 3
- large_taps: bfloat16 [4, 1024], P(None, 'tp'), may hold values from -3 to 3
- key_taps: bfloat16 [4, 8, 128], P(None, 'tp'), may hold values from -3 to 3
- query_taps: bfloat16 [4, 8, 128], P(None, 'tp'), may hold values from -3 to 3
- small_decay: float32 [16], P('tp'), may hold values from -12 to -2, as said below
- large_decay: float32 [8], P('tp'), may hold values from -12 to -2, as said below
- small_gain: bfloat16 [1024], P('tp'), may hold values from 0.099609375 to 1.8984375
- large_gain: bfloat16 [1024], P('tp'), may hold values from 0.099609375 to 1.8984375
- small_out: bfloat16 [1024, 2048], P('tp'), may hold values from -0.125 to 0.125
- large_out: bfloat16 [1024, 2048], P('tp'), may hold values from -0.125 to 0.125
- mixer_gain: bfloat16 [2048], replicated, may hold values from 0.099609375 to 1.8984375
- ffn_in_gain: bfloat16 [2048], replicated, may hold values from 0.099609375 to 1.8984375
- gate_proj: bfloat16 [2048, 5632], P('sp', 'tp'), may hold values from -0.125 to 0.125
- up_proj: bfloat16 [2048, 5632], P('sp', 'tp'), may hold values from -0.125 to 0.125
- down_proj: bfloat16 [2048, 5632], P('sp', 'tp'), may hold values from -0.078125 to 0.078125
- ffn_out_gain: bfloat16 [2048], replicated, may hold values from 0.099609375 to 1.8984375
Outputs:
- updated: bfloat16 [32768, 2048], P(('sp', 'tp'))
The draws below stay inside these ranges and needn't reach their ends.
Inputs may be any that keep to these rules, and one draw needn't show every extreme that they name: `small_decay`: log decay rates of the first group. `large_decay`: log decay rates of the second group.
All inputs are finite; a program needn't handle non-finite values.
Results may differ from the reference program's by a relative error of at most 0.014.
Values may be sent and summed in bfloat16 or wider, within the bound.
A program may use at most 192 MiB of HBM per device.

```python
import jax
import jax.numpy as jnp
from jax import lax

D = 2048
FF = 5632
HA = 16
PA = 64
HB = 8
PB = 128
GROUPS = 8
STATE = 128
CONV = 4
BLOCK = 128
TOK_DEV = 1024
TOKENS = 32768
HEAD_BLOCKS = 4


def step_law(key, heads, salt):
    rows = jnp.arange(TOKENS, dtype=jnp.int32) // TOK_DEV
    offset_key = jax.random.fold_in(key, 101)
    jitter_key = jax.random.fold_in(key, salt)
    offsets = jax.random.uniform(offset_key, (TOKENS // TOK_DEV,), jnp.float32, -1.5, 0.5)
    jitter = jnp.clip(0.5 * jax.random.normal(jitter_key, (TOKENS, heads), jnp.float32), -1.5, 1.5)
    return offsets[rows][:, None] + jitter


def decay_law(key, heads, salt):
    base_key = jax.random.fold_in(key, salt)
    order_key, slow_key, fast_key = jax.random.split(base_key, 3)
    fast_count = heads // 2
    ranks = jax.random.permutation(order_key, heads)
    slow_values = jnp.log(jax.random.uniform(slow_key, (heads,), jnp.float32, 0.25, 1.5) / TOKENS)
    fast_values = jnp.log(jax.random.uniform(fast_key, (heads,), jnp.float32, 1.0 / 60.0, 1.0 / 20.0))
    return jnp.where(ranks < fast_count, fast_values, slow_values)


def draw_small_step(key, part):
    return step_law(key, HA, 11)


def draw_large_step(key, part):
    return step_law(key, HB, 12)


def draw_small_decay(key, part):
    return decay_law(key, HA, 21)


def draw_large_decay(key, part):
    return decay_law(key, HB, 22)


def shard_levels(rng, shape, pieces, low, top_value):
    def one(position, parts):
        draws = jax.random.uniform(jax.random.fold_in(jax.random.fold_in(rng, 6), position), (parts,), jnp.float32, low / len(pieces), top_value / len(pieces))
        return jnp.repeat(jnp.exp(draws), shape[position] // parts).reshape((-1,) + (1,) * (len(shape) - position - 1))

    loudness = one(*pieces[0])
    for cut in pieces[1:]:
        loudness = loudness * one(*cut)
    return loudness


def scatter_about(rng, shape, width, bound, cuts=(), kind=jnp.bfloat16):
    level = shard_levels(rng, shape, cuts, -0.22, 0.18) if cuts else 1.0
    drawn = jax.random.normal(rng, shape, jnp.float32) * width * level
    return jnp.minimum(jnp.maximum(drawn, -bound), bound).astype(kind)


def setup_inputs(seed: int = 0) -> dict:
    arg_keys = jax.random.split(jax.random.key(seed), 26)
    return {
        "residual": scatter_about(arg_keys[0], (TOKENS, D), 1.0, 6.0, ((0, 32),)),
        "small_heads": scatter_about(arg_keys[1], (TOKENS, HA * PA), 1.0, 6.0, ((0, 32), (1, 4))),
        "large_heads": scatter_about(arg_keys[2], (TOKENS, HB * PB), 1.0, 6.0, ((0, 32), (1, 4))),
        "state_keys": scatter_about(arg_keys[3], (TOKENS, GROUPS, STATE), 1.0, 6.0, ((0, 32), (1, 4))),
        "state_queries": scatter_about(arg_keys[4], (TOKENS, GROUPS, STATE), 1.0, 6.0, ((0, 32), (1, 4))),
        "small_gate": scatter_about(arg_keys[5], (TOKENS, HA * PA), 1.0, 6.0, ((0, 32), (1, 4))),
        "large_gate": scatter_about(arg_keys[6], (TOKENS, HB * PB), 1.0, 6.0, ((0, 32), (1, 4))),
        "small_step": draw_small_step(jax.random.fold_in(arg_keys[25], 71), 0),
        "large_step": draw_large_step(jax.random.fold_in(arg_keys[25], 71), 0),
        "small_taps": scatter_about(arg_keys[9], (CONV, HA * PA), CONV ** -0.5, 3.0, ((1, 4),)),
        "large_taps": scatter_about(arg_keys[10], (CONV, HB * PB), CONV ** -0.5, 3.0, ((1, 4),)),
        "key_taps": scatter_about(arg_keys[11], (CONV, GROUPS, STATE), CONV ** -0.5, 3.0, ((1, 4),)),
        "query_taps": scatter_about(arg_keys[12], (CONV, GROUPS, STATE), CONV ** -0.5, 3.0, ((1, 4),)),
        "small_decay": draw_small_decay(jax.random.fold_in(arg_keys[25], 71), 0),
        "large_decay": draw_large_decay(jax.random.fold_in(arg_keys[25], 71), 0),
        "small_gain": jnp.clip(1.0 + 0.18 * jax.random.normal(arg_keys[15], (HA * PA,), jnp.float32), 0.099609375, 1.8984375).astype(jnp.bfloat16),
        "large_gain": jnp.clip(1.0 + 0.18 * jax.random.normal(arg_keys[16], (HB * PB,), jnp.float32), 0.099609375, 1.8984375).astype(jnp.bfloat16),
        "small_out": scatter_about(arg_keys[17], (HA * PA, D), (HA * PA + HB * PB) ** -0.5, 0.125, ((0, 4),)),
        "large_out": scatter_about(arg_keys[18], (HB * PB, D), (HA * PA + HB * PB) ** -0.5, 0.125, ((0, 4),)),
        "mixer_gain": jnp.clip(1.0 + 0.18 * jax.random.normal(arg_keys[19], (D,), jnp.float32), 0.099609375, 1.8984375).astype(jnp.bfloat16),
        "ffn_in_gain": jnp.clip(1.0 + 0.18 * jax.random.normal(arg_keys[20], (D,), jnp.float32), 0.099609375, 1.8984375).astype(jnp.bfloat16),
        "gate_proj": scatter_about(arg_keys[21], (D, FF), D ** -0.5, 0.125, ((0, 32), (1, 4))),
        "up_proj": scatter_about(arg_keys[22], (D, FF), D ** -0.5, 0.125, ((0, 32), (1, 4))),
        "down_proj": scatter_about(arg_keys[23], (D, FF), FF ** -0.5, 0.078125, ((0, 32), (1, 4))),
        "ffn_out_gain": jnp.clip(1.0 + 0.18 * jax.random.normal(arg_keys[24], (D,), jnp.float32), 0.099609375, 1.8984375).astype(jnp.bfloat16),
    }


EPS = 1e-06

def rounded(values):
    return lax.optimization_barrier(values.astype(jnp.bfloat16)).astype(jnp.float32)

def causal_taps(extended, tap_weights, length):
    kernel_len = tap_weights.shape[0]
    summed = jnp.zeros((length,) + extended.shape[1:], jnp.float32)
    for offset in range(kernel_len):
        window_rows = extended[offset:offset + length].astype(jnp.float32)
        summed = summed + tap_weights[offset].astype(jnp.float32) * window_rows
    return jax.nn.silu(summed).astype(jnp.bfloat16)

def block_pass(values, key_rows, queries, step_sizes, decay_rates):
    length, groups, head_count, head_dim = values.shape
    block_count = length // BLOCK
    state_len = key_rows.shape[-1]
    log_decay = -step_sizes * decay_rates
    causal = jnp.tril(jnp.ones((BLOCK, BLOCK), dtype=bool))
    highest = lax.Precision.HIGHEST

    def one_block(carry_state, block):
        block_values, block_keys, block_queries, block_steps, block_decay = block
        values_wide = block_values.astype(jnp.float32)
        keys_wide = block_keys.astype(jnp.float32)
        queries_wide = block_queries.astype(jnp.float32)
        cumulative = jnp.cumsum(block_decay, axis=0)
        scores = jnp.einsum('lgn,sgn->gls', queries_wide, keys_wide, precision=highest)
        cum_heads = jnp.transpose(cumulative, (1, 2, 0))
        gap_matrix = cum_heads[:, :, :, None] - cum_heads[:, :, None, :]
        decays = jnp.exp(jnp.where(causal, gap_matrix, -jnp.inf))
        step_heads = jnp.transpose(block_steps, (1, 2, 0))[:, :, None, :]
        weights = rounded(scores[:, None] * decays * step_heads)
        inside = jnp.einsum('ghls,sghp->lghp', weights, values_wide, precision=highest)
        carried = jnp.einsum('lgn,ghpn->lghp', queries_wide, carry_state, precision=highest)
        carried = carried * jnp.exp(cumulative)[..., None]
        tail_sum = cumulative[-1]
        scaled = rounded(values_wide * (block_steps * jnp.exp(tail_sum - cumulative))[..., None])
        fresh_state = jnp.einsum('lghp,lgn->ghpn', scaled, keys_wide, precision=highest)
        next_state = carry_state * jnp.exp(tail_sum)[..., None, None] + fresh_state
        return (next_state, inside + carried)
    blocked = (values.reshape(block_count, BLOCK, groups, head_count, head_dim), key_rows.reshape(block_count, BLOCK, groups, state_len), queries.reshape(block_count, BLOCK, groups, state_len), step_sizes.reshape(block_count, BLOCK, groups, head_count), log_decay.reshape(block_count, BLOCK, groups, head_count))
    start_state = jnp.zeros((groups, head_count, head_dim, state_len), jnp.float32)
    end_state, outputs = lax.scan(one_block, start_state, blocked)
    return outputs.reshape(length, groups, head_count, head_dim)

def head_group(values, key_rows, queries, step_raw, decay_log):
    length = values.shape[0]
    head_count = step_raw.shape[1]
    groups = key_rows.shape[1]
    per_group = head_count // groups
    head_dim = values.shape[1] // head_count
    step_sizes = jax.nn.softplus(step_raw.astype(jnp.float32)).reshape(length, groups, per_group)
    decay_rates = jnp.exp(decay_log.astype(jnp.float32)).reshape(groups, per_group)
    return block_pass(values.reshape(length, groups, per_group, head_dim), key_rows, queries, step_sizes, decay_rates)

def unit_rms(values):
    return values * lax.rsqrt(lax.optimization_barrier(jnp.mean(values * values, axis=-1, keepdims=True)) + EPS)

def gate_and_norm(mixed_heads, gate_raw, gain):
    length, groups, per_group, head_dim = mixed_heads.shape
    gated = mixed_heads.reshape(length, -1) * jax.nn.silu(gate_raw.astype(jnp.float32))
    normed = unit_rms(gated.reshape(length, groups * per_group, head_dim))
    return (normed.reshape(length, -1) * gain.astype(jnp.float32)).astype(jnp.bfloat16)

def blockwise_sum(pairs, length, features):
    summed = jnp.zeros((length, features), jnp.float32)
    for index in range(HEAD_BLOCKS):
        partial_value = jnp.zeros((length, features), jnp.float32)
        for left, right in pairs:
            cols = left.shape[1] // HEAD_BLOCKS
            partial_value = partial_value + jnp.dot(left[:, index * cols:(index + 1) * cols], right[index * cols:(index + 1) * cols], preferred_element_type=jnp.float32)
        summed = summed + rounded(partial_value)
    return summed

def reference(residual, small_heads, large_heads, state_keys, state_queries, small_gate, large_gate, small_step, large_step, small_taps, large_taps, key_taps, query_taps, small_decay, large_decay, small_gain, large_gain, small_out, large_out, mixer_gain, ffn_in_gain, gate_proj, up_proj, down_proj, ffn_out_gain):
    length = residual.shape[0]
    halo_rows = small_taps.shape[0] - 1

    def extended(values):
        return jnp.concatenate([jnp.zeros((halo_rows,) + values.shape[1:], values.dtype), values], axis=0)
    small_conv = causal_taps(extended(small_heads), small_taps, length)
    large_conv = causal_taps(extended(large_heads), large_taps, length)
    key_conv = causal_taps(extended(state_keys), key_taps, length)
    query_conv = causal_taps(extended(state_queries), query_taps, length)
    small_mix = head_group(small_conv, key_conv[:, 0::2], query_conv[:, 0::2], small_step, small_decay)
    large_mix = head_group(large_conv, key_conv[:, 1::2], query_conv[:, 1::2], large_step, large_decay)
    small_normed = gate_and_norm(small_mix, small_gate, small_gain)
    large_normed = gate_and_norm(large_mix, large_gate, large_gain)
    mix = blockwise_sum([(small_normed, small_out), (large_normed, large_out)], length, D)
    mixed = residual.astype(jnp.float32) + unit_rms(mix) * mixer_gain.astype(jnp.float32)
    normed_in = (unit_rms(mixed) * ffn_in_gain.astype(jnp.float32)).astype(jnp.bfloat16)
    gate = jnp.dot(normed_in, gate_proj, preferred_element_type=jnp.float32)
    up_values = jnp.dot(normed_in, up_proj, preferred_element_type=jnp.float32)
    hidden = (jax.nn.silu(gate) * up_values).astype(jnp.bfloat16)
    ffn = blockwise_sum([(hidden, jnp.transpose(down_proj))], length, D)
    updated = mixed + 0.5 * unit_rms(ffn) * ffn_out_gain.astype(jnp.float32)
    return updated.astype(jnp.bfloat16)
```

```python
import functools

import jax
import jax.numpy as jnp
from jax import lax
from jax.experimental import pallas as pl
from jax.experimental.pallas import tpu as pltpu
from jax.sharding import Mesh
from jax.sharding import PartitionSpec as P

BLOCK = 128
ROWS = 1024
NBLK = ROWS // BLOCK
SP = ("sp_0", "sp_1", "sp_2")
SP_TP = ("sp_0", "sp_1", "sp_2", "tp")
EPS = 1e-06
MESH = pl.DeviceIdType.MESH
F32 = jnp.float32
BF16 = jnp.bfloat16


def dot(a, b, contract=((1,), (0,)), precision=None):
    return lax.dot_general(
        a, b, (contract, ((), ())), preferred_element_type=F32, precision=precision
    )


def silu(v):
    return v * jax.nn.sigmoid(v)


def spread(m):
    rows = m.shape[0]
    low = lax.broadcasted_iota(jnp.int32, (rows, 128), 1) < 64
    cols = [jnp.broadcast_to(m[:, h : h + 1], (rows, 128)) for h in range(6)]
    return (
        jnp.where(low, cols[0], cols[1]),
        jnp.where(low, cols[2], cols[3]),
        cols[4],
        cols[5],
    )


def block_rows(b):
    return pl.ds(pl.multiple_of(b * BLOCK, BLOCK), BLOCK)


def ssm_kernel(
    sh, lh, ks, qs, sg, lg, sst, lst, stap, ltap, ktap, qtap, sdec, ldec, sgain, lgain,
    out,
    xs, xl, kc, qc, dtt, ct, ccol, dcol, hloc, eoff, inside,
    halo, mine, mine_tot, sbuf, sib, sib_tot, ysend, ytot_send, yrec, ytot, zsend, ztot_send, zrec, ztot, esend, ebuf,
    hs_sem, hr_sem, s1_sem, r1_sem, ys_sem, yr_sem, zs_sem, zr_sem, s4_sem, r4_sem,
):
    z = lax.axis_index("sp_0")
    y = lax.axis_index("sp_1")
    c = lax.axis_index("sp_2")
    sp = (z * 4 + y) * 2 + c
    nxt = lax.rem(sp + 1, 32)
    prv = lax.rem(sp + 31, 32)

    def at_sp(i):
        return {"sp_0": i // 8, "sp_1": lax.rem(i // 2, 4), "sp_2": lax.rem(i, 2)}

    ypeers = [{"sp_1": lax.rem(y + d, 4)} for d in (1, 2, 3)]
    zpeers = [{"sp_0": lax.rem(z + d, 4)} for d in (1, 2, 3)]
    sibling = {"sp_2": 1 - c}
    barrier = pltpu.get_barrier_semaphore()
    peers = [at_sp(nxt), at_sp(prv), sibling] + ypeers + zpeers
    for peer in peers:
        pl.semaphore_signal(barrier, inc=1, device_id=peer, device_id_type=MESH)
    pl.semaphore_wait(barrier, len(peers))

    sources = (sh, lh, ks, qs)
    halo_copies = [
        pltpu.make_async_remote_copy(
            src_ref=src.at[pl.ds(ROWS - 16, 16)], dst_ref=halo.at[i],
            send_sem=hs_sem.at[i], recv_sem=hr_sem.at[i],
            device_id=at_sp(nxt), device_id_type=MESH,
        )
        for i, src in enumerate(sources)
    ]
    for copy in halo_copies:
        copy.start()

    dtt[...] = jnp.zeros_like(dtt)
    dtt[0:4, :] = jax.nn.softplus(sst[...])
    dtt[4:6, :] = jax.nn.softplus(lst[...])
    ct[...] = jnp.zeros_like(ct)
    for h in range(6):
        d = sdec[h] if h < 4 else ldec[h - 4]
        rate = jnp.exp(jnp.full((1, ROWS), d, F32))
        ct[h : h + 1, :] = -dtt[h : h + 1, :] * rate
    tr = lax.broadcasted_iota(jnp.int32, (BLOCK, BLOCK), 0)
    tc = lax.broadcasted_iota(jnp.int32, (BLOCK, BLOCK), 1)
    upper = (tr <= tc).astype(F32)
    low = tc < 64
    causal = tc <= tr

    def sums(b, _):
        rows = block_rows(b)
        cum = dot(ct[:, rows], upper, precision=lax.Precision.HIGHEST)
        ct[:, rows] = cum
        pad = jnp.zeros((BLOCK - 8, BLOCK), F32)
        ccol[rows, :] = jnp.concatenate([cum, pad], axis=0).T
        dcol[rows, :] = jnp.concatenate([dtt[:, rows], pad], axis=0).T
        return 0

    lax.fori_loop(0, NBLK, sums, 0)

    taps = (stap, ltap, ktap, qtap)
    dests = (xs, xl, kc, qc)

    def conv_of(ext, tap):
        acc = jnp.zeros((BLOCK, 256), F32)
        for k in range(4):
            shifted = ext if k == 3 else pltpu.roll(ext, 3 - k, 0)
            acc = acc + tap[k : k + 1, :].astype(F32) * shifted[16:, :]
        return silu(acc).astype(BF16)

    def conv_block(b, _):
        start = pl.multiple_of(b * BLOCK - 16, 16)
        for src, tap, dst in zip(sources, taps, dests):
            ext = src[pl.ds(start, BLOCK + 16), :].astype(F32)
            dst[block_rows(b), :] = conv_of(ext, tap)
        return 0

    lax.fori_loop(1, NBLK, conv_block, 0)
    for copy in halo_copies:
        copy.wait()
    keep = jnp.where(sp == 0, 0.0, 1.0)
    for i, (src, tap, dst) in enumerate(zip(sources, taps, dests)):
        before = halo[i].astype(F32) * keep
        ext = jnp.concatenate([before, src[0:BLOCK, :].astype(F32)], axis=0)
        dst[0:BLOCK, :] = conv_of(ext, tap)

    mine[...] = jnp.zeros_like(mine)
    mine_tot[...] = jnp.zeros_like(mine_tot)

    def states(b, _):
        rows = block_rows(b)
        cb = ccol[rows, :]
        last = cb[BLOCK - 1 : BLOCK, :]
        scale = spread(dcol[rows, :] * jnp.exp(last - cb))
        xsb = xs[rows, :].astype(F32)
        xlb = xl[rows, :].astype(F32)
        us = jnp.concatenate([xsb[:, :128] * scale[0], xsb[:, 128:] * scale[1]], axis=1)
        ul = jnp.concatenate([xlb[:, :128] * scale[2], xlb[:, 128:] * scale[3]], axis=1)
        fresh_s = dot(kc[rows, 0:128], us.astype(BF16), ((0,), (0,)))
        fresh_l = dot(kc[rows, 128:256], ul.astype(BF16), ((0,), (0,)))
        state = mine[...]
        tot = mine_tot[...]
        hloc[b] = state
        eoff[b] = jnp.exp(tot)
        step = jnp.concatenate(spread(jnp.broadcast_to(last, (8, 128))), axis=1)
        mine[...] = state * jnp.exp(step)[0:1, :] + jnp.concatenate([fresh_s, fresh_l], axis=1)
        mine_tot[...] = tot + step
        return 0

    lax.fori_loop(0, NBLK, states, 0)

    sbuf[...] = mine[...].astype(BF16)
    r1 = [
        pltpu.make_async_remote_copy(
            src_ref=src, dst_ref=dst, send_sem=s1_sem.at[i], recv_sem=r1_sem.at[i],
            device_id=sibling, device_id_type=MESH,
        )
        for i, (src, dst) in enumerate(((sbuf, sib), (mine_tot, sib_tot)))
    ]
    for copy in r1:
        copy.start()

    def intra(b, _):
        rows = block_rows(b)
        cb = ccol[rows, :]
        parts = []
        for g, x in ((0, xs), (1, xl)):
            lanes = slice(g * 128, g * 128 + 128)
            scores = dot(qc[rows, lanes], kc[rows, lanes], ((1,), (1,)))
            heads = []
            for h in range(4) if g == 0 else range(4, 6):
                gap = jnp.broadcast_to(cb[:, h : h + 1], (BLOCK, BLOCK)) - ct[h : h + 1, rows]
                decay = jnp.exp(jnp.where(causal, gap, -1e30))
                w = (scores * decay * dtt[h : h + 1, rows]).astype(BF16)
                at = (h // 2 if g == 0 else h - 4) * 128
                heads.append(dot(w, x[rows, at : at + 128]))
            if g == 0:
                parts += [jnp.where(low, heads[0], heads[1]), jnp.where(low, heads[2], heads[3])]
            else:
                parts += heads
        inside[rows, :] = jnp.concatenate(parts, axis=1)
        return 0

    lax.fori_loop(0, 2, intra, 0)
    for copy in r1:
        copy.wait()

    half = pl.ds(pl.multiple_of(c * 64, 64), 64)
    my_half = mine[half, :]
    sib_half = sib[half, :].astype(F32)
    first = c == 0
    t_me = mine_tot[...]
    t_sib = sib_tot[...]
    early = jnp.where(first, my_half, sib_half)
    late = jnp.where(first, sib_half, my_half)
    t_late = jnp.where(first, t_sib, t_me)
    chip = early * jnp.exp(t_late)[0:1, :] + late
    chip_tot = t_me + t_sib
    ysend[...] = chip.astype(BF16)
    ytot_send[...] = chip_tot
    def peer_copies(send, tot_send, rec, tot_rec, sems, peers_):
        ss, rs = sems
        made = []
        for i, peer in enumerate(peers_):
            for j, (src, dst) in enumerate(((send, rec.at[i]), (tot_send, tot_rec.at[i]))):
                made.append(pltpu.make_async_remote_copy(
                    src_ref=src, dst_ref=dst, send_sem=ss.at[2 * i + j], recv_sem=rs.at[2 * i + j],
                    device_id=peer, device_id_type=MESH,
                ))
        return made

    r2 = peer_copies(ysend, ytot_send, yrec, ytot, (ys_sem, yr_sem), ypeers)
    for copy in r2:
        copy.start()
    lax.fori_loop(2, 5, intra, 0)
    for copy in r2:
        copy.wait()

    def before_of(pos, rec, tot_rec):
        e = jnp.zeros((64, 512), F32)
        t = jnp.zeros((8, 512), F32)
        for d in (3, 2, 1):
            valid = d <= pos
            e = jnp.where(valid, e * jnp.exp(tot_rec[d - 1])[0:1, :] + rec[d - 1].astype(F32), e)
            t = jnp.where(valid, t + tot_rec[d - 1], t)
        return e, t

    ey, ty = before_of(y, yrec, ytot)
    plane = ey * jnp.exp(chip_tot)[0:1, :] + chip
    plane_tot = ty + chip_tot
    for e in (1, 2, 3):
        valid = y + e <= 3
        plane = jnp.where(valid, plane * jnp.exp(ytot[3 - e])[0:1, :] + yrec[3 - e].astype(F32), plane)
        plane_tot = jnp.where(valid, plane_tot + ytot[3 - e], plane_tot)
    zsend[...] = plane.astype(BF16)
    ztot_send[...] = plane_tot
    r3 = peer_copies(zsend, ztot_send, zrec, ztot, (zs_sem, zr_sem), zpeers)
    for copy in r3:
        copy.start()
    lax.fori_loop(5, NBLK, intra, 0)
    for copy in r3:
        copy.wait()
    ez, _ = before_of(z, zrec, ztot)
    entering = ez * jnp.exp(ty)[0:1, :] + ey
    esend[...] = entering
    r4 = pltpu.make_async_remote_copy(
        src_ref=esend, dst_ref=ebuf.at[half], send_sem=s4_sem, recv_sem=r4_sem,
        device_id=sibling, device_id_type=MESH,
    )
    r4.start()
    r4.wait()
    own = esend[...]
    enter_rows = []
    for i in range(2):
        arrived = ebuf[i * 64 : i * 64 + 64, :]
        enter_rows.append(jnp.where(c == i, own, arrived))
    enter = jnp.concatenate(enter_rows, axis=0)
    second = enter * jnp.exp(t_sib)[0:1, :] + sib[...].astype(F32)
    mine[...] = jnp.where(first, enter, second)

    def finish(b, _):
        rows = block_rows(b)
        state = (hloc[b] + eoff[b][0:1, :] * mine[...]).astype(BF16)
        grow = spread(jnp.exp(ccol[rows, :]))
        carried = [dot(qc[rows, g * 128 : g * 128 + 128], state[:, g * 256 : g * 256 + 256]) for g in (0, 1)]
        for i in range(4):
            g, at = i // 2, (i % 2) * 128
            gate_ref = sg if g == 0 else lg
            gain_ref = sgain if g == 0 else lgain
            v = inside[rows, i * 128 : i * 128 + 128] + carried[g][:, at : at + 128] * grow[i]
            v = v * silu(gate_ref[rows, at : at + 128].astype(F32))
            sq = v * v
            if g == 0:
                s0 = jnp.sum(jnp.where(low, sq, 0.0), axis=1, keepdims=True)
                s1 = jnp.sum(jnp.where(low, 0.0, sq), axis=1, keepdims=True)
                inv = jnp.where(low, lax.rsqrt(s0 / 64 + EPS), lax.rsqrt(s1 / 64 + EPS))
            else:
                inv = lax.rsqrt(jnp.sum(sq, axis=1, keepdims=True) / 128 + EPS)
            v = v * inv * gain_ref[:, at : at + 128].astype(F32)
            out[rows, i * 128 : i * 128 + 128] = v.astype(BF16)
        return 0

    lax.fori_loop(0, NBLK, finish, 0)


def ssm(*operands):
    vm = pl.BlockSpec(memory_space=pltpu.VMEM)
    sm = pl.BlockSpec(memory_space=pltpu.SMEM)
    dma = pltpu.SemaphoreType.DMA
    rows_bf = pltpu.VMEM((ROWS, 256), BF16)
    return pl.pallas_call(
        ssm_kernel,
        name="ssm",
        out_shape=jax.ShapeDtypeStruct((ROWS, 512), BF16),
        in_specs=[vm] * 12 + [sm] * 2 + [vm] * 2,
        out_specs=vm,
        scratch_shapes=[
            rows_bf, rows_bf, rows_bf, rows_bf,
            pltpu.VMEM((8, ROWS), F32), pltpu.VMEM((8, ROWS), F32),
            pltpu.VMEM((ROWS, 128), F32), pltpu.VMEM((ROWS, 128), F32),
            pltpu.VMEM((NBLK, 128, 512), F32), pltpu.VMEM((NBLK, 8, 512), F32),
            pltpu.VMEM((ROWS, 512), F32),
            pltpu.VMEM((4, 16, 256), BF16),
            pltpu.VMEM((128, 512), F32), pltpu.VMEM((8, 512), F32),
            pltpu.VMEM((128, 512), BF16), pltpu.VMEM((128, 512), BF16), pltpu.VMEM((8, 512), F32),
            pltpu.VMEM((64, 512), BF16), pltpu.VMEM((8, 512), F32),
            pltpu.VMEM((3, 64, 512), BF16), pltpu.VMEM((3, 8, 512), F32),
            pltpu.VMEM((64, 512), BF16), pltpu.VMEM((8, 512), F32),
            pltpu.VMEM((3, 64, 512), BF16), pltpu.VMEM((3, 8, 512), F32),
            pltpu.VMEM((64, 512), F32), pltpu.VMEM((128, 512), F32),
            dma((4,)), dma((4,)), dma((2,)), dma((2,)), dma((6,)), dma((6,)), dma((6,)), dma((6,)), dma, dma,
        ],
        compiler_params=pltpu.CompilerParams(collective_id=0, has_side_effects=True, vmem_limit_bytes=48 * 1024 * 1024),
        cost_estimate=pl.CostEstimate(flops=4_000_000_000, bytes_accessed=5_000_000, transcendentals=0),
    )(*operands)


def unit_rms(values):
    return values * lax.rsqrt(jnp.mean(values * values, axis=-1, keepdims=True) + EPS)


def local(
    residual, small_heads, large_heads, state_keys, state_queries, small_gate, large_gate,
    small_step, large_step, small_taps, large_taps, key_taps, query_taps, small_decay, large_decay,
    small_gain, large_gain, small_out, large_out, mixer_gain, ffn_in_gain,
    gate_proj, up_proj, down_proj, ffn_out_gain,
):
    length = residual.shape[0]
    weights = lax.all_gather(
        jnp.concatenate([gate_proj, up_proj, down_proj], axis=1), SP, axis=0, tiled=True
    )
    ff = gate_proj.shape[1]
    normed = ssm(
        small_heads, large_heads, state_keys.reshape(length, 256), state_queries.reshape(length, 256),
        small_gate, large_gate, small_step.T, large_step.T, small_taps, large_taps,
        key_taps.reshape(4, 256), query_taps.reshape(4, 256), small_decay, large_decay,
        small_gain.reshape(1, 256), large_gain.reshape(1, 256),
    )
    partial_value = jnp.dot(normed[:, :256], small_out, preferred_element_type=F32)
    partial_value = partial_value + jnp.dot(normed[:, 256:], large_out, preferred_element_type=F32)
    mix = lax.psum_scatter(partial_value.astype(BF16), "tp", scatter_dimension=0, tiled=True).astype(F32)
    share = length // lax.axis_size("tp")
    own = lax.dynamic_slice_in_dim(residual, lax.axis_index("tp") * share, share, 0).astype(F32)
    mixed = own + unit_rms(mix) * mixer_gain.astype(F32)
    normed_in = (unit_rms(mixed) * ffn_in_gain.astype(F32)).astype(BF16)
    normed_in = lax.all_gather(normed_in, "tp", axis=0, tiled=True)
    gate = jnp.dot(normed_in, weights[:, :ff], preferred_element_type=F32)
    up_values = jnp.dot(normed_in, weights[:, ff : 2 * ff], preferred_element_type=F32)
    hidden = (jax.nn.silu(gate) * up_values).astype(BF16)
    ffn = lax.psum_scatter(
        lax.dot_general(
            hidden, weights[:, 2 * ff :], (((1,), (1,)), ((), ())), preferred_element_type=F32
        ).astype(BF16),
        "tp", scatter_dimension=0, tiled=True,
    ).astype(F32)
    updated = mixed + 0.5 * unit_rms(ffn) * ffn_out_gain.astype(F32)
    return updated.astype(BF16)


def solution(mesh):
    torus = Mesh(mesh.devices.reshape(4, 4, 2, mesh.shape["tp"]), ("sp_0", "sp_1", "sp_2", "tp"))
    in_specs = (
        P(SP, None), P(SP, "tp"), P(SP, "tp"), P(SP, "tp", None), P(SP, "tp", None),
        P(SP, "tp"), P(SP, "tp"), P(SP, "tp"), P(SP, "tp"),
        P(None, "tp"), P(None, "tp"), P(None, "tp", None), P(None, "tp", None),
        P("tp"), P("tp"), P("tp"), P("tp"), P("tp", None), P("tp", None),
        P(), P(), P(SP, "tp"), P(SP, "tp"), P(SP, "tp"), P(),
    )
    return jax.shard_map(local, mesh=torus, in_specs=in_specs, out_specs=P(SP_TP, None), check_vma=False)
```

```python
import functools

import jax
import jax.numpy as jnp
from jax import lax
from jax.experimental import pallas as pl
from jax.experimental.pallas import tpu as pltpu
from jax.sharding import Mesh
from jax.sharding import PartitionSpec as P

BLOCK = 128
ROWS = 1024
NBLK = ROWS // BLOCK
SP = ("sp_0", "sp_1", "sp_2")
SP_TP = ("sp_0", "sp_1", "sp_2", "tp")
EPS = 1e-06
MESH = pl.DeviceIdType.MESH
F32 = jnp.float32
BF16 = jnp.bfloat16


def dot(a, b, contract=((1,), (0,)), precision=None):
    return lax.dot_general(
        a, b, (contract, ((), ())), preferred_element_type=F32, precision=precision
    )


def silu(v):
    return v * jax.nn.sigmoid(v)


def spread(m):
    rows = m.shape[0]
    low = lax.broadcasted_iota(jnp.int32, (rows, 128), 1) < 64
    cols = [jnp.broadcast_to(m[:, h : h + 1], (rows, 128)) for h in range(6)]
    return (
        jnp.where(low, cols[0], cols[1]),
        jnp.where(low, cols[2], cols[3]),
        cols[4],
        cols[5],
    )


def block_rows(b):
    return pl.ds(pl.multiple_of(b * BLOCK, BLOCK), BLOCK)


OWN = 256
FF_DEV = 1408
UP_COLS = pl.ds(0, 2 * FF_DEV)
DOWN_COLS = pl.ds(2 * FF_DEV, FF_DEV)


class Net:
    def __init__(self, send_sems, recv_sems):
        self.send_sems, self.recv_sems, self.used = send_sems, recv_sems, 0

    def copy(self, src, dst, peer):
        i = self.used
        self.used += 1
        return pltpu.make_async_remote_copy(
            src_ref=src, dst_ref=dst, send_sem=self.send_sems.at[i], recv_sem=self.recv_sems.at[i],
            device_id=peer, device_id_type=MESH,
        )


class Ring:
    def __init__(self, net, axis, at, view, pieces=(None,)):
        self.net, self.at, self.view = net, at, view
        self.before, self.after = lax.rem(at + 3, 4), lax.rem(at + 1, 4)
        self.up, self.down = {axis: self.after}, {axis: self.before}
        self.ups = [net.copy(view(at, p), view(at, p), self.up) for p in pieces]
        self.downs = [net.copy(view(at, p), view(at, p), self.down) for p in pieces[::-1]]
        self.forwards = []

    def start(self):
        for pair in zip(self.ups, self.downs):
            for copy in pair:
                copy.start()

    def forward(self):
        self.ups[0].wait_recv()
        here = self.view(self.before, 0)
        self.forwards.append(self.net.copy(here, here, self.up))
        self.forwards[-1].start()
        self.downs[0].wait_recv()
        here = self.view(self.after, 1)
        self.forwards.append(self.net.copy(here, here, self.down))
        self.forwards[-1].start()

    def neighbours(self):
        for copy in self.ups[1:] + self.downs[1:]:
            copy.wait_recv()

    def finish(self):
        for copy in self.forwards:
            copy.wait_recv()
        for copy in self.ups + self.downs + self.forwards:
            copy.wait_send()


def layer_kernel(
    residual, sh_in, lh_in, ks_in, qs_in, sg_in, lg_in, gate_in, up_in, down_in, so_in, lo_in,
    steps, params, sdec, ldec,
    out,
    sh, lh, ks, qs, sg, lg,
    xs, xl, kc, qc, dtt, ct, ccol, dcol, hloc, eoff, inside,
    halo, mine, mine_tot, sbuf, sib, sib_tot, ysend, ytot_send, yrec, ytot, zsend, ztot_send, zrec, ztot, esend, ebuf,
    heads, chans, weights, projs, res, mixed, rows_in, hidden, parts_out, relay, relay_sum, from_left, from_right,
    send_sems, recv_sems, load_sems,
):
    z = lax.axis_index("sp_0")
    y = lax.axis_index("sp_1")
    c = lax.axis_index("sp_2")
    x = lax.axis_index("tp")
    sp = (z * 4 + y) * 2 + c
    nxt = lax.rem(sp + 1, 32)
    prv = lax.rem(sp + 31, 32)
    left, right, across = lax.rem(x + 3, 4), lax.rem(x + 1, 4), lax.rem(x + 2, 4)
    net = Net(send_sems, recv_sems)

    def at_sp(i):
        return {"sp_0": i // 8, "sp_1": lax.rem(i // 2, 4), "sp_2": lax.rem(i, 2)}

    loads = [
        pltpu.make_async_copy(src, dst, load_sems.at[i])
        for i, (src, dst) in enumerate((
            (sh_in, sh), (lh_in, lh), (ks_in, ks), (qs_in, qs),
            (gate_in, weights.at[z, y, c, :, pl.ds(0, FF_DEV)]),
            (up_in, weights.at[z, y, c, :, pl.ds(FF_DEV, FF_DEV)]),
            (down_in, weights.at[z, y, c, :, DOWN_COLS]),
            (so_in, projs.at[x, pl.ds(0, 256)]),
            (lo_in, projs.at[x, pl.ds(256, 256)]),
            (sg_in, sg), (lg_in, lg),
            (residual.at[pl.ds(pl.multiple_of(x * OWN, OWN), OWN)], res),
        ))
    ]
    for copy in loads:
        copy.start()
    loads_in, loads_own, loads_gate = loads[:4], loads[4:9], loads[9:]

    ypeers = [{"sp_1": lax.rem(y + d, 4)} for d in (1, 2, 3)]
    zpeers = [{"sp_0": lax.rem(z + d, 4)} for d in (1, 2, 3)]
    xpeers = [{"tp": i} for i in (across, right, left)]
    sibling = {"sp_2": 1 - c}
    barrier = pltpu.get_barrier_semaphore()
    peers = [at_sp(nxt), at_sp(prv), sibling] + ypeers + zpeers + xpeers
    for peer in peers:
        pl.semaphore_signal(barrier, inc=1, device_id=peer, device_id_type=MESH)
    pl.semaphore_wait(barrier, len(peers))

    sources = (sh, lh, ks, qs)
    halo_copies = [
        net.copy(src.at[pl.ds(ROWS - 16, 16)], halo.at[i], at_sp(nxt)) for i, src in enumerate((sh_in, lh_in, ks_in, qs_in))
    ]
    for copy in halo_copies:
        copy.start()

    def span(part, size):
        return pl.ds(0, size) if part is None else pl.ds(part * (size // 2), size // 2)

    def y_first(cols):
        return lambda i, p=None: weights.at[z, i, c, span(p, 32), cols]

    def z_first(cols):
        return lambda i, p=None: weights.at[i, y, c, pl.ds(32, 32) if p is None else pl.ds(32 + 16 * p, 16), cols]

    def z_view(cols):
        return lambda i, p=None: weights.at[i, span(p, 4), c, pl.ds(0, 32), cols]

    def y_view(cols):
        return lambda i, p=None: weights.at[span(p, 4), i, c, pl.ds(32, 32), cols]

    def proj_view(i, p=None):
        size = 256 if p is None else 128
        return projs.at[i, pl.ds(pl.multiple_of(c * 256 + (0 if p is None else p * 128), 128), size)]

    for copy in loads_own:
        copy.wait()
    first_rings = [
        Ring(net, axis, at, view(cols))
        for cols in (UP_COLS, DOWN_COLS)
        for axis, at, view in (("sp_1", y, y_first), ("sp_0", z, z_first))
    ]
    proj = Ring(net, "tp", x, proj_view)
    for ring in first_rings + [proj]:
        ring.start()

    dtt[...] = jax.nn.softplus(steps[...])
    ct[...] = jnp.zeros_like(ct)
    for h in range(6):
        d = sdec[h] if h < 4 else ldec[h - 4]
        rate = jnp.exp(jnp.full((1, ROWS), d, F32))
        ct[h : h + 1, :] = -dtt[h : h + 1, :] * rate
    tr = lax.broadcasted_iota(jnp.int32, (BLOCK, BLOCK), 0)
    tc = lax.broadcasted_iota(jnp.int32, (BLOCK, BLOCK), 1)
    upper = (tr <= tc).astype(F32)
    low = tc < 64
    causal = tc <= tr

    def sums(b, _):
        rows = block_rows(b)
        cum = dot(ct[:, rows], upper, precision=lax.Precision.HIGHEST)
        ct[:, rows] = cum
        pad = jnp.zeros((BLOCK - 8, BLOCK), F32)
        ccol[rows, :] = jnp.concatenate([cum, pad], axis=0).T
        dcol[rows, :] = jnp.concatenate([dtt[:, rows], pad], axis=0).T
        return 0

    lax.fori_loop(0, NBLK, sums, 0)

    taps = [params[3:7, i * 256 : i * 256 + 256] for i in range(4)]
    dests = (xs, xl, kc, qc)

    def conv_of(ext, tap):
        acc = jnp.zeros((BLOCK, 256), F32)
        for k in range(4):
            shifted = ext if k == 3 else pltpu.roll(ext, 3 - k, 0)
            acc = acc + tap[k : k + 1, :] * shifted[16:, :]
        return silu(acc).astype(BF16)

    def conv_block(b, _):
        start = pl.multiple_of(b * BLOCK - 16, 16)
        for src, tap, dst in zip(sources, taps, dests):
            ext = src[pl.ds(start, BLOCK + 16), :].astype(F32)
            dst[block_rows(b), :] = conv_of(ext, tap)
        return 0

    for copy in loads_in:
        copy.wait()
    lax.fori_loop(1, NBLK, conv_block, 0)
    for copy in halo_copies:
        copy.wait()
    keep = jnp.where(sp == 0, 0.0, 1.0)
    for i, (src, tap, dst) in enumerate(zip(sources, taps, dests)):
        before = halo[i].astype(F32) * keep
        ext = jnp.concatenate([before, src[0:BLOCK, :].astype(F32)], axis=0)
        dst[0:BLOCK, :] = conv_of(ext, tap)

    for ring in first_rings:
        ring.forward()

    mine[...] = jnp.zeros_like(mine)
    mine_tot[...] = jnp.zeros_like(mine_tot)

    def states(b, _):
        rows = block_rows(b)
        cb = ccol[rows, :]
        last = cb[BLOCK - 1 : BLOCK, :]
        scale = spread(dcol[rows, :] * jnp.exp(last - cb))
        xsb = xs[rows, :].astype(F32)
        xlb = xl[rows, :].astype(F32)
        us = jnp.concatenate([xsb[:, :128] * scale[0], xsb[:, 128:] * scale[1]], axis=1)
        ul = jnp.concatenate([xlb[:, :128] * scale[2], xlb[:, 128:] * scale[3]], axis=1)
        fresh_s = dot(kc[rows, 0:128], us.astype(BF16), ((0,), (0,)))
        fresh_l = dot(kc[rows, 128:256], ul.astype(BF16), ((0,), (0,)))
        state = mine[...]
        tot = mine_tot[...]
        hloc[b] = state
        eoff[b] = jnp.exp(tot)
        step = jnp.concatenate(spread(jnp.broadcast_to(last, (8, 128))), axis=1)
        mine[...] = state * jnp.exp(step)[0:1, :] + jnp.concatenate([fresh_s, fresh_l], axis=1)
        mine_tot[...] = tot + step
        return 0

    lax.fori_loop(0, NBLK, states, 0)

    sbuf[...] = mine[...].astype(BF16)
    r1 = [net.copy(sbuf, sib, sibling), net.copy(mine_tot, sib_tot, sibling)]
    for copy in r1:
        copy.start()

    def intra(b, _):
        rows = block_rows(b)
        cb = ccol[rows, :]
        parts = []
        for g, vals in ((0, xs), (1, xl)):
            lanes = slice(g * 128, g * 128 + 128)
            scores = dot(qc[rows, lanes], kc[rows, lanes], ((1,), (1,)))
            found = []
            for h in range(4) if g == 0 else range(4, 6):
                gap = jnp.broadcast_to(cb[:, h : h + 1], (BLOCK, BLOCK)) - ct[h : h + 1, rows]
                decay = jnp.exp(jnp.where(causal, gap, -1e30))
                w = (scores * decay * dtt[h : h + 1, rows]).astype(BF16)
                at = (h // 2 if g == 0 else h - 4) * 128
                found.append(dot(w, vals[rows, at : at + 128]))
            if g == 0:
                parts += [jnp.where(low, found[0], found[1]), jnp.where(low, found[2], found[3])]
            else:
                parts += found
        inside[rows, :] = jnp.concatenate(parts, axis=1)
        return 0

    lax.fori_loop(0, 2, intra, 0)
    for copy in r1:
        copy.wait()

    half = pl.ds(pl.multiple_of(c * 64, 64), 64)
    my_half = mine[half, :]
    sib_half = sib[half, :].astype(F32)
    first = c == 0
    t_me = mine_tot[...]
    t_sib = sib_tot[...]
    early = jnp.where(first, my_half, sib_half)
    late = jnp.where(first, sib_half, my_half)
    t_late = jnp.where(first, t_sib, t_me)
    chip = early * jnp.exp(t_late)[0:1, :] + late
    chip_tot = t_me + t_sib
    ysend[...] = chip.astype(BF16)
    ytot_send[...] = chip_tot

    def peer_copies(send, tot_send, rec, tot_rec, peers_):
        made = []
        for i, peer in enumerate(peers_):
            made += [net.copy(send, rec.at[i], peer), net.copy(tot_send, tot_rec.at[i], peer)]
        return made

    r2 = peer_copies(ysend, ytot_send, yrec, ytot, ypeers)
    for copy in r2:
        copy.start()
    lax.fori_loop(2, 5, intra, 0)
    for copy in r2:
        copy.wait()

    def before_of(pos, rec, tot_rec):
        e = jnp.zeros((64, 512), F32)
        t = jnp.zeros((8, 512), F32)
        for d in (3, 2, 1):
            valid = d <= pos
            e = jnp.where(valid, e * jnp.exp(tot_rec[d - 1])[0:1, :] + rec[d - 1].astype(F32), e)
            t = jnp.where(valid, t + tot_rec[d - 1], t)
        return e, t

    ey, ty = before_of(y, yrec, ytot)
    plane = ey * jnp.exp(chip_tot)[0:1, :] + chip
    plane_tot = ty + chip_tot
    for e in (1, 2, 3):
        valid = y + e <= 3
        plane = jnp.where(valid, plane * jnp.exp(ytot[3 - e])[0:1, :] + yrec[3 - e].astype(F32), plane)
        plane_tot = jnp.where(valid, plane_tot + ytot[3 - e], plane_tot)
    zsend[...] = plane.astype(BF16)
    ztot_send[...] = plane_tot
    r3 = peer_copies(zsend, ztot_send, zrec, ztot, zpeers)
    for copy in r3:
        copy.start()
    for ring in first_rings:
        ring.finish()
    second_rings = [
        Ring(net, axis, at, view(cols))
        for cols in (UP_COLS, DOWN_COLS)
        for axis, at, view in (("sp_0", z, z_view), ("sp_1", y, y_view))
    ]
    for ring in second_rings:
        ring.start()
    shared = [
        [net.copy(z_view(cols)(z), z_view(cols)(z), sibling), net.copy(y_view(cols)(y), y_view(cols)(y), sibling)]
        for cols in (UP_COLS, DOWN_COLS)
    ]
    for group in shared:
        for copy in group:
            copy.start()
    lax.fori_loop(5, NBLK, intra, 0)
    for copy in r3:
        copy.wait()
    ez, _ = before_of(z, zrec, ztot)
    entering = ez * jnp.exp(ty)[0:1, :] + ey
    esend[...] = entering
    r4 = net.copy(esend, ebuf.at[half], sibling)
    r4.start()
    r4.wait()
    own = esend[...]
    enter_rows = []
    for i in range(2):
        arrived = ebuf[i * 64 : i * 64 + 64, :]
        enter_rows.append(jnp.where(c == i, own, arrived))
    enter = jnp.concatenate(enter_rows, axis=0)
    second = enter * jnp.exp(t_sib)[0:1, :] + sib[...].astype(F32)
    mine[...] = jnp.where(first, enter, second)

    proj.forward()
    shared_proj = [net.copy(proj_view(i), proj_view(i), sibling) for i in (x, left, right)]
    for copy in shared_proj:
        copy.start()
    for copy in loads_gate:
        copy.wait()

    def finish(b, _):
        rows = block_rows(b)
        state = (hloc[b] + eoff[b][0:1, :] * mine[...]).astype(BF16)
        grow = spread(jnp.exp(ccol[rows, :]))
        carried = [dot(qc[rows, g * 128 : g * 128 + 128], state[:, g * 256 : g * 256 + 256]) for g in (0, 1)]
        for i in range(4):
            g, at = i // 2, (i % 2) * 128
            gate_ref = sg if g == 0 else lg
            v = inside[rows, i * 128 : i * 128 + 128] + carried[g][:, at : at + 128] * grow[i]
            v = v * silu(gate_ref[rows, at : at + 128].astype(F32))
            sq = v * v
            if g == 0:
                s0 = jnp.sum(jnp.where(low, sq, 0.0), axis=1, keepdims=True)
                s1 = jnp.sum(jnp.where(low, 0.0, sq), axis=1, keepdims=True)
                inv = jnp.where(low, lax.rsqrt(s0 / 64 + EPS), lax.rsqrt(s1 / 64 + EPS))
            else:
                inv = lax.rsqrt(jnp.sum(sq, axis=1, keepdims=True) / 128 + EPS)
            v = v * inv * params[7:8, i * 128 : i * 128 + 128]
            heads[rows, i * 128 : i * 128 + 128] = v.astype(BF16)
        return 0


    exchange = []
    for peer in (across, right, left, x):
        for b in range(2):
            finish(peer * 2 + b, 0)
        rows = pl.ds(pl.multiple_of(peer * OWN, OWN), OWN)
        if peer is not x:
            exchange.append(net.copy(heads.at[rows], chans.at[x], {"tp": peer}))
            exchange[-1].start()
    own_rows = pl.ds(pl.multiple_of(x * OWN, OWN), OWN)
    chans[x] = heads[own_rows, :]

    def share(copies):
        for copy in copies:
            copy.start()
        return copies

    def share_arrived(k, which):
        zr, yr = second_rings[2 * k], second_rings[2 * k + 1]
        cols = (UP_COLS, DOWN_COLS)[k]
        zs = [zr.before, zr.after] if which == 0 else [lax.rem(z + 2, 4)]
        ys = [yr.before, yr.after] if which == 0 else [lax.rem(y + 2, 4)]
        return share(
            [net.copy(z_view(cols)(i), z_view(cols)(i), sibling) for i in zs]
            + [net.copy(y_view(cols)(i), y_view(cols)(i), sibling) for i in ys]
        )

    proj.finish()
    shared_proj += share([net.copy(proj_view(across), proj_view(across), sibling)])
    for k in (0, 1):
        second_rings[2 * k].forward()
        second_rings[2 * k + 1].forward()
        shared[k] += share_arrived(k, 0)
    for copy in shared_proj + exchange:
        copy.wait()

    def project(n, _):
        cols = pl.ds(pl.multiple_of(n * 256, 256), 256)
        acc = dot(chans[0], projs[0, :, cols])
        for i in range(1, 4):
            acc = acc + dot(chans[i], projs[i, :, cols])
        mixed[:, cols] = acc
        return 0

    lax.fori_loop(0, 8, project, 0)

    def norms(r, _):
        rows = pl.ds(pl.multiple_of(r * 32, 32), 32)
        v = mixed[rows, :]
        v = v * lax.rsqrt(jnp.mean(v * v, axis=1, keepdims=True) + EPS)
        v = res[rows, :].astype(F32) + v * params[0:1, :]
        mixed[rows, :] = v
        v = v * lax.rsqrt(jnp.mean(v * v, axis=1, keepdims=True) + EPS)
        rows_in[x, rows, :] = (v * params[1:2, :]).astype(BF16)
        return 0

    lax.fori_loop(0, OWN // 32, norms, 0)

    gather = Ring(net, "tp", x, lambda i, p: rows_in.at[i, pl.ds(p * 128, 128)], (0, 1))
    gather.start()

    def wait_weights(k):
        second_rings[2 * k].finish()
        second_rings[2 * k + 1].finish()
        for copy in shared[k] + share_arrived(k, 1):
            copy.wait()

    def gate_up(i):
        def tile(n, _):
            g_cols = pl.ds(pl.multiple_of(n * 128, 128), 128)
            u_cols = pl.ds(pl.multiple_of(FF_DEV + n * 128, 128), 128)
            w = jnp.concatenate(
                [weights[:, :, :, :, g_cols].reshape(2048, 128), weights[:, :, :, :, u_cols].reshape(2048, 128)], axis=1
            )
            both = dot(rows_in[i], w)
            hidden[:, g_cols] = (silu(both[:, :128]) * both[:, 128:]).astype(BF16)
            return 0

        lax.fori_loop(0, FF_DEV // 128, tile, 0)

    def down(i):
        def tile(n, _):
            w = weights[n // 2, pl.ds(lax.rem(n, 2) * 2, 2), :, :, DOWN_COLS].reshape(256, FF_DEV)
            parts_out[i, :, pl.ds(pl.multiple_of(n * 256, 256), 256)] = dot(hidden[...], w, ((1,), (1,))).astype(BF16)
            return 0

        lax.fori_loop(0, 8, tile, 0)

    h0, h1 = pl.ds(0, 128), pl.ds(128, 128)
    to_left, to_right = {"tp": left}, {"tp": right}
    wait_weights(0)
    gate_up(x)
    wait_weights(1)
    down(x)
    gather.forward()
    gather.neighbours()
    gate_up(left)
    down(left)
    sends = [net.copy(parts_out.at[left, h0], from_right.at[h0], to_left)]
    sends[-1].start()
    gate_up(right)
    down(right)
    sends.append(net.copy(parts_out.at[right, h1], from_left.at[h1], to_right))
    sends[-1].start()
    gather.finish()
    gate_up(across)
    down(across)
    relays = share([
        net.copy(parts_out.at[across, h0], relay.at[0], to_right),
        net.copy(parts_out.at[across, h1], relay.at[1], to_left),
    ])
    for k, (peer, rows, dst, to) in enumerate(((right, h0, from_left, to_right), (left, h1, from_right, to_left))):
        relays[k].wait_recv()
        relay_sum[k] = (parts_out[peer, rows, :].astype(F32) + relay[k].astype(F32)).astype(BF16)
        sends.append(net.copy(relay_sum.at[k], dst.at[rows], to))
        sends[-1].start()
    for copy in relays:
        copy.wait_send()
    for copy in sends:
        copy.wait()

    def last(r, _):
        rows = pl.ds(pl.multiple_of(r * 32, 32), 32)
        v = parts_out[x, rows, :].astype(F32) + from_left[rows, :].astype(F32) + from_right[rows, :].astype(F32)
        v = v * lax.rsqrt(jnp.mean(v * v, axis=1, keepdims=True) + EPS)
        out[rows, :] = (mixed[rows, :] + 0.5 * v * params[2:3, :]).astype(BF16)
        return 0

    lax.fori_loop(0, OWN // 32, last, 0)


COPIES = 120


def layer(*operands):
    vm = pl.BlockSpec(memory_space=pltpu.VMEM)
    sm = pl.BlockSpec(memory_space=pltpu.SMEM)
    hbm = pl.BlockSpec(memory_space=pl.ANY)
    dma = pltpu.SemaphoreType.DMA
    chan = pltpu.VMEM((ROWS, 256), BF16)
    return pl.pallas_call(
        layer_kernel,
        name="layer",
        out_shape=jax.ShapeDtypeStruct((OWN, 2048), BF16),
        in_specs=[hbm] * 12 + [vm] * 2 + [sm] * 2,
        out_specs=vm,
        scratch_shapes=[chan] * 10 + [
            pltpu.VMEM((8, ROWS), F32), pltpu.VMEM((8, ROWS), F32),
            pltpu.VMEM((ROWS, 128), F32), pltpu.VMEM((ROWS, 128), F32),
            pltpu.VMEM((NBLK, 128, 512), F32), pltpu.VMEM((NBLK, 8, 512), F32),
            pltpu.VMEM((ROWS, 512), F32),
            pltpu.VMEM((4, 16, 256), BF16),
            pltpu.VMEM((128, 512), F32), pltpu.VMEM((8, 512), F32),
            pltpu.VMEM((128, 512), BF16), pltpu.VMEM((128, 512), BF16), pltpu.VMEM((8, 512), F32),
            pltpu.VMEM((64, 512), BF16), pltpu.VMEM((8, 512), F32),
            pltpu.VMEM((3, 64, 512), BF16), pltpu.VMEM((3, 8, 512), F32),
            pltpu.VMEM((64, 512), BF16), pltpu.VMEM((8, 512), F32),
            pltpu.VMEM((3, 64, 512), BF16), pltpu.VMEM((3, 8, 512), F32),
            pltpu.VMEM((64, 512), F32), pltpu.VMEM((128, 512), F32),
            pltpu.VMEM((ROWS, 512), BF16), pltpu.VMEM((4, OWN, 512), BF16),
            pltpu.VMEM((4, 4, 2, 64, 3 * FF_DEV), BF16), pltpu.VMEM((4, 512, 2048), BF16),
            pltpu.VMEM((OWN, 2048), BF16), pltpu.VMEM((OWN, 2048), F32),
            pltpu.VMEM((4, OWN, 2048), BF16), pltpu.VMEM((OWN, FF_DEV), BF16),
            pltpu.VMEM((4, OWN, 2048), BF16),
            pltpu.VMEM((2, 128, 2048), BF16), pltpu.VMEM((2, 128, 2048), BF16),
            pltpu.VMEM((OWN, 2048), BF16), pltpu.VMEM((OWN, 2048), BF16),
            dma((COPIES,)), dma((COPIES,)), dma((12,)),
        ],
        compiler_params=pltpu.CompilerParams(
            collective_id=0, has_side_effects=True, vmem_limit_bytes=67043328
        ),
        cost_estimate=pl.CostEstimate(flops=22_000_000_000, bytes_accessed=30_000_000, transcendentals=0),
    )(*operands)


def local(
    residual, small_heads, large_heads, state_keys, state_queries, small_gate, large_gate,
    small_step, large_step, small_taps, large_taps, key_taps, query_taps, small_decay, large_decay,
    small_gain, large_gain, small_out, large_out, mixer_gain, ffn_in_gain,
    gate_proj, up_proj, down_proj, ffn_out_gain,
):
    taps = jnp.concatenate([small_taps, large_taps, key_taps.reshape(4, 256), query_taps.reshape(4, 256)], axis=1)
    head_gain = jnp.concatenate([small_gain, large_gain]).reshape(1, 512)
    params = jnp.concatenate(
        [
            jnp.stack([mixer_gain, ffn_in_gain, ffn_out_gain]),
            jnp.pad(taps, ((0, 0), (0, 1024))),
            jnp.pad(head_gain, ((0, 0), (0, 1536))),
        ]
    ).astype(F32)
    steps = jnp.concatenate([small_step.T, large_step.T, jnp.zeros((2, ROWS), F32)])
    return layer(
        residual, small_heads, large_heads, state_keys.reshape(ROWS, 256), state_queries.reshape(ROWS, 256),
        small_gate, large_gate, gate_proj, up_proj, down_proj, small_out, large_out,
        steps, params, small_decay, large_decay,
    )


def solution(mesh):
    torus = Mesh(mesh.devices.reshape(4, 4, 2, mesh.shape["tp"]), ("sp_0", "sp_1", "sp_2", "tp"))
    in_specs = (
        P(SP, None), P(SP, "tp"), P(SP, "tp"), P(SP, "tp", None), P(SP, "tp", None),
        P(SP, "tp"), P(SP, "tp"), P(SP, "tp"), P(SP, "tp"),
        P(None, "tp"), P(None, "tp"), P(None, "tp", None), P(None, "tp", None),
        P("tp"), P("tp"), P("tp"), P("tp"), P("tp", None), P("tp", None),
        P(), P(), P(SP, "tp"), P(SP, "tp"), P(SP, "tp"), P(),
    )
    return jax.shard_map(local, mesh=torus, in_specs=in_specs, out_specs=P(SP_TP, None), check_vma=False)
```

```python
import functools

import jax
import jax.numpy as jnp
from jax import lax
from jax.experimental import pallas as pl
from jax.experimental.pallas import tpu as pltpu
from jax.sharding import Mesh
from jax.sharding import PartitionSpec as P

BLOCK = 128
ROWS = 1024
NBLK = ROWS // BLOCK
SP = ("sp_0", "sp_1", "sp_2")
SP_TP = ("sp_0", "sp_1", "sp_2", "tp")
EPS = 1e-06
MESH = pl.DeviceIdType.MESH
F32 = jnp.float32
BF16 = jnp.bfloat16


def dot(a, b, contract=((1,), (0,)), precision=None):
    return lax.dot_general(
        a, b, (contract, ((), ())), preferred_element_type=F32, precision=precision
    )


def silu(v):
    return v * jax.nn.sigmoid(v)


def spread(m):
    rows = m.shape[0]
    low = lax.broadcasted_iota(jnp.int32, (rows, 128), 1) < 64
    cols = [jnp.broadcast_to(m[:, h : h + 1], (rows, 128)) for h in range(6)]
    return (
        jnp.where(low, cols[0], cols[1]),
        jnp.where(low, cols[2], cols[3]),
        cols[4],
        cols[5],
    )


def block_rows(b):
    return pl.ds(pl.multiple_of(b * BLOCK, BLOCK), BLOCK)


OWN = 256
STEPS = 4
PART = OWN // STEPS
FF_DEV = 1408
UP_COLS = pl.ds(0, 2 * FF_DEV)
DOWN_COLS = pl.ds(2 * FF_DEV, FF_DEV)


class Net:
    def __init__(self, send_sems, recv_sems):
        self.send_sems, self.recv_sems, self.used = send_sems, recv_sems, 0

    def copy(self, src, dst, peer):
        i = self.used
        self.used += 1
        return pltpu.make_async_remote_copy(
            src_ref=src, dst_ref=dst, send_sem=self.send_sems.at[i], recv_sem=self.recv_sems.at[i],
            device_id=peer, device_id_type=MESH,
        )


class Ring:
    def __init__(self, net, axis, at, view, pieces=(None,)):
        self.net, self.at, self.view = net, at, view
        self.before, self.after = lax.rem(at + 3, 4), lax.rem(at + 1, 4)
        self.up, self.down = {axis: self.after}, {axis: self.before}
        self.ups = [net.copy(view(at, p), view(at, p), self.up) for p in pieces]
        self.downs = [net.copy(view(at, p), view(at, p), self.down) for p in pieces[::-1]]
        self.forwards = []

    def start(self):
        for pair in zip(self.ups, self.downs):
            for copy in pair:
                copy.start()

    def forward(self):
        self.ups[0].wait_recv()
        here = self.view(self.before, 0)
        self.forwards.append(self.net.copy(here, here, self.up))
        self.forwards[-1].start()
        self.downs[0].wait_recv()
        here = self.view(self.after, 1)
        self.forwards.append(self.net.copy(here, here, self.down))
        self.forwards[-1].start()

    def neighbours(self):
        for copy in self.ups[1:] + self.downs[1:]:
            copy.wait_recv()

    def finish(self):
        for copy in self.forwards:
            copy.wait_recv()
        for copy in self.ups + self.downs + self.forwards:
            copy.wait_send()


def layer_kernel(
    residual, sh_in, lh_in, ks_in, qs_in, sg_in, lg_in, gate_in, up_in, down_in, so_in, lo_in,
    small_steps, large_steps, params, sdec, ldec,
    out,
    xs, xl, kc, qc, sg, lg,
    dtt, ct, ccol, dcol, hloc, eoff, inside,
    halo, mine, mine_tot, sbuf, sib, sib_tot, ysend, ytot_send, yrec, ytot, zsend, ztot_send, zrec, ztot, esend, ebuf,
    chans, weights, projs, res, mix, mixed, rows_in, hidden, parts_out, relay, relay_sum, from_left, from_right,
    send_sems, recv_sems, load_sems,
):
    z = lax.axis_index("sp_0")
    y = lax.axis_index("sp_1")
    c = lax.axis_index("sp_2")
    x = lax.axis_index("tp")
    sp = (z * 4 + y) * 2 + c
    nxt = lax.rem(sp + 1, 32)
    prv = lax.rem(sp + 31, 32)
    left, right, across = lax.rem(x + 3, 4), lax.rem(x + 1, 4), lax.rem(x + 2, 4)
    net = Net(send_sems, recv_sems)

    def at_sp(i):
        return {"sp_0": i // 8, "sp_1": lax.rem(i // 2, 4), "sp_2": lax.rem(i, 2)}

    loads = [
        pltpu.make_async_copy(src, dst, load_sems.at[i])
        for i, (src, dst) in enumerate((
            (sh_in, xs), (lh_in, xl), (ks_in, kc), (qs_in, qc),
            (gate_in, weights.at[z, y, c, :, pl.ds(0, FF_DEV)]),
            (up_in, weights.at[z, y, c, :, pl.ds(FF_DEV, FF_DEV)]),
            (down_in, weights.at[z, y, c, :, DOWN_COLS]),
            (so_in, projs.at[x, pl.ds(0, 256)]),
            (lo_in, projs.at[x, pl.ds(256, 256)]),
            (sg_in, sg), (lg_in, lg),
            (residual, res),
        ))
    ]
    for copy in loads:
        copy.start()
    loads_in, loads_own, loads_gate = loads[:4], loads[4:9], loads[9:]

    ypeers = [{"sp_1": lax.rem(y + d, 4)} for d in (1, 2, 3)]
    zpeers = [{"sp_0": lax.rem(z + d, 4)} for d in (1, 2, 3)]
    xpeers = [{"tp": i} for i in (across, right, left)]
    sibling = {"sp_2": 1 - c}
    barrier = pltpu.get_barrier_semaphore()
    peers = [at_sp(nxt), at_sp(prv), sibling] + ypeers + zpeers + xpeers
    for peer in peers:
        pl.semaphore_signal(barrier, inc=1, device_id=peer, device_id_type=MESH)
    pl.semaphore_wait(barrier, len(peers))

    halo_copies = [
        net.copy(src.at[pl.ds(ROWS - 16, 16)], halo.at[i], at_sp(nxt)) for i, src in enumerate((sh_in, lh_in, ks_in, qs_in))
    ]
    for copy in halo_copies:
        copy.start()

    def span(part, size):
        return pl.ds(0, size) if part is None else pl.ds(part * (size // 2), size // 2)

    def y_first(cols):
        return lambda i, p=None: weights.at[z, i, c, span(p, 32), cols]

    def z_first(cols):
        return lambda i, p=None: weights.at[i, y, c, pl.ds(32, 32) if p is None else pl.ds(32 + 16 * p, 16), cols]

    def z_view(cols):
        return lambda i, p=None: weights.at[i, span(p, 4), c, pl.ds(0, 32), cols]

    def y_view(cols):
        return lambda i, p=None: weights.at[span(p, 4), i, c, pl.ds(32, 32), cols]

    def proj_view(i, p=None):
        size = 256 if p is None else 128
        return projs.at[i, pl.ds(pl.multiple_of(c * 256 + (0 if p is None else p * 128), 128), size)]

    for copy in loads_own:
        copy.wait()
    first_rings = [
        Ring(net, axis, at, view(cols))
        for cols in (UP_COLS, DOWN_COLS)
        for axis, at, view in (("sp_1", y, y_first), ("sp_0", z, z_first))
    ]
    proj = Ring(net, "tp", x, proj_view)
    for ring in first_rings + [proj]:
        ring.start()

    dtt[...] = jnp.zeros_like(dtt)
    dtt[0:4, :] = jax.nn.softplus(small_steps[...])
    dtt[4:6, :] = jax.nn.softplus(large_steps[...])
    ct[...] = jnp.zeros_like(ct)
    for h in range(6):
        d = sdec[h] if h < 4 else ldec[h - 4]
        rate = jnp.exp(jnp.full((1, ROWS), d, F32))
        ct[h : h + 1, :] = -dtt[h : h + 1, :] * rate
    tr = lax.broadcasted_iota(jnp.int32, (BLOCK, BLOCK), 0)
    tc = lax.broadcasted_iota(jnp.int32, (BLOCK, BLOCK), 1)
    upper = (tr <= tc).astype(F32)
    low = tc < 64
    low_part = low[:PART]
    causal = tc <= tr

    def sums(b, _):
        rows = block_rows(b)
        cum = dot(ct[:, rows], upper, precision=lax.Precision.HIGHEST)
        ct[:, rows] = cum
        pad = jnp.zeros((BLOCK - 8, BLOCK), F32)
        ccol[rows, :] = jnp.concatenate([cum, pad], axis=0).T
        dcol[rows, :] = jnp.concatenate([dtt[:, rows], pad], axis=0).T
        return 0

    lax.fori_loop(0, NBLK, sums, 0)

    taps = [params[3:7, i * 256 : i * 256 + 256] for i in range(4)]
    keep = jnp.where(sp == 0, 0.0, 1.0)

    def conv_of(ext, tap):
        acc = jnp.zeros((BLOCK, 256), F32)
        for k in range(4):
            shifted = ext if k == 3 else pltpu.roll(ext, 3 - k, 0)
            acc = acc + tap[k : k + 1, :] * shifted[16:, :]
        return silu(acc).astype(BF16)

    def convolve(which):
        refs = (xs, xl, kc, qc)

        def conv_block(i, _):
            b = NBLK - 1 - i
            start = pl.multiple_of(b * BLOCK - 16, 16)
            for k in which:
                refs[k][block_rows(b), :] = conv_of(refs[k][pl.ds(start, BLOCK + 16), :].astype(F32), taps[k])
            return 0

        lax.fori_loop(0, NBLK - 1, conv_block, 0)
        for k in which:
            halo_copies[k].wait()
        for k in which:
            ext = jnp.concatenate([halo[k].astype(F32) * keep, refs[k][0:BLOCK, :].astype(F32)], axis=0)
            refs[k][0:BLOCK, :] = conv_of(ext, taps[k])

    for copy in loads_in:
        copy.wait()
    convolve((0, 1, 2))
    for ring in first_rings:
        ring.forward()

    mine[...] = jnp.zeros_like(mine)
    mine_tot[...] = jnp.zeros_like(mine_tot)

    def states(b, _):
        rows = block_rows(b)
        cb = ccol[rows, :]
        last = cb[BLOCK - 1 : BLOCK, :]
        scale = spread(dcol[rows, :] * jnp.exp(last - cb))
        xsb = xs[rows, :].astype(F32)
        xlb = xl[rows, :].astype(F32)
        us = jnp.concatenate([xsb[:, :128] * scale[0], xsb[:, 128:] * scale[1]], axis=1)
        ul = jnp.concatenate([xlb[:, :128] * scale[2], xlb[:, 128:] * scale[3]], axis=1)
        fresh_s = dot(kc[rows, 0:128], us.astype(BF16), ((0,), (0,)))
        fresh_l = dot(kc[rows, 128:256], ul.astype(BF16), ((0,), (0,)))
        state = mine[...]
        tot = mine_tot[...]
        hloc[b] = state
        eoff[b] = jnp.exp(tot)
        step = jnp.concatenate(spread(jnp.broadcast_to(last, (8, 128))), axis=1)
        mine[...] = state * jnp.exp(step)[0:1, :] + jnp.concatenate([fresh_s, fresh_l], axis=1)
        mine_tot[...] = tot + step
        return 0

    lax.fori_loop(0, NBLK, states, 0)

    sbuf[...] = mine[...].astype(BF16)
    r1 = [net.copy(sbuf, sib, sibling), net.copy(mine_tot, sib_tot, sibling)]
    for copy in r1:
        copy.start()
    convolve((3,))

    def intra(b, _):
        rows = block_rows(b)
        cb = ccol[rows, :]
        parts = []
        for g, vals in ((0, xs), (1, xl)):
            lanes = slice(g * 128, g * 128 + 128)
            scores = dot(qc[rows, lanes], kc[rows, lanes], ((1,), (1,)))
            found = []
            for h in range(4) if g == 0 else range(4, 6):
                gap = jnp.broadcast_to(cb[:, h : h + 1], (BLOCK, BLOCK)) - ct[h : h + 1, rows]
                decay = jnp.exp(jnp.where(causal, gap, -1e30))
                w = (scores * decay * dtt[h : h + 1, rows]).astype(BF16)
                at = (h // 2 if g == 0 else h - 4) * 128
                found.append(dot(w, vals[rows, at : at + 128]))
            if g == 0:
                parts += [jnp.where(low, found[0], found[1]), jnp.where(low, found[2], found[3])]
            else:
                parts += found
        inside[rows, :] = jnp.concatenate(parts, axis=1)
        return 0

    for copy in r1:
        copy.wait()

    half = pl.ds(pl.multiple_of(c * 64, 64), 64)
    my_half = mine[half, :]
    sib_half = sib[half, :].astype(F32)
    first = c == 0
    t_me = mine_tot[...]
    t_sib = sib_tot[...]
    early = jnp.where(first, my_half, sib_half)
    late = jnp.where(first, sib_half, my_half)
    t_late = jnp.where(first, t_sib, t_me)
    chip = early * jnp.exp(t_late)[0:1, :] + late
    chip_tot = t_me + t_sib
    ysend[...] = chip.astype(BF16)
    ytot_send[...] = chip_tot

    def peer_copies(send, tot_send, rec, tot_rec, peers_):
        made = []
        for i, peer in enumerate(peers_):
            made += [net.copy(send, rec.at[i], peer), net.copy(tot_send, tot_rec.at[i], peer)]
        return made

    r2 = peer_copies(ysend, ytot_send, yrec, ytot, ypeers)
    for copy in r2:
        copy.start()
    lax.fori_loop(0, 4, intra, 0)
    for copy in r2:
        copy.wait()

    def before_of(pos, rec, tot_rec):
        e = jnp.zeros((64, 512), F32)
        t = jnp.zeros((8, 512), F32)
        for d in (3, 2, 1):
            valid = d <= pos
            e = jnp.where(valid, e * jnp.exp(tot_rec[d - 1])[0:1, :] + rec[d - 1].astype(F32), e)
            t = jnp.where(valid, t + tot_rec[d - 1], t)
        return e, t

    ey, ty = before_of(y, yrec, ytot)
    plane = ey * jnp.exp(chip_tot)[0:1, :] + chip
    plane_tot = ty + chip_tot
    for e in (1, 2, 3):
        valid = y + e <= 3
        plane = jnp.where(valid, plane * jnp.exp(ytot[3 - e])[0:1, :] + yrec[3 - e].astype(F32), plane)
        plane_tot = jnp.where(valid, plane_tot + ytot[3 - e], plane_tot)
    zsend[...] = plane.astype(BF16)
    ztot_send[...] = plane_tot
    r3 = peer_copies(zsend, ztot_send, zrec, ztot, zpeers)
    for copy in r3:
        copy.start()
    for ring in first_rings:
        ring.finish()
    second_rings = [
        Ring(net, axis, at, view(cols))
        for cols in (UP_COLS, DOWN_COLS)
        for axis, at, view in (("sp_0", z, z_view), ("sp_1", y, y_view))
    ]
    for ring in second_rings:
        ring.start()
    shared = [
        [net.copy(z_view(cols)(z), z_view(cols)(z), sibling), net.copy(y_view(cols)(y), y_view(cols)(y), sibling)]
        for cols in (UP_COLS, DOWN_COLS)
    ]
    for group in shared:
        for copy in group:
            copy.start()
    lax.fori_loop(4, NBLK, intra, 0)
    for copy in r3:
        copy.wait()
    ez, _ = before_of(z, zrec, ztot)
    entering = ez * jnp.exp(ty)[0:1, :] + ey
    esend[...] = entering
    r4 = net.copy(esend, ebuf.at[half], sibling)
    r4.start()
    r4.wait()
    own = esend[...]
    enter_rows = []
    for i in range(2):
        arrived = ebuf[i * 64 : i * 64 + 64, :]
        enter_rows.append(jnp.where(c == i, own, arrived))
    enter = jnp.concatenate(enter_rows, axis=0)
    second = enter * jnp.exp(t_sib)[0:1, :] + sib[...].astype(F32)
    mine[...] = jnp.where(first, enter, second)

    proj.forward()
    shared_proj = [net.copy(proj_view(i), proj_view(i), sibling) for i in (x, left, right)]
    for copy in shared_proj:
        copy.start()
    for copy in loads_gate:
        copy.wait()

    def share(copies):
        for copy in copies:
            copy.start()
        return copies

    def finish(s, j):
        b = 2 * j + s // 2
        rows = pl.ds(pl.multiple_of(j * OWN + s * PART, PART), PART)
        state = (hloc[b] + eoff[b][0:1, :] * mine[...]).astype(BF16)
        grow = spread(jnp.exp(ccol[rows, :]))
        carried = [dot(qc[rows, g * 128 : g * 128 + 128], state[:, g * 256 : g * 256 + 256]) for g in (0, 1)]
        for i in range(4):
            g, at = i // 2, (i % 2) * 128
            gate_ref = sg if g == 0 else lg
            v = inside[rows, i * 128 : i * 128 + 128] + carried[g][:, at : at + 128] * grow[i]
            v = v * silu(gate_ref[rows, at : at + 128].astype(F32))
            sq = v * v
            if g == 0:
                s0 = jnp.sum(jnp.where(low_part, sq, 0.0), axis=1, keepdims=True)
                s1 = jnp.sum(jnp.where(low_part, 0.0, sq), axis=1, keepdims=True)
                inv = jnp.where(low_part, lax.rsqrt(s0 / 64 + EPS), lax.rsqrt(s1 / 64 + EPS))
            else:
                inv = lax.rsqrt(jnp.sum(sq, axis=1, keepdims=True) / 128 + EPS)
            v = v * inv * params[7:8, i * 128 : i * 128 + 128]
            chans[x, s, pl.ds(pl.multiple_of(j * PART, PART), PART), i * 128 : i * 128 + 128] = v.astype(BF16)
        return 0


    gathers = [
        Ring(net, "tp", x, lambda i, p, s=s: chans.at[i, s, pl.ds(p * 128, 128)], (0, 1)) for s in range(STEPS)
    ]

    def finish_step(s):
        lax.fori_loop(0, 4, lambda j, _: finish(s, j), 0)

    def share_arrived(k, which):
        zr, yr = second_rings[2 * k], second_rings[2 * k + 1]
        cols = (UP_COLS, DOWN_COLS)[k]
        zs = [zr.before, zr.after] if which == 0 else [lax.rem(z + 2, 4)]
        ys = [yr.before, yr.after] if which == 0 else [lax.rem(y + 2, 4)]
        return share(
            [net.copy(z_view(cols)(i), z_view(cols)(i), sibling) for i in zs]
            + [net.copy(y_view(cols)(i), y_view(cols)(i), sibling) for i in ys]
        )

    def forward_weights(k):
        second_rings[2 * k].forward()
        second_rings[2 * k + 1].forward()
        shared[k] += share_arrived(k, 0)

    def wait_weights(k):
        second_rings[2 * k].finish()
        second_rings[2 * k + 1].finish()
        for copy in shared[k] + share_arrived(k, 1):
            copy.wait()

    def project(s):
        def tile(n, _):
            cols = pl.ds(pl.multiple_of(n * 256, 256), 256)
            acc = dot(chans[0, s], projs[0, :, cols])
            for i in range(1, 4):
                acc = acc + dot(chans[i, s], projs[i, :, cols])
            mix[:, cols] = acc
            return 0

        lax.fori_loop(0, 8, tile, 0)

        def norms(r, _):
            rows = pl.ds(pl.multiple_of(r * 32, 32), 32)
            v = mix[rows, :]
            v = v * lax.rsqrt(jnp.mean(v * v, axis=1, keepdims=True) + EPS)
            at = (r // 2) * OWN + lax.rem(r, 2) * 32 + s * PART
            v = res[pl.ds(pl.multiple_of(at, 32), 32), :].astype(F32) + v * params[0:1, :]
            mix[rows, :] = v
            v = v * lax.rsqrt(jnp.mean(v * v, axis=1, keepdims=True) + EPS)
            rows_in[rows, :] = (v * params[1:2, :]).astype(BF16)
            return 0

        lax.fori_loop(0, OWN // 32, norms, 0)
        mixed[s * PART : s * PART + PART, :] = mix[pl.ds(pl.multiple_of(x * PART, PART), PART), :]

    def gate_up():
        def tile(n, _):
            g_cols = pl.ds(pl.multiple_of(n * 128, 128), 128)
            u_cols = pl.ds(pl.multiple_of(FF_DEV + n * 128, 128), 128)
            w = jnp.concatenate(
                [weights[:, :, :, :, g_cols].reshape(2048, 128), weights[:, :, :, :, u_cols].reshape(2048, 128)], axis=1
            )
            both = dot(rows_in[...], w)
            hidden[:, g_cols] = (silu(both[:, :128]) * both[:, 128:]).astype(BF16)
            return 0

        lax.fori_loop(0, FF_DEV // 128, tile, 0)

    def down(s):
        def tile(n, _):
            w = weights[n // 2, pl.ds(lax.rem(n, 2) * 2, 2), :, :, DOWN_COLS].reshape(256, FF_DEV)
            part = dot(hidden[...], w, ((1,), (1,))).astype(BF16).reshape(4, PART, 256)
            parts_out[:, s * PART : s * PART + PART, pl.ds(pl.multiple_of(n * 256, 256), 256)] = part
            return 0

        lax.fori_loop(0, 8, tile, 0)

    to_left, to_right = {"tp": left}, {"tp": right}
    relays, sends = [None] * STEPS, [None] * STEPS

    def halves(s):
        return pl.ds(s * PART, PART // 2), pl.ds(s * PART + PART // 2, PART // 2)

    def send_parts(s):
        h0, h1 = halves(s)
        kept = pl.ds(s * (PART // 2), PART // 2)
        relays[s] = share([
            net.copy(parts_out.at[across, h0], relay.at[0, kept], to_right),
            net.copy(parts_out.at[across, h1], relay.at[1, kept], to_left),
        ])
        sends[s] = share([
            net.copy(parts_out.at[left, h0], from_right.at[h0], to_left),
            net.copy(parts_out.at[right, h1], from_left.at[h1], to_right),
        ])

    def send_sums(s):
        h0, h1 = halves(s)
        kept = pl.ds(s * (PART // 2), PART // 2)
        for k, (peer, rows, dst, to) in enumerate(((right, h0, from_left, to_right), (left, h1, from_right, to_left))):
            relays[s][k].wait_recv()
            relay_sum[k, kept] = (parts_out[peer, rows, :].astype(F32) + relay[k, kept].astype(F32)).astype(BF16)
            sends[s] += share([net.copy(relay_sum.at[k, kept], dst.at[rows], to)])

    def last(s):
        for copy in relays[s]:
            copy.wait_send()
        for copy in sends[s]:
            copy.wait()

        def rows_of(r, _):
            rows = pl.ds(pl.multiple_of(s * PART + r * 32, 32), 32)
            v = parts_out[x, rows, :].astype(F32) + from_left[rows, :].astype(F32) + from_right[rows, :].astype(F32)
            v = v * lax.rsqrt(jnp.mean(v * v, axis=1, keepdims=True) + EPS)
            out[rows, :] = (mixed[rows, :] + 0.5 * v * params[2:3, :]).astype(BF16)
            return 0

        lax.fori_loop(0, PART // 32, rows_of, 0)

    finish_step(0)
    gathers[0].start()
    finish_step(1)
    gathers[1].start()
    finish_step(2)
    finish_step(3)
    forward_weights(0)
    gathers[0].forward()
    gathers[2].start()
    proj.finish()
    shared_proj += share([net.copy(proj_view(across), proj_view(across), sibling)])
    gathers[1].forward()
    gathers[3].start()
    forward_weights(1)
    for copy in shared_proj:
        copy.wait()
    for s in range(STEPS):
        gathers[s].neighbours()
        gathers[s].finish()
        project(s)
        if s == 0:
            gathers[2].forward()
            wait_weights(0)
        gate_up()
        if s == 0:
            gathers[3].forward()
            wait_weights(1)
        else:
            send_sums(s - 1)
        down(s)
        send_parts(s)
    for s in range(STEPS - 1):
        last(s)
    send_sums(STEPS - 1)
    last(STEPS - 1)


COPIES = 160


def layer(*operands):
    vm = pl.BlockSpec(memory_space=pltpu.VMEM)
    sm = pl.BlockSpec(memory_space=pltpu.SMEM)
    hbm = pl.BlockSpec(memory_space=pl.ANY)
    dma = pltpu.SemaphoreType.DMA
    chan = pltpu.VMEM((ROWS, 256), BF16)
    return pl.pallas_call(
        layer_kernel,
        name="layer",
        out_shape=jax.ShapeDtypeStruct((OWN, 2048), BF16),
        in_specs=[hbm] * 12 + [vm] * 3 + [sm] * 2,
        out_specs=vm,
        scratch_shapes=[chan] * 6 + [
            pltpu.VMEM((8, ROWS), F32), pltpu.VMEM((8, ROWS), F32),
            pltpu.VMEM((ROWS, 128), F32), pltpu.VMEM((ROWS, 128), F32),
            pltpu.VMEM((NBLK, 128, 512), F32), pltpu.VMEM((NBLK, 8, 512), F32),
            pltpu.VMEM((ROWS, 512), F32),
            pltpu.VMEM((4, 16, 256), BF16),
            pltpu.VMEM((128, 512), F32), pltpu.VMEM((8, 512), F32),
            pltpu.VMEM((128, 512), BF16), pltpu.VMEM((128, 512), BF16), pltpu.VMEM((8, 512), F32),
            pltpu.VMEM((64, 512), BF16), pltpu.VMEM((8, 512), F32),
            pltpu.VMEM((3, 64, 512), BF16), pltpu.VMEM((3, 8, 512), F32),
            pltpu.VMEM((64, 512), BF16), pltpu.VMEM((8, 512), F32),
            pltpu.VMEM((3, 64, 512), BF16), pltpu.VMEM((3, 8, 512), F32),
            pltpu.VMEM((64, 512), F32), pltpu.VMEM((128, 512), F32),
            pltpu.VMEM((4, STEPS, OWN, 512), BF16),
            pltpu.VMEM((4, 4, 2, 64, 3 * FF_DEV), BF16), pltpu.VMEM((4, 512, 2048), BF16),
            pltpu.VMEM((ROWS, 2048), BF16), pltpu.VMEM((OWN, 2048), F32), pltpu.VMEM((OWN, 2048), F32),
            pltpu.VMEM((OWN, 2048), BF16), pltpu.VMEM((OWN, FF_DEV), BF16),
            pltpu.VMEM((4, OWN, 2048), BF16),
            pltpu.VMEM((2, 128, 2048), BF16), pltpu.VMEM((2, 128, 2048), BF16),
            pltpu.VMEM((OWN, 2048), BF16), pltpu.VMEM((OWN, 2048), BF16),
            dma((COPIES,)), dma((COPIES,)), dma((12,)),
        ],
        compiler_params=pltpu.CompilerParams(
            collective_id=0, has_side_effects=True, vmem_limit_bytes=67043328
        ),
        cost_estimate=pl.CostEstimate(flops=22_000_000_000, bytes_accessed=30_000_000, transcendentals=0),
    )(*operands)


def local(
    residual, small_heads, large_heads, state_keys, state_queries, small_gate, large_gate,
    small_step, large_step, small_taps, large_taps, key_taps, query_taps, small_decay, large_decay,
    small_gain, large_gain, small_out, large_out, mixer_gain, ffn_in_gain,
    gate_proj, up_proj, down_proj, ffn_out_gain,
):
    def placed(array, row, lane):
        array = array.astype(F32)
        return jnp.pad(array, ((row, 8 - row - array.shape[0]), (lane, 2048 - lane - array.shape[1])))

    params = placed(mixer_gain[None], 0, 0) + placed(ffn_in_gain[None], 1, 0) + placed(ffn_out_gain[None], 2, 0)
    taps = (small_taps, large_taps, key_taps.reshape(4, 256), query_taps.reshape(4, 256))
    for i, tap in enumerate(taps):
        params = params + placed(tap, 3, 256 * i)
    params = params + placed(small_gain[None], 7, 0) + placed(large_gain[None], 7, 256)
    return layer(
        residual, small_heads, large_heads, state_keys.reshape(ROWS, 256), state_queries.reshape(ROWS, 256),
        small_gate, large_gate, gate_proj, up_proj, down_proj, small_out, large_out,
        small_step.T, large_step.T, params, small_decay, large_decay,
    )


def solution(mesh):
    torus = Mesh(mesh.devices.reshape(4, 4, 2, mesh.shape["tp"]), ("sp_0", "sp_1", "sp_2", "tp"))
    in_specs = (
        P(SP, None), P(SP, "tp"), P(SP, "tp"), P(SP, "tp", None), P(SP, "tp", None),
        P(SP, "tp"), P(SP, "tp"), P(SP, "tp"), P(SP, "tp"),
        P(None, "tp"), P(None, "tp"), P(None, "tp", None), P(None, "tp", None),
        P("tp"), P("tp"), P("tp"), P("tp"), P("tp", None), P("tp", None),
        P(), P(), P(SP, "tp"), P(SP, "tp"), P(SP, "tp"), P(),
    )
    return jax.shard_map(local, mesh=torus, in_specs=in_specs, out_specs=P(SP_TP, None), check_vma=False)
```

```python
import functools

import jax
import jax.numpy as jnp
from jax import lax
from jax.experimental import pallas as pl
from jax.experimental.pallas import tpu as pltpu
from jax.sharding import Mesh
from jax.sharding import PartitionSpec as P

BLOCK = 128
ROWS = 1024
NBLK = ROWS // BLOCK
SP = ("sp_0", "sp_1", "sp_2")
SP_TP = ("sp_0", "sp_1", "sp_2", "tp")
EPS = 1e-06
MESH = pl.DeviceIdType.MESH
F32 = jnp.float32
BF16 = jnp.bfloat16


def dot(a, b, contract=((1,), (0,)), precision=None):
    return lax.dot_general(
        a, b, (contract, ((), ())), preferred_element_type=F32, precision=precision
    )


def silu(v):
    return v * jax.nn.sigmoid(v)


def spread(m):
    rows = m.shape[0]
    low = lax.broadcasted_iota(jnp.int32, (rows, 128), 1) < 64
    cols = [jnp.broadcast_to(m[:, h : h + 1], (rows, 128)) for h in range(6)]
    return (
        jnp.where(low, cols[0], cols[1]),
        jnp.where(low, cols[2], cols[3]),
        cols[4],
        cols[5],
    )


def block_rows(b):
    return pl.ds(pl.multiple_of(b * BLOCK, BLOCK), BLOCK)


OWN = 256
STEPS = 4
PART = OWN // STEPS
FF_DEV = 1408
UP_COLS = pl.ds(0, 2 * FF_DEV)
DOWN_COLS = pl.ds(2 * FF_DEV, FF_DEV)


class Net:
    def __init__(self, send_sems, recv_sems):
        self.send_sems, self.recv_sems, self.used = send_sems, recv_sems, 0

    def copy(self, src, dst, peer):
        i = self.used
        self.used += 1
        return pltpu.make_async_remote_copy(
            src_ref=src, dst_ref=dst, send_sem=self.send_sems.at[i], recv_sem=self.recv_sems.at[i],
            device_id=peer, device_id_type=MESH,
        )


class Ring:
    def __init__(self, net, axis, at, view, pieces=(None,)):
        self.net, self.at, self.view = net, at, view
        self.before, self.after = lax.rem(at + 3, 4), lax.rem(at + 1, 4)
        self.up, self.down = {axis: self.after}, {axis: self.before}
        self.ups = [net.copy(view(at, p), view(at, p), self.up) for p in pieces]
        self.downs = [net.copy(view(at, p), view(at, p), self.down) for p in pieces[::-1]]
        self.forwards = []

    def start(self):
        for pair in zip(self.ups, self.downs):
            for copy in pair:
                copy.start()

    def forward(self):
        self.ups[0].wait_recv()
        here = self.view(self.before, 0)
        self.forwards.append(self.net.copy(here, here, self.up))
        self.forwards[-1].start()
        self.downs[0].wait_recv()
        here = self.view(self.after, 1)
        self.forwards.append(self.net.copy(here, here, self.down))
        self.forwards[-1].start()

    def neighbours(self):
        for copy in self.ups[1:] + self.downs[1:]:
            copy.wait_recv()

    def finish(self):
        for copy in self.forwards:
            copy.wait_recv()
        for copy in self.ups + self.downs + self.forwards:
            copy.wait_send()


def layer_kernel(
    residual, sh_in, lh_in, ks_in, qs_in, sg_in, lg_in, gate_in, up_in, down_in, so_in, lo_in,
    small_steps, large_steps, mixer_gain, ffn_in_gain, ffn_out_gain, sgain, lgain, stap, ltap, ktap, qtap, sdec, ldec,
    out,
    xs, xl, kc, qc, sg, lg,
    dtt, ct, ccol, dcol, hloc, eoff, inside,
    halo, mine, mine_tot, sbuf, sib, sib_tot, ysend, ytot_send, yrec, ytot, zsend, ztot_send, zrec, ztot, esend, ebuf,
    chans, weights, projs, res, mix, mixed, rows_in, hidden, parts_out, relay, relay_sum, from_left, from_right,
    params, send_sems, recv_sems, load_sems,
):
    z = lax.axis_index("sp_0")
    y = lax.axis_index("sp_1")
    c = lax.axis_index("sp_2")
    x = lax.axis_index("tp")
    sp = (z * 4 + y) * 2 + c
    nxt = lax.rem(sp + 1, 32)
    prv = lax.rem(sp + 31, 32)
    left, right, across = lax.rem(x + 3, 4), lax.rem(x + 1, 4), lax.rem(x + 2, 4)
    net = Net(send_sems, recv_sems)

    def at_sp(i):
        return {"sp_0": i // 8, "sp_1": lax.rem(i // 2, 4), "sp_2": lax.rem(i, 2)}

    loads = [
        pltpu.make_async_copy(src, dst, load_sems.at[i])
        for i, (src, dst) in enumerate((
            (sh_in, xs), (lh_in, xl), (ks_in, kc), (qs_in, qc),
            (gate_in, weights.at[z, y, c, :, pl.ds(0, FF_DEV)]),
            (up_in, weights.at[z, y, c, :, pl.ds(FF_DEV, FF_DEV)]),
            (down_in, weights.at[z, y, c, :, DOWN_COLS]),
            (so_in, projs.at[x, pl.ds(0, 256)]),
            (lo_in, projs.at[x, pl.ds(256, 256)]),
            (sg_in, sg), (lg_in, lg),
            (residual, res),
        ))
    ]
    for copy in loads:
        copy.start()
    loads_in, loads_own, loads_gate = loads[:4], loads[4:9], loads[9:]

    ypeers = [{"sp_1": lax.rem(y + d, 4)} for d in (1, 2, 3)]
    zpeers = [{"sp_0": lax.rem(z + d, 4)} for d in (1, 2, 3)]
    xpeers = [{"tp": i} for i in (across, right, left)]
    sibling = {"sp_2": 1 - c}
    barrier = pltpu.get_barrier_semaphore()
    peers = [at_sp(nxt), at_sp(prv), sibling] + ypeers + zpeers + xpeers
    for peer in peers:
        pl.semaphore_signal(barrier, inc=1, device_id=peer, device_id_type=MESH)
    pl.semaphore_wait(barrier, len(peers))

    halo_copies = [
        net.copy(src.at[pl.ds(ROWS - 16, 16)], halo.at[i], at_sp(nxt)) for i, src in enumerate((sh_in, lh_in, ks_in, qs_in))
    ]
    for copy in halo_copies:
        copy.start()

    def span(part, size):
        return pl.ds(0, size) if part is None else pl.ds(part * (size // 2), size // 2)

    def y_first(cols):
        return lambda i, p=None: weights.at[z, i, c, span(p, 32), cols]

    def z_first(cols):
        return lambda i, p=None: weights.at[i, y, c, pl.ds(32, 32) if p is None else pl.ds(32 + 16 * p, 16), cols]

    def z_view(cols):
        return lambda i, p=None: weights.at[i, span(p, 4), c, pl.ds(0, 32), cols]

    def y_view(cols):
        return lambda i, p=None: weights.at[span(p, 4), i, c, pl.ds(32, 32), cols]

    def proj_view(i, p=None):
        size = 256 if p is None else 128
        return projs.at[i, pl.ds(pl.multiple_of(c * 256 + (0 if p is None else p * 128), 128), size)]

    for copy in loads_own:
        copy.wait()
    first_rings = [
        Ring(net, axis, at, view(cols))
        for cols in (UP_COLS, DOWN_COLS)
        for axis, at, view in (("sp_1", y, y_first), ("sp_0", z, z_first))
    ]
    proj = Ring(net, "tp", x, proj_view)
    for ring in first_rings + [proj]:
        ring.start()

    for i, gain in enumerate((mixer_gain, ffn_in_gain, ffn_out_gain)):
        params[i : i + 1, :] = gain[...].astype(F32).reshape(1, 2048)
    for i, gain in enumerate((sgain, lgain)):
        params[7:8, i * 256 : i * 256 + 256] = gain[...].astype(F32).reshape(1, 256)
    for i, tap in enumerate((stap, ltap)):
        params[3:7, i * 256 : i * 256 + 256] = tap[...].astype(F32)
    for i, tap in enumerate((ktap, qtap)):
        for g in (0, 1):
            at = 512 + i * 256 + g * 128
            params[3:7, at : at + 128] = tap[:, g, :].astype(F32)

    dtt[...] = jnp.zeros_like(dtt)
    dtt[0:4, :] = jax.nn.softplus(small_steps[...])
    dtt[4:6, :] = jax.nn.softplus(large_steps[...])
    ct[...] = jnp.zeros_like(ct)
    for h in range(6):
        d = sdec[h] if h < 4 else ldec[h - 4]
        rate = jnp.exp(jnp.full((1, ROWS), d, F32))
        ct[h : h + 1, :] = -dtt[h : h + 1, :] * rate
    tr = lax.broadcasted_iota(jnp.int32, (BLOCK, BLOCK), 0)
    tc = lax.broadcasted_iota(jnp.int32, (BLOCK, BLOCK), 1)
    upper = (tr <= tc).astype(F32)
    low = tc < 64
    low_part = low[:PART]
    causal = tc <= tr

    def sums(b, _):
        rows = block_rows(b)
        cum = dot(ct[:, rows], upper, precision=lax.Precision.HIGHEST)
        ct[:, rows] = cum
        pad = jnp.zeros((BLOCK - 8, BLOCK), F32)
        ccol[rows, :] = jnp.concatenate([cum, pad], axis=0).T
        dcol[rows, :] = jnp.concatenate([dtt[:, rows], pad], axis=0).T
        return 0

    lax.fori_loop(0, NBLK, sums, 0, unroll=True)

    taps = [params[3:7, i * 256 : i * 256 + 256] for i in range(4)]
    keep = jnp.where(sp == 0, 0.0, 1.0)

    def conv_of(ext, tap):
        acc = jnp.zeros((BLOCK, 256), F32)
        for k in range(4):
            shifted = ext if k == 3 else pltpu.roll(ext, 3 - k, 0)
            acc = acc + tap[k : k + 1, :] * shifted[16:, :]
        return silu(acc).astype(BF16)

    def convolve(which):
        refs = (xs, xl, kc, qc)

        def conv_block(i, _):
            b = NBLK - 1 - i
            start = pl.multiple_of(b * BLOCK - 16, 16)
            for k in which:
                refs[k][block_rows(b), :] = conv_of(refs[k][pl.ds(start, BLOCK + 16), :].astype(F32), taps[k])
            return 0

        lax.fori_loop(0, NBLK - 1, conv_block, 0)
        for k in which:
            halo_copies[k].wait()
        for k in which:
            ext = jnp.concatenate([halo[k].astype(F32) * keep, refs[k][0:BLOCK, :].astype(F32)], axis=0)
            refs[k][0:BLOCK, :] = conv_of(ext, taps[k])

    for copy in loads_in:
        copy.wait()
    convolve((0, 1, 2))
    for ring in first_rings:
        ring.forward()

    mine[...] = jnp.zeros_like(mine)
    mine_tot[...] = jnp.zeros_like(mine_tot)

    def states(b, _):
        rows = block_rows(b)
        cb = ccol[rows, :]
        last = cb[BLOCK - 1 : BLOCK, :]
        scale = spread(dcol[rows, :] * jnp.exp(last - cb))
        xsb = xs[rows, :].astype(F32)
        xlb = xl[rows, :].astype(F32)
        us = jnp.concatenate([xsb[:, :128] * scale[0], xsb[:, 128:] * scale[1]], axis=1)
        ul = jnp.concatenate([xlb[:, :128] * scale[2], xlb[:, 128:] * scale[3]], axis=1)
        fresh_s = dot(kc[rows, 0:128], us.astype(BF16), ((0,), (0,)))
        fresh_l = dot(kc[rows, 128:256], ul.astype(BF16), ((0,), (0,)))
        state = mine[...]
        tot = mine_tot[...]
        hloc[b] = state
        eoff[b] = jnp.exp(tot)
        step = jnp.concatenate(spread(jnp.broadcast_to(last, (8, 128))), axis=1)
        mine[...] = state * jnp.exp(step)[0:1, :] + jnp.concatenate([fresh_s, fresh_l], axis=1)
        mine_tot[...] = tot + step
        return 0

    lax.fori_loop(0, NBLK, states, 0, unroll=2)

    sbuf[...] = mine[...].astype(BF16)
    r1 = [net.copy(sbuf, sib, sibling), net.copy(mine_tot, sib_tot, sibling)]
    for copy in r1:
        copy.start()
    convolve((3,))

    def intra(b, _):
        rows = block_rows(b)
        cb = ccol[rows, :]
        parts = []
        for g, vals in ((0, xs), (1, xl)):
            lanes = slice(g * 128, g * 128 + 128)
            scores = dot(qc[rows, lanes], kc[rows, lanes], ((1,), (1,)))
            found = []
            for h in range(4) if g == 0 else range(4, 6):
                gap = jnp.broadcast_to(cb[:, h : h + 1], (BLOCK, BLOCK)) - ct[h : h + 1, rows]
                decay = jnp.exp(jnp.where(causal, gap, -1e30))
                w = (scores * decay * dtt[h : h + 1, rows]).astype(BF16)
                at = (h // 2 if g == 0 else h - 4) * 128
                found.append(dot(w, vals[rows, at : at + 128]))
            if g == 0:
                parts += [jnp.where(low, found[0], found[1]), jnp.where(low, found[2], found[3])]
            else:
                parts += found
        inside[rows, :] = jnp.concatenate(parts, axis=1)
        return 0

    for copy in r1:
        copy.wait()

    half = pl.ds(pl.multiple_of(c * 64, 64), 64)
    my_half = mine[half, :]
    sib_half = sib[half, :].astype(F32)
    first = c == 0
    t_me = mine_tot[...]
    t_sib = sib_tot[...]
    early = jnp.where(first, my_half, sib_half)
    late = jnp.where(first, sib_half, my_half)
    t_late = jnp.where(first, t_sib, t_me)
    chip = early * jnp.exp(t_late)[0:1, :] + late
    chip_tot = t_me + t_sib
    ysend[...] = chip.astype(BF16)
    ytot_send[...] = chip_tot

    def peer_copies(send, tot_send, rec, tot_rec, peers_):
        made = []
        for i, peer in enumerate(peers_):
            made += [net.copy(send, rec.at[i], peer), net.copy(tot_send, tot_rec.at[i], peer)]
        return made

    r2 = peer_copies(ysend, ytot_send, yrec, ytot, ypeers)
    for copy in r2:
        copy.start()
    lax.fori_loop(0, 4, intra, 0)
    for copy in r2:
        copy.wait()

    def before_of(pos, rec, tot_rec):
        e = jnp.zeros((64, 512), F32)
        t = jnp.zeros((8, 512), F32)
        for d in (3, 2, 1):
            valid = d <= pos
            e = jnp.where(valid, e * jnp.exp(tot_rec[d - 1])[0:1, :] + rec[d - 1].astype(F32), e)
            t = jnp.where(valid, t + tot_rec[d - 1], t)
        return e, t

    ey, ty = before_of(y, yrec, ytot)
    plane = ey * jnp.exp(chip_tot)[0:1, :] + chip
    plane_tot = ty + chip_tot
    for e in (1, 2, 3):
        valid = y + e <= 3
        plane = jnp.where(valid, plane * jnp.exp(ytot[3 - e])[0:1, :] + yrec[3 - e].astype(F32), plane)
        plane_tot = jnp.where(valid, plane_tot + ytot[3 - e], plane_tot)
    zsend[...] = plane.astype(BF16)
    ztot_send[...] = plane_tot
    r3 = peer_copies(zsend, ztot_send, zrec, ztot, zpeers)
    for copy in r3:
        copy.start()
    for ring in first_rings:
        ring.finish()
    second_rings = [
        Ring(net, axis, at, view(cols))
        for cols in (UP_COLS, DOWN_COLS)
        for axis, at, view in (("sp_0", z, z_view), ("sp_1", y, y_view))
    ]
    for ring in second_rings:
        ring.start()
    shared = [
        [net.copy(z_view(cols)(z), z_view(cols)(z), sibling), net.copy(y_view(cols)(y), y_view(cols)(y), sibling)]
        for cols in (UP_COLS, DOWN_COLS)
    ]
    for group in shared:
        for copy in group:
            copy.start()
    lax.fori_loop(4, NBLK, intra, 0)
    for copy in r3:
        copy.wait()
    ez, _ = before_of(z, zrec, ztot)
    entering = ez * jnp.exp(ty)[0:1, :] + ey
    esend[...] = entering
    r4 = net.copy(esend, ebuf.at[half], sibling)
    r4.start()
    r4.wait()
    own = esend[...]
    enter_rows = []
    for i in range(2):
        arrived = ebuf[i * 64 : i * 64 + 64, :]
        enter_rows.append(jnp.where(c == i, own, arrived))
    enter = jnp.concatenate(enter_rows, axis=0)
    second = enter * jnp.exp(t_sib)[0:1, :] + sib[...].astype(F32)
    mine[...] = jnp.where(first, enter, second)

    proj.forward()
    shared_proj = [net.copy(proj_view(i), proj_view(i), sibling) for i in (x, left, right)]
    for copy in shared_proj:
        copy.start()
    for copy in loads_gate:
        copy.wait()

    def share(copies):
        for copy in copies:
            copy.start()
        return copies

    def finish(s, j):
        b = 2 * j + s // 2
        rows = pl.ds(pl.multiple_of(j * OWN + s * PART, PART), PART)
        state = (hloc[b] + eoff[b][0:1, :] * mine[...]).astype(BF16)
        grow = spread(jnp.exp(ccol[rows, :]))
        carried = [dot(qc[rows, g * 128 : g * 128 + 128], state[:, g * 256 : g * 256 + 256]) for g in (0, 1)]
        for i in range(4):
            g, at = i // 2, (i % 2) * 128
            gate_ref = sg if g == 0 else lg
            v = inside[rows, i * 128 : i * 128 + 128] + carried[g][:, at : at + 128] * grow[i]
            v = v * silu(gate_ref[rows, at : at + 128].astype(F32))
            sq = v * v
            if g == 0:
                s0 = jnp.sum(jnp.where(low_part, sq, 0.0), axis=1, keepdims=True)
                s1 = jnp.sum(jnp.where(low_part, 0.0, sq), axis=1, keepdims=True)
                inv = jnp.where(low_part, lax.rsqrt(s0 / 64 + EPS), lax.rsqrt(s1 / 64 + EPS))
            else:
                inv = lax.rsqrt(jnp.sum(sq, axis=1, keepdims=True) / 128 + EPS)
            v = v * inv * params[7:8, i * 128 : i * 128 + 128]
            chans[x, s, pl.ds(pl.multiple_of(j * PART, PART), PART), i * 128 : i * 128 + 128] = v.astype(BF16)
        return 0


    gathers = [
        Ring(net, "tp", x, lambda i, p, s=s: chans.at[i, s, pl.ds(p * 128, 128)], (0, 1)) for s in range(STEPS)
    ]

    def finish_step(s):
        lax.fori_loop(0, 4, lambda j, _: finish(s, j), 0, unroll=True)

    def share_arrived(k, which):
        zr, yr = second_rings[2 * k], second_rings[2 * k + 1]
        cols = (UP_COLS, DOWN_COLS)[k]
        zs = [zr.before, zr.after] if which == 0 else [lax.rem(z + 2, 4)]
        ys = [yr.before, yr.after] if which == 0 else [lax.rem(y + 2, 4)]
        return share(
            [net.copy(z_view(cols)(i), z_view(cols)(i), sibling) for i in zs]
            + [net.copy(y_view(cols)(i), y_view(cols)(i), sibling) for i in ys]
        )

    def forward_weights(k):
        second_rings[2 * k].forward()
        second_rings[2 * k + 1].forward()
        shared[k] += share_arrived(k, 0)

    def wait_weights(k):
        second_rings[2 * k].finish()
        second_rings[2 * k + 1].finish()
        for copy in shared[k] + share_arrived(k, 1):
            copy.wait()

    def project(s):
        def tile(n, _):
            cols = pl.ds(pl.multiple_of(n * 256, 256), 256)
            acc = dot(chans[0, s], projs[0, :, cols])
            for i in range(1, 4):
                acc = acc + dot(chans[i, s], projs[i, :, cols])
            mix[:, cols] = acc
            return 0

        lax.fori_loop(0, 8, tile, 0, unroll=True)

        def norms(r, _):
            rows = pl.ds(pl.multiple_of(r * 32, 32), 32)
            v = mix[rows, :]
            v = v * lax.rsqrt(jnp.mean(v * v, axis=1, keepdims=True) + EPS)
            at = (r // 2) * OWN + lax.rem(r, 2) * 32 + s * PART
            v = res[pl.ds(pl.multiple_of(at, 32), 32), :].astype(F32) + v * params[0:1, :]
            mix[rows, :] = v
            v = v * lax.rsqrt(jnp.mean(v * v, axis=1, keepdims=True) + EPS)
            rows_in[rows, :] = (v * params[1:2, :]).astype(BF16)
            return 0

        lax.fori_loop(0, OWN // 32, norms, 0, unroll=4)
        mixed[s * PART : s * PART + PART, :] = mix[pl.ds(pl.multiple_of(x * PART, PART), PART), :]

    def gate_up():
        def tile(n, _):
            g_cols = pl.ds(pl.multiple_of(n * 128, 128), 128)
            u_cols = pl.ds(pl.multiple_of(FF_DEV + n * 128, 128), 128)
            w = jnp.concatenate(
                [weights[:, :, :, :, g_cols].reshape(2048, 128), weights[:, :, :, :, u_cols].reshape(2048, 128)], axis=1
            )
            both = dot(rows_in[...], w)
            hidden[:, g_cols] = (silu(both[:, :128]) * both[:, 128:]).astype(BF16)
            return 0

        lax.fori_loop(0, FF_DEV // 128, tile, 0, unroll=True)

    def down(s):
        def tile(n, _):
            w = weights[n // 2, pl.ds(lax.rem(n, 2) * 2, 2), :, :, DOWN_COLS].reshape(256, FF_DEV)
            part = dot(hidden[...], w, ((1,), (1,))).astype(BF16).reshape(4, PART, 256)
            parts_out[:, s * PART : s * PART + PART, pl.ds(pl.multiple_of(n * 256, 256), 256)] = part
            return 0

        lax.fori_loop(0, 8, tile, 0, unroll=True)

    to_left, to_right = {"tp": left}, {"tp": right}
    relays, sends = [None] * STEPS, [None] * STEPS

    def halves(s):
        return pl.ds(s * PART, PART // 2), pl.ds(s * PART + PART // 2, PART // 2)

    def send_parts(s):
        h0, h1 = halves(s)
        kept = pl.ds(s * (PART // 2), PART // 2)
        relays[s] = share([
            net.copy(parts_out.at[across, h0], relay.at[0, kept], to_right),
            net.copy(parts_out.at[across, h1], relay.at[1, kept], to_left),
        ])
        sends[s] = share([
            net.copy(parts_out.at[left, h0], from_right.at[h0], to_left),
            net.copy(parts_out.at[right, h1], from_left.at[h1], to_right),
        ])

    def send_sums(s):
        h0, h1 = halves(s)
        kept = pl.ds(s * (PART // 2), PART // 2)
        for k, (peer, rows, dst, to) in enumerate(((right, h0, from_left, to_right), (left, h1, from_right, to_left))):
            relays[s][k].wait_recv()
            relay_sum[k, kept] = (parts_out[peer, rows, :].astype(F32) + relay[k, kept].astype(F32)).astype(BF16)
            sends[s] += share([net.copy(relay_sum.at[k, kept], dst.at[rows], to)])

    def last(s):
        for copy in relays[s]:
            copy.wait_send()
        for copy in sends[s]:
            copy.wait()

        def rows_of(r, _):
            rows = pl.ds(pl.multiple_of(s * PART + r * 32, 32), 32)
            v = parts_out[x, rows, :].astype(F32) + from_left[rows, :].astype(F32) + from_right[rows, :].astype(F32)
            v = v * lax.rsqrt(jnp.mean(v * v, axis=1, keepdims=True) + EPS)
            out[rows, :] = (mixed[rows, :] + 0.5 * v * params[2:3, :]).astype(BF16)
            return 0

        lax.fori_loop(0, PART // 32, rows_of, 0)

    finish_step(0)
    gathers[0].start()
    finish_step(1)
    gathers[1].start()
    finish_step(2)
    finish_step(3)
    forward_weights(0)
    proj.finish()
    shared_proj += share([net.copy(proj_view(across), proj_view(across), sibling)])
    gathers[0].forward()
    gathers[2].start()
    forward_weights(1)
    gathers[1].forward()
    gathers[3].start()
    for copy in shared_proj:
        copy.wait()
    for s in range(STEPS):
        gathers[s].neighbours()
        gathers[s].finish()
        project(s)
        if s == 0:
            gathers[2].forward()
            wait_weights(0)
        gate_up()
        if s == 0:
            gathers[3].forward()
            wait_weights(1)
        else:
            send_sums(s - 1)
        down(s)
        send_parts(s)
    for s in range(STEPS - 1):
        last(s)
    send_sums(STEPS - 1)
    last(STEPS - 1)


COPIES = 160


def layer(*operands):
    vm = pl.BlockSpec(memory_space=pltpu.VMEM)
    sm = pl.BlockSpec(memory_space=pltpu.SMEM)
    hbm = pl.BlockSpec(memory_space=pl.ANY)
    dma = pltpu.SemaphoreType.DMA
    chan = pltpu.VMEM((ROWS, 256), BF16)
    return pl.pallas_call(
        layer_kernel,
        name="layer",
        out_shape=jax.ShapeDtypeStruct((OWN, 2048), BF16),
        in_specs=[hbm] * 12 + [vm] * 11 + [sm] * 2,
        out_specs=vm,
        scratch_shapes=[chan] * 6 + [
            pltpu.VMEM((8, ROWS), F32), pltpu.VMEM((8, ROWS), F32),
            pltpu.VMEM((ROWS, 128), F32), pltpu.VMEM((ROWS, 128), F32),
            pltpu.VMEM((NBLK, 128, 512), F32), pltpu.VMEM((NBLK, 8, 512), F32),
            pltpu.VMEM((ROWS, 512), F32),
            pltpu.VMEM((4, 16, 256), BF16),
            pltpu.VMEM((128, 512), F32), pltpu.VMEM((8, 512), F32),
            pltpu.VMEM((128, 512), BF16), pltpu.VMEM((128, 512), BF16), pltpu.VMEM((8, 512), F32),
            pltpu.VMEM((64, 512), BF16), pltpu.VMEM((8, 512), F32),
            pltpu.VMEM((3, 64, 512), BF16), pltpu.VMEM((3, 8, 512), F32),
            pltpu.VMEM((64, 512), BF16), pltpu.VMEM((8, 512), F32),
            pltpu.VMEM((3, 64, 512), BF16), pltpu.VMEM((3, 8, 512), F32),
            pltpu.VMEM((64, 512), F32), pltpu.VMEM((128, 512), F32),
            pltpu.VMEM((4, STEPS, OWN, 512), BF16),
            pltpu.VMEM((4, 4, 2, 64, 3 * FF_DEV), BF16), pltpu.VMEM((4, 512, 2048), BF16),
            pltpu.VMEM((ROWS, 2048), BF16), pltpu.VMEM((OWN, 2048), F32), pltpu.VMEM((OWN, 2048), F32),
            pltpu.VMEM((OWN, 2048), BF16), pltpu.VMEM((OWN, FF_DEV), BF16),
            pltpu.VMEM((4, OWN, 2048), BF16),
            pltpu.VMEM((2, 128, 2048), BF16), pltpu.VMEM((2, 128, 2048), BF16),
            pltpu.VMEM((OWN, 2048), BF16), pltpu.VMEM((OWN, 2048), BF16),
            pltpu.VMEM((8, 2048), F32),
            dma((COPIES,)), dma((COPIES,)), dma((12,)),
        ],
        compiler_params=pltpu.CompilerParams(
            collective_id=0, has_side_effects=True, vmem_limit_bytes=67043328
        ),
        cost_estimate=pl.CostEstimate(flops=22_000_000_000, bytes_accessed=30_000_000, transcendentals=0),
    )(*operands)


def local(
    residual, small_heads, large_heads, state_keys, state_queries, small_gate, large_gate,
    small_step, large_step, small_taps, large_taps, key_taps, query_taps, small_decay, large_decay,
    small_gain, large_gain, small_out, large_out, mixer_gain, ffn_in_gain,
    gate_proj, up_proj, down_proj, ffn_out_gain,
):
    return layer(
        residual, small_heads, large_heads, state_keys.reshape(ROWS, 256), state_queries.reshape(ROWS, 256),
        small_gate, large_gate, gate_proj, up_proj, down_proj, small_out, large_out,
        small_step.T, large_step.T, mixer_gain, ffn_in_gain, ffn_out_gain, small_gain, large_gain,
        small_taps, large_taps, key_taps, query_taps, small_decay, large_decay,
    )


def solution(mesh):
    torus = Mesh(mesh.devices.reshape(4, 4, 2, mesh.shape["tp"]), ("sp_0", "sp_1", "sp_2", "tp"))
    in_specs = (
        P(SP, None), P(SP, "tp"), P(SP, "tp"), P(SP, "tp", None), P(SP, "tp", None),
        P(SP, "tp"), P(SP, "tp"), P(SP, "tp"), P(SP, "tp"),
        P(None, "tp"), P(None, "tp"), P(None, "tp", None), P(None, "tp", None),
        P("tp"), P("tp"), P("tp"), P("tp"), P("tp", None), P("tp", None),
        P(), P(), P(SP, "tp"), P(SP, "tp"), P(SP, "tp"), P(),
    )
    return jax.shard_map(local, mesh=torus, in_specs=in_specs, out_specs=P(SP_TP, None), check_vma=False)
```

```python
import functools

import jax
import jax.numpy as jnp
from jax import lax
from jax.experimental import pallas as pl
from jax.experimental.pallas import tpu as pltpu
from jax.sharding import Mesh
from jax.sharding import PartitionSpec as P

BLOCK = 128
ROWS = 1024
NBLK = ROWS // BLOCK
SP = ("sp_0", "sp_1", "sp_2")
SP_TP = ("sp_0", "sp_1", "sp_2", "tp")
EPS = 1e-06
MESH = pl.DeviceIdType.MESH
F32 = jnp.float32
BF16 = jnp.bfloat16


def dot(a, b, contract=((1,), (0,)), precision=None):
    return lax.dot_general(
        a, b, (contract, ((), ())), preferred_element_type=F32, precision=precision
    )


def silu(v):
    return v * jax.nn.sigmoid(v)


def spread(m):
    rows = m.shape[0]
    low = lax.broadcasted_iota(jnp.int32, (rows, 128), 1) < 64
    cols = [jnp.broadcast_to(m[:, h : h + 1], (rows, 128)) for h in range(6)]
    return (
        jnp.where(low, cols[0], cols[1]),
        jnp.where(low, cols[2], cols[3]),
        cols[4],
        cols[5],
    )


def spread_all(m):
    return jnp.concatenate(spread(m), axis=1)


def block_rows(b):
    return pl.ds(pl.multiple_of(b * BLOCK, BLOCK), BLOCK)


OWN = 256
STEPS = 4
PART = OWN // STEPS
MAIN = 192
FF_DEV = 1408
UP_COLS = pl.ds(0, 2 * FF_DEV)
DOWN_COLS = pl.ds(2 * FF_DEV, FF_DEV)


class Net:
    def __init__(self, send_sems, recv_sems):
        self.send_sems, self.recv_sems, self.used = send_sems, recv_sems, 0

    def copy(self, src, dst, peer):
        i = self.used
        self.used += 1
        return pltpu.make_async_remote_copy(
            src_ref=src, dst_ref=dst, send_sem=self.send_sems.at[i], recv_sem=self.recv_sems.at[i],
            device_id=peer, device_id_type=MESH,
        )


class Ring:
    def __init__(self, net, axis, at, view, pieces=(None,)):
        self.net, self.at, self.view = net, at, view
        self.before, self.after = lax.rem(at + 3, 4), lax.rem(at + 1, 4)
        self.up, self.down = {axis: self.after}, {axis: self.before}
        self.ups = [net.copy(view(at, p), view(at, p), self.up) for p in pieces]
        self.downs = [net.copy(view(at, p), view(at, p), self.down) for p in pieces[::-1]]
        self.forwards = []

    def start(self):
        for pair in zip(self.ups, self.downs):
            for copy in pair:
                copy.start()

    def forward(self):
        self.ups[0].wait_recv()
        here = self.view(self.before, 0)
        self.forwards.append(self.net.copy(here, here, self.up))
        self.forwards[-1].start()
        self.downs[0].wait_recv()
        here = self.view(self.after, 1)
        self.forwards.append(self.net.copy(here, here, self.down))
        self.forwards[-1].start()

    def neighbours(self):
        for copy in self.ups[1:] + self.downs[1:]:
            copy.wait_recv()

    def finish(self):
        for copy in self.forwards:
            copy.wait_recv()
        for copy in self.ups + self.downs + self.forwards:
            copy.wait_send()


def layer_kernel(
    residual, sh_in, lh_in, ks_in, qs_in, sg_in, lg_in, gate_in, up_in, down_in, so_in, lo_in,
    small_steps, large_steps, mixer_gain, ffn_in_gain, ffn_out_gain, sgain, lgain, stap, ltap, ktap, qtap, sdec, ldec,
    out,
    xs, xl, kc, qc, sg, lg,
    dtt, ct, ccol, dcol, hloc, eoff, inside,
    halo, mine, mine_tot, sbuf, sib, sib_tot, ysend, ytot_send, yrec, ytot, zsend, ztot_send, zrec, ztot, esend, ebuf,
    chans, weights, projs, res, mix, mixed, rows_in, hidden, parts_out, relay, relay_sum, from_left, from_right,
    params, send_sems, recv_sems, load_sems,
):
    z = lax.axis_index("sp_0")
    y = lax.axis_index("sp_1")
    c = lax.axis_index("sp_2")
    x = lax.axis_index("tp")
    sp = (z * 4 + y) * 2 + c
    nxt = lax.rem(sp + 1, 32)
    prv = lax.rem(sp + 31, 32)
    left, right, across = lax.rem(x + 3, 4), lax.rem(x + 1, 4), lax.rem(x + 2, 4)
    net = Net(send_sems, recv_sems)

    def at_sp(i):
        return {"sp_0": i // 8, "sp_1": lax.rem(i // 2, 4), "sp_2": lax.rem(i, 2)}

    loads = [
        pltpu.make_async_copy(src, dst, load_sems.at[i])
        for i, (src, dst) in enumerate((
            (sh_in, xs), (lh_in, xl), (ks_in, kc), (qs_in, qc),
            (gate_in, weights.at[z, y, c, :, pl.ds(0, FF_DEV)]),
            (up_in, weights.at[z, y, c, :, pl.ds(FF_DEV, FF_DEV)]),
            (down_in, weights.at[z, y, c, :, DOWN_COLS]),
            (so_in, projs.at[x, pl.ds(0, 256)]),
            (lo_in, projs.at[x, pl.ds(256, 256)]),
            (sg_in, sg), (lg_in, lg),
            (residual, res),
        ))
    ]
    for copy in loads:
        copy.start()
    loads_in, loads_own, loads_gate = loads[:4], loads[4:9], loads[9:]

    ypeers = [{"sp_1": lax.rem(y + d, 4)} for d in (1, 2, 3)]
    zpeers = [{"sp_0": lax.rem(z + d, 4)} for d in (1, 2, 3)]
    xpeers = [{"tp": i} for i in (across, right, left)]
    sibling = {"sp_2": 1 - c}
    barrier = pltpu.get_barrier_semaphore()
    peers = [at_sp(nxt), at_sp(prv), sibling] + ypeers + zpeers + xpeers
    for peer in peers:
        pl.semaphore_signal(barrier, inc=1, device_id=peer, device_id_type=MESH)
    pl.semaphore_wait(barrier, len(peers))

    halo_copies = [
        net.copy(src.at[pl.ds(ROWS - 16, 16)], halo.at[i], at_sp(nxt)) for i, src in enumerate((sh_in, lh_in, ks_in, qs_in))
    ]
    for copy in halo_copies:
        copy.start()

    def span(part, size):
        return pl.ds(0, size) if part is None else pl.ds(part * (size // 2), size // 2)

    def y_first(cols):
        return lambda i, p=None: weights.at[z, i, c, span(p, 32), cols]

    def z_first(cols):
        return lambda i, p=None: weights.at[i, y, c, pl.ds(32, 32) if p is None else pl.ds(32 + 16 * p, 16), cols]

    def z_view(cols):
        return lambda i, p=None: weights.at[i, span(p, 4), c, pl.ds(0, 32), cols]

    def y_view(cols):
        return lambda i, p=None: weights.at[span(p, 4), i, c, pl.ds(32, 32), cols]

    def proj_view(i, p=None):
        size = MAIN if p is None else MAIN // 2
        return projs.at[i, pl.ds(pl.multiple_of(c * 256 + (0 if p is None else p * size), 32), size)]

    def slice_view(place, side, i, p=None):
        rows = pl.ds(pl.multiple_of(c * 256 + MAIN + 16 * place, 16), 16)
        return projs.at[i, rows, pl.ds(side * 1024, 1024) if p is None else pl.ds(side * 1024 + 512 * p, 512)]

    for copy in loads_own:
        copy.wait()
    first_rings = [
        Ring(net, axis, at, view(cols))
        for cols in (UP_COLS, DOWN_COLS)
        for axis, at, view in (("sp_1", y, y_first), ("sp_0", z, z_first))
    ]
    proj = Ring(net, "tp", x, proj_view)
    cross_rings = [
        Ring(net, "tp", x, functools.partial(slice_view, place, side)) for side, place in enumerate((y, z))
    ]
    for ring in first_rings + cross_rings + [proj]:
        ring.start()

    for i, gain in enumerate((mixer_gain, ffn_in_gain, ffn_out_gain)):
        params[i : i + 1, :] = gain[...].astype(F32).reshape(1, 2048)
    for i, gain in enumerate((sgain, lgain)):
        params[7:8, i * 256 : i * 256 + 256] = gain[...].astype(F32).reshape(1, 256)
    for i, tap in enumerate((stap, ltap)):
        params[3:7, i * 256 : i * 256 + 256] = tap[...].astype(F32)
    for i, tap in enumerate((ktap, qtap)):
        for g in (0, 1):
            at = 512 + i * 256 + g * 128
            params[3:7, at : at + 128] = tap[:, g, :].astype(F32)

    dtt[...] = jnp.zeros_like(dtt)
    dtt[0:4, :] = jax.nn.softplus(small_steps[...])
    dtt[4:6, :] = jax.nn.softplus(large_steps[...])
    ct[...] = jnp.zeros_like(ct)
    for h in range(6):
        d = sdec[h] if h < 4 else ldec[h - 4]
        rate = jnp.exp(jnp.full((1, ROWS), d, F32))
        ct[h : h + 1, :] = -dtt[h : h + 1, :] * rate
    tr = lax.broadcasted_iota(jnp.int32, (BLOCK, BLOCK), 0)
    tc = lax.broadcasted_iota(jnp.int32, (BLOCK, BLOCK), 1)
    upper = (tr <= tc).astype(F32)
    low = tc < 64
    low_part = low[:PART]
    causal = tc <= tr

    def sums(b, _):
        rows = block_rows(b)
        cum = dot(ct[:, rows], upper, precision=lax.Precision.HIGHEST)
        ct[:, rows] = cum
        pad = jnp.zeros((BLOCK - 8, BLOCK), F32)
        ccol[rows, :] = jnp.concatenate([cum, pad], axis=0).T
        dcol[rows, :] = jnp.concatenate([dtt[:, rows], pad], axis=0).T
        return 0

    lax.fori_loop(0, NBLK, sums, 0, unroll=True)

    taps = [params[3:7, i * 256 : i * 256 + 256] for i in range(4)]
    keep = jnp.where(sp == 0, 0.0, 1.0)

    def conv_of(ext, tap):
        acc = jnp.zeros((BLOCK, 256), F32)
        for k in range(4):
            shifted = ext if k == 3 else pltpu.roll(ext, 3 - k, 0)
            acc = acc + tap[k : k + 1, :] * shifted[16:, :]
        return silu(acc).astype(BF16)

    def convolve(which):
        refs = (xs, xl, kc, qc)

        def conv_block(i, _):
            b = NBLK - 1 - i
            start = pl.multiple_of(b * BLOCK - 16, 16)
            for k in which:
                refs[k][block_rows(b), :] = conv_of(refs[k][pl.ds(start, BLOCK + 16), :].astype(F32), taps[k])
            return 0

        lax.fori_loop(0, NBLK - 1, conv_block, 0)
        for k in which:
            halo_copies[k].wait()
        for k in which:
            ext = jnp.concatenate([halo[k].astype(F32) * keep, refs[k][0:BLOCK, :].astype(F32)], axis=0)
            refs[k][0:BLOCK, :] = conv_of(ext, taps[k])

    for copy in loads_in:
        copy.wait()
    convolve((0, 1, 2))
    for ring in first_rings + cross_rings:
        ring.forward()

    mine[...] = jnp.zeros_like(mine)
    mine_tot[...] = jnp.zeros_like(mine_tot)

    def states(b, _):
        rows = block_rows(b)
        cb = ccol[rows, :]
        last = cb[BLOCK - 1 : BLOCK, :]
        scale = spread(dcol[rows, :] * jnp.exp(last - cb))
        xsb = xs[rows, :].astype(F32)
        xlb = xl[rows, :].astype(F32)
        us = jnp.concatenate([xsb[:, :128] * scale[0], xsb[:, 128:] * scale[1]], axis=1)
        ul = jnp.concatenate([xlb[:, :128] * scale[2], xlb[:, 128:] * scale[3]], axis=1)
        fresh_s = dot(kc[rows, 0:128], us.astype(BF16), ((0,), (0,)))
        fresh_l = dot(kc[rows, 128:256], ul.astype(BF16), ((0,), (0,)))
        state = mine[...]
        tot = mine_tot[...]
        hloc[b] = state
        eoff[b] = jnp.exp(spread_all(tot))
        step = jnp.broadcast_to(last, (8, 128))
        mine[...] = state * jnp.exp(spread_all(step))[0:1, :] + jnp.concatenate([fresh_s, fresh_l], axis=1)
        mine_tot[...] = tot + step
        return 0

    lax.fori_loop(0, NBLK, states, 0, unroll=2)

    sbuf[...] = mine[...].astype(BF16)
    r1 = [net.copy(sbuf, sib, sibling), net.copy(mine_tot, sib_tot, sibling)]
    for copy in r1:
        copy.start()
    convolve((3,))

    def intra(b, _):
        rows = block_rows(b)
        cb = ccol[rows, :]
        parts = []
        for g, vals in ((0, xs), (1, xl)):
            lanes = slice(g * 128, g * 128 + 128)
            scores = dot(qc[rows, lanes], kc[rows, lanes], ((1,), (1,)))
            found = []
            for h in range(4) if g == 0 else range(4, 6):
                gap = jnp.broadcast_to(cb[:, h : h + 1], (BLOCK, BLOCK)) - ct[h : h + 1, rows]
                decay = jnp.exp(jnp.where(causal, gap, -1e30))
                w = (scores * decay * dtt[h : h + 1, rows]).astype(BF16)
                at = (h // 2 if g == 0 else h - 4) * 128
                found.append(dot(w, vals[rows, at : at + 128]))
            if g == 0:
                parts += [jnp.where(low, found[0], found[1]), jnp.where(low, found[2], found[3])]
            else:
                parts += found
        inside[rows, :] = jnp.concatenate(parts, axis=1)
        return 0

    for copy in r1:
        copy.wait()

    half = pl.ds(pl.multiple_of(c * 64, 64), 64)
    my_half = mine[half, :]
    sib_half = sib[half, :].astype(F32)
    first = c == 0
    t_me = mine_tot[...]
    t_sib = sib_tot[...]
    early = jnp.where(first, my_half, sib_half)
    late = jnp.where(first, sib_half, my_half)
    t_late = jnp.where(first, t_sib, t_me)
    chip = early * jnp.exp(spread_all(t_late))[0:1, :] + late
    chip_tot = t_me + t_sib
    ysend[...] = chip.astype(BF16)
    ytot_send[...] = chip_tot

    def peer_copies(send, tot_send, rec, tot_rec, peers_):
        made = []
        for i, peer in enumerate(peers_):
            made += [net.copy(send, rec.at[i], peer), net.copy(tot_send, tot_rec.at[i], peer)]
        return made

    r2 = peer_copies(ysend, ytot_send, yrec, ytot, ypeers)
    for copy in r2:
        copy.start()
    lax.fori_loop(0, 4, intra, 0)
    for copy in r2:
        copy.wait()

    def before_of(pos, rec, tot_rec):
        e = jnp.zeros((64, 512), F32)
        t = jnp.zeros((8, 128), F32)
        for d in (3, 2, 1):
            valid = d <= pos
            e = jnp.where(valid, e * jnp.exp(spread_all(tot_rec[d - 1]))[0:1, :] + rec[d - 1].astype(F32), e)
            t = jnp.where(valid, t + tot_rec[d - 1], t)
        return e, t

    ey, ty = before_of(y, yrec, ytot)
    plane = ey * jnp.exp(spread_all(chip_tot))[0:1, :] + chip
    plane_tot = ty + chip_tot
    for e in (1, 2, 3):
        valid = y + e <= 3
        plane = jnp.where(valid, plane * jnp.exp(spread_all(ytot[3 - e]))[0:1, :] + yrec[3 - e].astype(F32), plane)
        plane_tot = jnp.where(valid, plane_tot + ytot[3 - e], plane_tot)
    zsend[...] = plane.astype(BF16)
    ztot_send[...] = plane_tot
    r3 = peer_copies(zsend, ztot_send, zrec, ztot, zpeers)
    for copy in r3:
        copy.start()
    for ring in first_rings + cross_rings:
        ring.finish()
    slice_rings = [
        Ring(net, axis, at, lambda j, p=None, i=i, side=side: slice_view(j, side, i, p))
        for i in (left, right, across)
        for side, (axis, at) in enumerate((("sp_1", y), ("sp_0", z)))
    ]
    for ring in slice_rings:
        ring.start()
    second_rings = [
        Ring(net, axis, at, view(cols))
        for cols in (UP_COLS, DOWN_COLS)
        for axis, at, view in (("sp_0", z, z_view), ("sp_1", y, y_view))
    ]
    shared = [[], []]

    def start_weights(k):
        cols = (UP_COLS, DOWN_COLS)[k]
        second_rings[2 * k].start()
        second_rings[2 * k + 1].start()
        shared[k] += [
            net.copy(z_view(cols)(z), z_view(cols)(z), sibling), net.copy(y_view(cols)(y), y_view(cols)(y), sibling)
        ]
        for copy in shared[k]:
            copy.start()

    start_weights(0)
    lax.fori_loop(4, NBLK, intra, 0)
    for copy in r3:
        copy.wait()
    for ring in slice_rings:
        ring.forward()
    ez, _ = before_of(z, zrec, ztot)
    entering = ez * jnp.exp(spread_all(ty))[0:1, :] + ey
    esend[...] = entering
    r4 = net.copy(esend, ebuf.at[half], sibling)
    r4.start()
    r4.wait()
    own = esend[...]
    enter_rows = []
    for i in range(2):
        arrived = ebuf[i * 64 : i * 64 + 64, :]
        enter_rows.append(jnp.where(c == i, own, arrived))
    enter = jnp.concatenate(enter_rows, axis=0)
    second = enter * jnp.exp(spread_all(t_sib))[0:1, :] + sib[...].astype(F32)
    mine[...] = jnp.where(first, enter, second)

    proj.forward()
    shared_proj = [net.copy(proj_view(i), proj_view(i), sibling) for i in (x, left, right)]
    for copy in shared_proj:
        copy.start()
    for copy in loads_gate:
        copy.wait()

    def share(copies):
        for copy in copies:
            copy.start()
        return copies

    def finish(s, j):
        b = 2 * j + s // 2
        rows = pl.ds(pl.multiple_of(j * OWN + s * PART, PART), PART)
        state = (hloc[b] + eoff[b][0:1, :] * mine[...]).astype(BF16)
        grow = spread(jnp.exp(ccol[rows, :]))
        carried = [dot(qc[rows, g * 128 : g * 128 + 128], state[:, g * 256 : g * 256 + 256]) for g in (0, 1)]
        for i in range(4):
            g, at = i // 2, (i % 2) * 128
            gate_ref = sg if g == 0 else lg
            v = inside[rows, i * 128 : i * 128 + 128] + carried[g][:, at : at + 128] * grow[i]
            v = v * silu(gate_ref[rows, at : at + 128].astype(F32))
            sq = v * v
            if g == 0:
                s0 = jnp.sum(jnp.where(low_part, sq, 0.0), axis=1, keepdims=True)
                s1 = jnp.sum(jnp.where(low_part, 0.0, sq), axis=1, keepdims=True)
                inv = jnp.where(low_part, lax.rsqrt(s0 / 64 + EPS), lax.rsqrt(s1 / 64 + EPS))
            else:
                inv = lax.rsqrt(jnp.sum(sq, axis=1, keepdims=True) / 128 + EPS)
            v = v * inv * params[7:8, i * 128 : i * 128 + 128]
            chans[x, s, pl.ds(pl.multiple_of(j * PART, PART), PART), i * 128 : i * 128 + 128] = v.astype(BF16)
        return 0


    gathers = [
        Ring(net, "tp", x, lambda i, p, s=s: chans.at[i, s, pl.ds(p * 128, 128)], (0, 1)) for s in range(STEPS)
    ]

    def finish_step(s):
        lax.fori_loop(0, 4, lambda j, _: finish(s, j), 0, unroll=True)

    def share_arrived(k, which):
        zr, yr = second_rings[2 * k], second_rings[2 * k + 1]
        cols = (UP_COLS, DOWN_COLS)[k]
        zs = [zr.before, zr.after] if which == 0 else [lax.rem(z + 2, 4)]
        ys = [yr.before, yr.after] if which == 0 else [lax.rem(y + 2, 4)]
        return share(
            [net.copy(z_view(cols)(i), z_view(cols)(i), sibling) for i in zs]
            + [net.copy(y_view(cols)(i), y_view(cols)(i), sibling) for i in ys]
        )

    def forward_weights(k):
        second_rings[2 * k].forward()
        second_rings[2 * k + 1].forward()
        shared[k] += share_arrived(k, 0)

    def wait_weights(k):
        second_rings[2 * k].finish()
        second_rings[2 * k + 1].finish()
        for copy in shared[k] + share_arrived(k, 1):
            copy.wait()

    def project(s):
        def tile(n, _):
            cols = pl.ds(pl.multiple_of(n * 256, 256), 256)
            acc = dot(chans[0, s], projs[0, :, cols])
            for i in range(1, 4):
                acc = acc + dot(chans[i, s], projs[i, :, cols])
            mix[:, cols] = acc
            return 0

        lax.fori_loop(0, 8, tile, 0, unroll=True)

        def norms(r, _):
            rows = pl.ds(pl.multiple_of(r * 32, 32), 32)
            v = mix[rows, :]
            v = v * lax.rsqrt(jnp.mean(v * v, axis=1, keepdims=True) + EPS)
            at = (r // 2) * OWN + lax.rem(r, 2) * 32 + s * PART
            v = res[pl.ds(pl.multiple_of(at, 32), 32), :].astype(F32) + v * params[0:1, :]
            mix[rows, :] = v
            v = v * lax.rsqrt(jnp.mean(v * v, axis=1, keepdims=True) + EPS)
            rows_in[rows, :] = (v * params[1:2, :]).astype(BF16)
            return 0

        lax.fori_loop(0, OWN // 32, norms, 0, unroll=4)
        mixed[s * PART : s * PART + PART, :] = mix[pl.ds(pl.multiple_of(x * PART, PART), PART), :]

    def gate_up():
        def tile(n, _):
            g_cols = pl.ds(pl.multiple_of(n * 128, 128), 128)
            u_cols = pl.ds(pl.multiple_of(FF_DEV + n * 128, 128), 128)
            w = jnp.concatenate(
                [weights[:, :, :, :, g_cols].reshape(2048, 128), weights[:, :, :, :, u_cols].reshape(2048, 128)], axis=1
            )
            both = dot(rows_in[...], w)
            hidden[:, g_cols] = (silu(both[:, :128]) * both[:, 128:]).astype(BF16)
            return 0

        lax.fori_loop(0, FF_DEV // 128, tile, 0, unroll=True)

    def down(s):
        def tile(n, _):
            w = weights[n // 2, pl.ds(lax.rem(n, 2) * 2, 2), :, :, DOWN_COLS].reshape(256, FF_DEV)
            part = dot(hidden[...], w, ((1,), (1,))).astype(BF16).reshape(4, PART, 256)
            parts_out[:, s * PART : s * PART + PART, pl.ds(pl.multiple_of(n * 256, 256), 256)] = part
            return 0

        lax.fori_loop(0, 8, tile, 0, unroll=True)

    to_left, to_right = {"tp": left}, {"tp": right}
    relays, sends = [None] * STEPS, [None] * STEPS

    def halves(s):
        return pl.ds(s * PART, PART // 2), pl.ds(s * PART + PART // 2, PART // 2)

    def send_parts(s):
        h0, h1 = halves(s)
        kept = pl.ds(s * (PART // 2), PART // 2)
        relays[s] = share([
            net.copy(parts_out.at[across, h0], relay.at[0, kept], to_right),
            net.copy(parts_out.at[across, h1], relay.at[1, kept], to_left),
        ])
        sends[s] = share([
            net.copy(parts_out.at[left, h0], from_right.at[h0], to_left),
            net.copy(parts_out.at[right, h1], from_left.at[h1], to_right),
        ])

    def send_sums(s):
        h0, h1 = halves(s)
        kept = pl.ds(s * (PART // 2), PART // 2)
        for k, (peer, rows, dst, to) in enumerate(((right, h0, from_left, to_right), (left, h1, from_right, to_left))):
            relays[s][k].wait_recv()
            relay_sum[k, kept] = (parts_out[peer, rows, :].astype(F32) + relay[k, kept].astype(F32)).astype(BF16)
            sends[s] += share([net.copy(relay_sum.at[k, kept], dst.at[rows], to)])

    def last(s):
        for copy in relays[s]:
            copy.wait_send()
        for copy in sends[s]:
            copy.wait()

        def rows_of(r, _):
            rows = pl.ds(pl.multiple_of(s * PART + r * 32, 32), 32)
            v = parts_out[x, rows, :].astype(F32) + from_left[rows, :].astype(F32) + from_right[rows, :].astype(F32)
            v = v * lax.rsqrt(jnp.mean(v * v, axis=1, keepdims=True) + EPS)
            out[rows, :] = (mixed[rows, :] + 0.5 * v * params[2:3, :]).astype(BF16)
            return 0

        lax.fori_loop(0, PART // 32, rows_of, 0)

    finish_step(0)
    gathers[0].start()
    finish_step(1)
    gathers[1].start()
    finish_step(2)
    finish_step(3)
    forward_weights(0)
    start_weights(1)
    proj.finish()
    shared_proj += share([net.copy(proj_view(across), proj_view(across), sibling)])
    for ring in slice_rings:
        ring.finish()
    for i in (left, right, across):
        here = projs.at[i, pl.ds(pl.multiple_of(c * 256 + MAIN, 32), 256 - MAIN)]
        shared_proj += share([net.copy(here, here, sibling)])
    gathers[0].forward()
    gathers[2].start()
    forward_weights(1)
    gathers[1].forward()
    gathers[3].start()
    for copy in shared_proj:
        copy.wait()
    def project_step(s):
        gathers[s].neighbours()
        gathers[s].finish()
        project(s)

    project_step(0)
    gathers[2].forward()
    for s in range(STEPS):
        if s == 0:
            wait_weights(0)
        gate_up()
        if s == 0:
            gathers[3].forward()
        if s + 1 < STEPS:
            project_step(s + 1)
        if s == 0:
            wait_weights(1)
        else:
            send_sums(s - 1)
        down(s)
        send_parts(s)
    for s in range(STEPS - 1):
        last(s)
    send_sums(STEPS - 1)
    last(STEPS - 1)


COPIES = 200


def layer(*operands):
    vm = pl.BlockSpec(memory_space=pltpu.VMEM)
    sm = pl.BlockSpec(memory_space=pltpu.SMEM)
    hbm = pl.BlockSpec(memory_space=pl.ANY)
    dma = pltpu.SemaphoreType.DMA
    chan = pltpu.VMEM((ROWS, 256), BF16)
    return pl.pallas_call(
        layer_kernel,
        name="layer",
        out_shape=jax.ShapeDtypeStruct((OWN, 2048), BF16),
        in_specs=[hbm] * 12 + [vm] * 11 + [sm] * 2,
        out_specs=vm,
        scratch_shapes=[chan] * 6 + [
            pltpu.VMEM((8, ROWS), F32), pltpu.VMEM((8, ROWS), F32),
            pltpu.VMEM((ROWS, 128), F32), pltpu.VMEM((ROWS, 128), F32),
            pltpu.VMEM((NBLK, 128, 512), F32), pltpu.VMEM((NBLK, 8, 512), F32),
            pltpu.VMEM((ROWS, 512), F32),
            pltpu.VMEM((4, 16, 256), BF16),
            pltpu.VMEM((128, 512), F32), pltpu.VMEM((8, 128), F32),
            pltpu.VMEM((128, 512), BF16), pltpu.VMEM((128, 512), BF16), pltpu.VMEM((8, 128), F32),
            pltpu.VMEM((64, 512), BF16), pltpu.VMEM((8, 128), F32),
            pltpu.VMEM((3, 64, 512), BF16), pltpu.VMEM((3, 8, 128), F32),
            pltpu.VMEM((64, 512), BF16), pltpu.VMEM((8, 128), F32),
            pltpu.VMEM((3, 64, 512), BF16), pltpu.VMEM((3, 8, 128), F32),
            pltpu.VMEM((64, 512), F32), pltpu.VMEM((128, 512), F32),
            pltpu.VMEM((4, STEPS, OWN, 512), BF16),
            pltpu.VMEM((4, 4, 2, 64, 3 * FF_DEV), BF16), pltpu.VMEM((4, 512, 2048), BF16),
            pltpu.VMEM((ROWS, 2048), BF16), pltpu.VMEM((OWN, 2048), F32), pltpu.VMEM((OWN, 2048), F32),
            pltpu.VMEM((OWN, 2048), BF16), pltpu.VMEM((OWN, FF_DEV), BF16),
            pltpu.VMEM((4, OWN, 2048), BF16),
            pltpu.VMEM((2, 128, 2048), BF16), pltpu.VMEM((2, 128, 2048), BF16),
            pltpu.VMEM((OWN, 2048), BF16), pltpu.VMEM((OWN, 2048), BF16),
            pltpu.VMEM((8, 2048), F32),
            dma((COPIES,)), dma((COPIES,)), dma((12,)),
        ],
        compiler_params=pltpu.CompilerParams(
            collective_id=0, has_side_effects=True, vmem_limit_bytes=67043328
        ),
        cost_estimate=pl.CostEstimate(flops=22_000_000_000, bytes_accessed=30_000_000, transcendentals=0),
    )(*operands)


def local(
    residual, small_heads, large_heads, state_keys, state_queries, small_gate, large_gate,
    small_step, large_step, small_taps, large_taps, key_taps, query_taps, small_decay, large_decay,
    small_gain, large_gain, small_out, large_out, mixer_gain, ffn_in_gain,
    gate_proj, up_proj, down_proj, ffn_out_gain,
):
    return layer(
        residual, small_heads, large_heads, state_keys.reshape(ROWS, 256), state_queries.reshape(ROWS, 256),
        small_gate, large_gate, gate_proj, up_proj, down_proj, small_out, large_out,
        small_step.T, large_step.T, mixer_gain, ffn_in_gain, ffn_out_gain, small_gain, large_gain,
        small_taps, large_taps, key_taps, query_taps, small_decay, large_decay,
    )


def solution(mesh):
    torus = Mesh(mesh.devices.reshape(4, 4, 2, mesh.shape["tp"]), ("sp_0", "sp_1", "sp_2", "tp"))
    in_specs = (
        P(SP, None), P(SP, "tp"), P(SP, "tp"), P(SP, "tp", None), P(SP, "tp", None),
        P(SP, "tp"), P(SP, "tp"), P(SP, "tp"), P(SP, "tp"),
        P(None, "tp"), P(None, "tp"), P(None, "tp", None), P(None, "tp", None),
        P("tp"), P("tp"), P("tp"), P("tp"), P("tp", None), P("tp", None),
        P(), P(), P(SP, "tp"), P(SP, "tp"), P(SP, "tp"), P(),
    )
    return jax.shard_map(local, mesh=torus, in_specs=in_specs, out_specs=P(SP_TP, None), check_vma=False)
```

```python
import functools

import jax
import jax.numpy as jnp
from jax import lax
from jax.experimental import pallas as pl
from jax.experimental.pallas import tpu as pltpu
from jax.sharding import Mesh
from jax.sharding import PartitionSpec as P

BLOCK = 128
ROWS = 1024
NBLK = ROWS // BLOCK
SP = ("sp_0", "sp_1", "sp_2")
SP_TP = ("sp_0", "sp_1", "sp_2", "tp")
EPS = 1e-06
MESH = pl.DeviceIdType.MESH
F32 = jnp.float32
BF16 = jnp.bfloat16


def dot(a, b, contract=((1,), (0,)), precision=None):
    return lax.dot_general(
        a, b, (contract, ((), ())), preferred_element_type=F32, precision=precision
    )


def silu(v):
    return v * jax.nn.sigmoid(v)


def spread(m):
    rows = m.shape[0]
    low = lax.broadcasted_iota(jnp.int32, (rows, 128), 1) < 64
    cols = [jnp.broadcast_to(m[:, h : h + 1], (rows, 128)) for h in range(6)]
    return (
        jnp.where(low, cols[0], cols[1]),
        jnp.where(low, cols[2], cols[3]),
        cols[4],
        cols[5],
    )


def spread_all(m):
    return jnp.concatenate(spread(m), axis=1)


def block_rows(b):
    return pl.ds(pl.multiple_of(b * BLOCK, BLOCK), BLOCK)


OWN = 256
STEPS = 4
PART = OWN // STEPS
MAIN = 192
FF_DEV = 1408
UP_COLS = pl.ds(0, 2 * FF_DEV)
DOWN_COLS = pl.ds(2 * FF_DEV, FF_DEV)


class Net:
    def __init__(self, send_sems, recv_sems):
        self.send_sems, self.recv_sems, self.used = send_sems, recv_sems, 0

    def copy(self, src, dst, peer):
        i = self.used
        self.used += 1
        return pltpu.make_async_remote_copy(
            src_ref=src, dst_ref=dst, send_sem=self.send_sems.at[i], recv_sem=self.recv_sems.at[i],
            device_id=peer, device_id_type=MESH,
        )


class Ring:
    def __init__(self, net, axis, at, view, pieces=(None,)):
        self.net, self.at, self.view = net, at, view
        self.before, self.after = lax.rem(at + 3, 4), lax.rem(at + 1, 4)
        self.up, self.down = {axis: self.after}, {axis: self.before}
        self.ups = [net.copy(view(at, p), view(at, p), self.up) for p in pieces]
        self.downs = [net.copy(view(at, p), view(at, p), self.down) for p in pieces[::-1]]
        self.forwards = []

    def start(self):
        for pair in zip(self.ups, self.downs):
            for copy in pair:
                copy.start()

    def forward(self):
        self.ups[0].wait_recv()
        here = self.view(self.before, 0)
        self.forwards.append(self.net.copy(here, here, self.up))
        self.forwards[-1].start()
        self.downs[0].wait_recv()
        here = self.view(self.after, 1)
        self.forwards.append(self.net.copy(here, here, self.down))
        self.forwards[-1].start()

    def neighbours(self):
        for copy in self.ups[1:] + self.downs[1:]:
            copy.wait_recv()

    def finish(self):
        for copy in self.forwards:
            copy.wait_recv()
        for copy in self.ups + self.downs + self.forwards:
            copy.wait_send()


def layer_kernel(
    residual, sh_in, lh_in, ks_in, qs_in, sg_in, lg_in, gate_in, up_in, down_in, so_in, lo_in,
    small_steps, large_steps, mixer_gain, ffn_in_gain, ffn_out_gain, sgain, lgain, stap, ltap, ktap, qtap, sdec, ldec,
    out,
    xs, xl, kc, qc, sg, lg,
    dtt, ct, ccol, dcol, hloc, eoff, inside,
    halo, mine, mine_tot, sbuf, sib, sib_tot, ysend, ytot_send, yrec, ytot, zsend, ztot_send, zrec, ztot, esend, ebuf,
    chans, weights, projs, res, mix, mixed, rows_in, hidden, parts_out, relay, relay_sum, from_left, from_right,
    params, send_sems, recv_sems, load_sems,
):
    z = lax.axis_index("sp_0")
    y = lax.axis_index("sp_1")
    c = lax.axis_index("sp_2")
    x = lax.axis_index("tp")
    sp = (z * 4 + y) * 2 + c
    nxt = lax.rem(sp + 1, 32)
    prv = lax.rem(sp + 31, 32)
    left, right, across = lax.rem(x + 3, 4), lax.rem(x + 1, 4), lax.rem(x + 2, 4)
    net = Net(send_sems, recv_sems)

    def at_sp(i):
        return {"sp_0": i // 8, "sp_1": lax.rem(i // 2, 4), "sp_2": lax.rem(i, 2)}

    loads = [
        pltpu.make_async_copy(src, dst, load_sems.at[i])
        for i, (src, dst) in enumerate((
            (sh_in, xs), (lh_in, xl), (ks_in, kc), (qs_in, qc),
            (gate_in, weights.at[z, y, c, :, pl.ds(0, FF_DEV)]),
            (up_in, weights.at[z, y, c, :, pl.ds(FF_DEV, FF_DEV)]),
            (down_in, weights.at[z, y, c, :, DOWN_COLS]),
            (so_in, projs.at[x, pl.ds(0, 256)]),
            (lo_in, projs.at[x, pl.ds(256, 256)]),
            (sg_in, sg), (lg_in, lg),
            (residual, res),
        ))
    ]
    for copy in loads:
        copy.start()
    loads_in, loads_own, loads_gate = loads[:4], loads[4:9], loads[9:]

    ypeers = [{"sp_1": lax.rem(y + d, 4)} for d in (1, 2, 3)]
    zpeers = [{"sp_0": lax.rem(z + d, 4)} for d in (1, 2, 3)]
    xpeers = [{"tp": i} for i in (across, right, left)]
    sibling = {"sp_2": 1 - c}
    barrier = pltpu.get_barrier_semaphore()
    peers = [at_sp(nxt), at_sp(prv), sibling] + ypeers + zpeers + xpeers
    for peer in peers:
        pl.semaphore_signal(barrier, inc=1, device_id=peer, device_id_type=MESH)
    pl.semaphore_wait(barrier, len(peers))

    halo_copies = [
        net.copy(src.at[pl.ds(ROWS - 16, 16)], halo.at[i], at_sp(nxt)) for i, src in enumerate((sh_in, lh_in, ks_in, qs_in))
    ]
    for copy in halo_copies:
        copy.start()

    def span(part, size):
        return pl.ds(0, size) if part is None else pl.ds(part * (size // 2), size // 2)

    def y_first(cols):
        return lambda i, p=None: weights.at[z, i, c, span(p, 32), cols]

    def z_first(cols):
        return lambda i, p=None: weights.at[i, y, c, pl.ds(32, 32) if p is None else pl.ds(32 + 16 * p, 16), cols]

    def z_view(cols):
        return lambda i, p=None: weights.at[i, span(p, 4), c, pl.ds(0, 32), cols]

    def y_view(cols):
        return lambda i, p=None: weights.at[span(p, 4), i, c, pl.ds(32, 32), cols]

    def proj_view(i, p=None):
        size = MAIN if p is None else MAIN // 2
        return projs.at[i, pl.ds(pl.multiple_of(c * 256 + (0 if p is None else p * size), 32), size)]

    def slice_view(place, side, i, p=None):
        rows = pl.ds(pl.multiple_of(c * 256 + MAIN + 16 * place, 16), 16)
        return projs.at[i, rows, pl.ds(side * 1024, 1024) if p is None else pl.ds(side * 1024 + 512 * p, 512)]

    for copy in loads_own:
        copy.wait()
    first_rings = [
        Ring(net, axis, at, view(cols))
        for cols in (UP_COLS, DOWN_COLS)
        for axis, at, view in (("sp_1", y, y_first), ("sp_0", z, z_first))
    ]
    proj = Ring(net, "tp", x, proj_view, (0, 1))
    cross_rings = [
        Ring(net, "tp", x, functools.partial(slice_view, place, side)) for side, place in enumerate((y, z))
    ]
    for ring in first_rings + cross_rings + [proj]:
        ring.start()

    for i, gain in enumerate((mixer_gain, ffn_in_gain, ffn_out_gain)):
        params[i : i + 1, :] = gain[...].astype(F32).reshape(1, 2048)
    for i, gain in enumerate((sgain, lgain)):
        params[7:8, i * 256 : i * 256 + 256] = gain[...].astype(F32).reshape(1, 256)
    for i, tap in enumerate((stap, ltap)):
        params[3:7, i * 256 : i * 256 + 256] = tap[...].astype(F32)
    for i, tap in enumerate((ktap, qtap)):
        for g in (0, 1):
            at = 512 + i * 256 + g * 128
            params[3:7, at : at + 128] = tap[:, g, :].astype(F32)

    dtt[...] = jnp.zeros_like(dtt)
    dtt[0:4, :] = jax.nn.softplus(small_steps[...])
    dtt[4:6, :] = jax.nn.softplus(large_steps[...])
    ct[...] = jnp.zeros_like(ct)
    for h in range(6):
        d = sdec[h] if h < 4 else ldec[h - 4]
        rate = jnp.exp(jnp.full((1, ROWS), d, F32))
        ct[h : h + 1, :] = -dtt[h : h + 1, :] * rate
    tr = lax.broadcasted_iota(jnp.int32, (BLOCK, BLOCK), 0)
    tc = lax.broadcasted_iota(jnp.int32, (BLOCK, BLOCK), 1)
    upper = (tr <= tc).astype(F32)
    low = tc < 64
    low_part = low[:PART]
    causal = tc <= tr

    def sums(b, _):
        rows = block_rows(b)
        cum = dot(ct[:, rows], upper, precision=lax.Precision.HIGHEST)
        ct[:, rows] = cum
        pad = jnp.zeros((BLOCK - 8, BLOCK), F32)
        ccol[rows, :] = jnp.concatenate([cum, pad], axis=0).T
        dcol[rows, :] = jnp.concatenate([dtt[:, rows], pad], axis=0).T
        return 0

    lax.fori_loop(0, NBLK, sums, 0, unroll=True)

    taps = [params[3:7, i * 256 : i * 256 + 256] for i in range(4)]
    keep = jnp.where(sp == 0, 0.0, 1.0)

    def conv_of(ext, tap):
        acc = jnp.zeros((BLOCK, 256), F32)
        for k in range(4):
            shifted = ext if k == 3 else pltpu.roll(ext, 3 - k, 0)
            acc = acc + tap[k : k + 1, :] * shifted[16:, :]
        return silu(acc).astype(BF16)

    def convolve(which):
        refs = (xs, xl, kc, qc)

        def conv_block(i, _):
            b = NBLK - 1 - i
            start = pl.multiple_of(b * BLOCK - 16, 16)
            for k in which:
                refs[k][block_rows(b), :] = conv_of(refs[k][pl.ds(start, BLOCK + 16), :].astype(F32), taps[k])
            return 0

        lax.fori_loop(0, NBLK - 1, conv_block, 0)
        for k in which:
            halo_copies[k].wait()
        for k in which:
            ext = jnp.concatenate([halo[k].astype(F32) * keep, refs[k][0:BLOCK, :].astype(F32)], axis=0)
            refs[k][0:BLOCK, :] = conv_of(ext, taps[k])

    for copy in loads_in:
        copy.wait()
    convolve((0, 1, 2))
    for ring in first_rings + cross_rings:
        ring.forward()

    mine[...] = jnp.zeros_like(mine)
    mine_tot[...] = jnp.zeros_like(mine_tot)

    def states(b, _):
        rows = block_rows(b)
        cb = ccol[rows, :]
        last = cb[BLOCK - 1 : BLOCK, :]
        scale = spread(dcol[rows, :] * jnp.exp(last - cb))
        xsb = xs[rows, :].astype(F32)
        xlb = xl[rows, :].astype(F32)
        us = jnp.concatenate([xsb[:, :128] * scale[0], xsb[:, 128:] * scale[1]], axis=1)
        ul = jnp.concatenate([xlb[:, :128] * scale[2], xlb[:, 128:] * scale[3]], axis=1)
        fresh_s = dot(kc[rows, 0:128], us.astype(BF16), ((0,), (0,)))
        fresh_l = dot(kc[rows, 128:256], ul.astype(BF16), ((0,), (0,)))
        state = mine[...]
        tot = mine_tot[...]
        hloc[b] = state
        eoff[b] = jnp.exp(spread_all(tot))
        step = jnp.broadcast_to(last, (8, 128))
        mine[...] = state * jnp.exp(spread_all(step))[0:1, :] + jnp.concatenate([fresh_s, fresh_l], axis=1)
        mine_tot[...] = tot + step
        return 0

    lax.fori_loop(0, NBLK, states, 0, unroll=2)

    sbuf[...] = mine[...].astype(BF16)
    r1 = [net.copy(sbuf, sib, sibling), net.copy(mine_tot, sib_tot, sibling)]
    for copy in r1:
        copy.start()
    convolve((3,))

    def intra(b, _):
        rows = block_rows(b)
        cb = ccol[rows, :]
        parts = []
        for g, vals in ((0, xs), (1, xl)):
            lanes = slice(g * 128, g * 128 + 128)
            scores = dot(qc[rows, lanes], kc[rows, lanes], ((1,), (1,)))
            found = []
            for h in range(4) if g == 0 else range(4, 6):
                gap = jnp.broadcast_to(cb[:, h : h + 1], (BLOCK, BLOCK)) - ct[h : h + 1, rows]
                decay = jnp.exp(jnp.where(causal, gap, -1e30))
                w = (scores * decay * dtt[h : h + 1, rows]).astype(BF16)
                at = (h // 2 if g == 0 else h - 4) * 128
                found.append(dot(w, vals[rows, at : at + 128]))
            if g == 0:
                parts += [jnp.where(low, found[0], found[1]), jnp.where(low, found[2], found[3])]
            else:
                parts += found
        inside[rows, :] = jnp.concatenate(parts, axis=1)
        return 0

    for copy in r1:
        copy.wait()

    half = pl.ds(pl.multiple_of(c * 64, 64), 64)
    my_half = mine[half, :]
    sib_half = sib[half, :].astype(F32)
    first = c == 0
    t_me = mine_tot[...]
    t_sib = sib_tot[...]
    early = jnp.where(first, my_half, sib_half)
    late = jnp.where(first, sib_half, my_half)
    t_late = jnp.where(first, t_sib, t_me)
    chip = early * jnp.exp(spread_all(t_late))[0:1, :] + late
    chip_tot = t_me + t_sib
    ysend[...] = chip.astype(BF16)
    ytot_send[...] = chip_tot

    def peer_copies(send, tot_send, rec, tot_rec, peers_):
        made = []
        for i, peer in enumerate(peers_):
            made += [net.copy(send, rec.at[i], peer), net.copy(tot_send, tot_rec.at[i], peer)]
        return made

    r2 = peer_copies(ysend, ytot_send, yrec, ytot, ypeers)
    for copy in r2:
        copy.start()
    lax.fori_loop(0, 4, intra, 0)
    for copy in r2:
        copy.wait()

    def before_of(pos, rec, tot_rec):
        e = jnp.zeros((64, 512), F32)
        t = jnp.zeros((8, 128), F32)
        for d in (3, 2, 1):
            valid = d <= pos
            e = jnp.where(valid, e * jnp.exp(spread_all(tot_rec[d - 1]))[0:1, :] + rec[d - 1].astype(F32), e)
            t = jnp.where(valid, t + tot_rec[d - 1], t)
        return e, t

    ey, ty = before_of(y, yrec, ytot)
    plane = ey * jnp.exp(spread_all(chip_tot))[0:1, :] + chip
    plane_tot = ty + chip_tot
    for e in (1, 2, 3):
        valid = y + e <= 3
        plane = jnp.where(valid, plane * jnp.exp(spread_all(ytot[3 - e]))[0:1, :] + yrec[3 - e].astype(F32), plane)
        plane_tot = jnp.where(valid, plane_tot + ytot[3 - e], plane_tot)
    zsend[...] = plane.astype(BF16)
    ztot_send[...] = plane_tot
    r3 = peer_copies(zsend, ztot_send, zrec, ztot, zpeers)
    for copy in r3:
        copy.start()
    for ring in first_rings + cross_rings:
        ring.finish()
    slice_rings = [
        Ring(net, axis, at, lambda j, p=None, i=i, side=side: slice_view(j, side, i, p))
        for i in (left, right, across)
        for side, (axis, at) in enumerate((("sp_1", y), ("sp_0", z)))
    ]
    for ring in slice_rings:
        ring.start()
    second_rings = [
        Ring(net, axis, at, view(cols), (0, 1))
        for cols in (UP_COLS, DOWN_COLS)
        for axis, at, view in (("sp_0", z, z_view), ("sp_1", y, y_view))
    ]
    shared = [[], []]

    def start_weights(k):
        cols = (UP_COLS, DOWN_COLS)[k]
        second_rings[2 * k].start()
        second_rings[2 * k + 1].start()
        shared[k] += [
            net.copy(z_view(cols)(z), z_view(cols)(z), sibling), net.copy(y_view(cols)(y), y_view(cols)(y), sibling)
        ]
        for copy in shared[k]:
            copy.start()

    start_weights(0)
    proj.forward()
    lax.fori_loop(4, NBLK, intra, 0)
    for copy in r3:
        copy.wait()
    for ring in slice_rings:
        ring.forward()
    ez, _ = before_of(z, zrec, ztot)
    entering = ez * jnp.exp(spread_all(ty))[0:1, :] + ey
    esend[...] = entering
    r4 = net.copy(esend, ebuf.at[half], sibling)
    r4.start()
    r4.wait()
    own = esend[...]
    enter_rows = []
    for i in range(2):
        arrived = ebuf[i * 64 : i * 64 + 64, :]
        enter_rows.append(jnp.where(c == i, own, arrived))
    enter = jnp.concatenate(enter_rows, axis=0)
    second = enter * jnp.exp(spread_all(t_sib))[0:1, :] + sib[...].astype(F32)
    mine[...] = jnp.where(first, enter, second)

    for copy in loads_gate:
        copy.wait()

    def share(copies):
        for copy in copies:
            copy.start()
        return copies

    def finish(s, j):
        b = 2 * j + s // 2
        rows = pl.ds(pl.multiple_of(j * OWN + s * PART, PART), PART)
        state = (hloc[b] + eoff[b][0:1, :] * mine[...]).astype(BF16)
        grow = spread(jnp.exp(ccol[rows, :]))
        carried = [dot(qc[rows, g * 128 : g * 128 + 128], state[:, g * 256 : g * 256 + 256]) for g in (0, 1)]
        for i in range(4):
            g, at = i // 2, (i % 2) * 128
            gate_ref = sg if g == 0 else lg
            v = inside[rows, i * 128 : i * 128 + 128] + carried[g][:, at : at + 128] * grow[i]
            v = v * silu(gate_ref[rows, at : at + 128].astype(F32))
            sq = v * v
            if g == 0:
                s0 = jnp.sum(jnp.where(low_part, sq, 0.0), axis=1, keepdims=True)
                s1 = jnp.sum(jnp.where(low_part, 0.0, sq), axis=1, keepdims=True)
                inv = jnp.where(low_part, lax.rsqrt(s0 / 64 + EPS), lax.rsqrt(s1 / 64 + EPS))
            else:
                inv = lax.rsqrt(jnp.sum(sq, axis=1, keepdims=True) / 128 + EPS)
            v = v * inv * params[7:8, i * 128 : i * 128 + 128]
            chans[x, s, pl.ds(pl.multiple_of(j * PART, PART), PART), i * 128 : i * 128 + 128] = v.astype(BF16)
        return 0


    gathers = [
        Ring(net, "tp", x, lambda i, p, s=s: chans.at[i, s, pl.ds(p * 128, 128)], (0, 1)) for s in range(STEPS)
    ]

    def finish_step(s):
        lax.fori_loop(0, 4, lambda j, _: finish(s, j), 0, unroll=True)

    def share_arrived(k, which):
        zr, yr = second_rings[2 * k], second_rings[2 * k + 1]
        cols = (UP_COLS, DOWN_COLS)[k]
        zs = [zr.before, zr.after] if which == 0 else [lax.rem(z + 2, 4)]
        ys = [yr.before, yr.after] if which == 0 else [lax.rem(y + 2, 4)]
        return share(
            [net.copy(z_view(cols)(i), z_view(cols)(i), sibling) for i in zs]
            + [net.copy(y_view(cols)(i), y_view(cols)(i), sibling) for i in ys]
        )

    def forward_weights(k):
        second_rings[2 * k].forward()
        second_rings[2 * k + 1].forward()

    def share_weights(k):
        second_rings[2 * k].neighbours()
        second_rings[2 * k + 1].neighbours()
        shared[k] += share_arrived(k, 0)

    def wait_weights(k):
        second_rings[2 * k].finish()
        second_rings[2 * k + 1].finish()
        for copy in shared[k] + share_arrived(k, 1):
            copy.wait()

    def project(s):
        def tile(n, _):
            cols = pl.ds(pl.multiple_of(n * 256, 256), 256)
            acc = dot(chans[0, s], projs[0, :, cols])
            for i in range(1, 4):
                acc = acc + dot(chans[i, s], projs[i, :, cols])
            mix[:, cols] = acc
            return 0

        lax.fori_loop(0, 8, tile, 0, unroll=True)

        def norms(r, _):
            rows = pl.ds(pl.multiple_of(r * 32, 32), 32)
            v = mix[rows, :]
            v = v * lax.rsqrt(jnp.mean(v * v, axis=1, keepdims=True) + EPS)
            at = (r // 2) * OWN + lax.rem(r, 2) * 32 + s * PART
            v = res[pl.ds(pl.multiple_of(at, 32), 32), :].astype(F32) + v * params[0:1, :]
            mix[rows, :] = v
            v = v * lax.rsqrt(jnp.mean(v * v, axis=1, keepdims=True) + EPS)
            rows_in[rows, :] = (v * params[1:2, :]).astype(BF16)
            return 0

        lax.fori_loop(0, OWN // 32, norms, 0, unroll=4)
        mixed[s * PART : s * PART + PART, :] = mix[pl.ds(pl.multiple_of(x * PART, PART), PART), :]

    def gate_up():
        def tile(n, _):
            g_cols = pl.ds(pl.multiple_of(n * 128, 128), 128)
            u_cols = pl.ds(pl.multiple_of(FF_DEV + n * 128, 128), 128)
            w = jnp.concatenate(
                [weights[:, :, :, :, g_cols].reshape(2048, 128), weights[:, :, :, :, u_cols].reshape(2048, 128)], axis=1
            )
            both = dot(rows_in[...], w)
            hidden[:, g_cols] = (silu(both[:, :128]) * both[:, 128:]).astype(BF16)
            return 0

        lax.fori_loop(0, FF_DEV // 128, tile, 0, unroll=True)

    def down(s):
        def tile(n, _):
            w = weights[n // 2, pl.ds(lax.rem(n, 2) * 2, 2), :, :, DOWN_COLS].reshape(256, FF_DEV)
            part = dot(hidden[...], w, ((1,), (1,))).astype(BF16).reshape(4, PART, 256)
            parts_out[:, s * PART : s * PART + PART, pl.ds(pl.multiple_of(n * 256, 256), 256)] = part
            return 0

        lax.fori_loop(0, 8, tile, 0, unroll=True)

    to_left, to_right = {"tp": left}, {"tp": right}
    relays, sends = [None] * STEPS, [None] * STEPS

    def halves(s):
        return pl.ds(s * PART, PART // 2), pl.ds(s * PART + PART // 2, PART // 2)

    def send_parts(s):
        h0, h1 = halves(s)
        kept = pl.ds(s * (PART // 2), PART // 2)
        relays[s] = share([
            net.copy(parts_out.at[across, h0], relay.at[0, kept], to_right),
            net.copy(parts_out.at[across, h1], relay.at[1, kept], to_left),
        ])
        sends[s] = share([
            net.copy(parts_out.at[left, h0], from_right.at[h0], to_left),
            net.copy(parts_out.at[right, h1], from_left.at[h1], to_right),
        ])

    def send_sums(s):
        h0, h1 = halves(s)
        kept = pl.ds(s * (PART // 2), PART // 2)
        for k, (peer, rows, dst, to) in enumerate(((right, h0, from_left, to_right), (left, h1, from_right, to_left))):
            relays[s][k].wait_recv()
            relay_sum[k, kept] = (parts_out[peer, rows, :].astype(F32) + relay[k, kept].astype(F32)).astype(BF16)
            sends[s] += share([net.copy(relay_sum.at[k, kept], dst.at[rows], to)])

    def last(s):
        for copy in relays[s]:
            copy.wait_send()
        for copy in sends[s]:
            copy.wait()

        def rows_of(r, _):
            rows = pl.ds(pl.multiple_of(s * PART + r * 32, 32), 32)
            v = parts_out[x, rows, :].astype(F32) + from_left[rows, :].astype(F32) + from_right[rows, :].astype(F32)
            v = v * lax.rsqrt(jnp.mean(v * v, axis=1, keepdims=True) + EPS)
            out[rows, :] = (mixed[rows, :] + 0.5 * v * params[2:3, :]).astype(BF16)
            return 0

        lax.fori_loop(0, PART // 32, rows_of, 0)

    finish_step(0)
    gathers[0].start()
    finish_step(1)
    gathers[1].start()
    finish_step(2)
    finish_step(3)
    forward_weights(0)
    start_weights(1)
    proj.neighbours()
    shared_proj = share([net.copy(proj_view(i), proj_view(i), sibling) for i in (left, right)])
    proj.finish()
    shared_proj += share([net.copy(proj_view(across), proj_view(across), sibling)])
    gathers[0].forward()
    gathers[2].start()
    for ring in slice_rings:
        ring.finish()
    for i in (left, right, across):
        here = projs.at[i, pl.ds(pl.multiple_of(c * 256 + MAIN, 32), 256 - MAIN)]
        shared_proj += share([net.copy(here, here, sibling)])
    gathers[1].forward()
    gathers[3].start()
    share_weights(0)
    for copy in shared_proj:
        copy.wait()
    def project_step(s):
        gathers[s].neighbours()
        gathers[s].finish()
        project(s)

    project_step(0)
    gathers[2].forward()
    for s in range(STEPS):
        if s == 0:
            wait_weights(0)
            forward_weights(1)
        elif s > 1:
            project_step(s)
        gate_up()
        if s == 0:
            gathers[3].forward()
            share_weights(1)
            project_step(1)
            wait_weights(1)
        else:
            send_sums(s - 1)
        down(s)
        send_parts(s)
    for s in range(STEPS - 1):
        last(s)
    send_sums(STEPS - 1)
    last(STEPS - 1)


COPIES = 200


def layer(*operands):
    vm = pl.BlockSpec(memory_space=pltpu.VMEM)
    sm = pl.BlockSpec(memory_space=pltpu.SMEM)
    hbm = pl.BlockSpec(memory_space=pl.ANY)
    dma = pltpu.SemaphoreType.DMA
    chan = pltpu.VMEM((ROWS, 256), BF16)
    return pl.pallas_call(
        layer_kernel,
        name="layer",
        out_shape=jax.ShapeDtypeStruct((OWN, 2048), BF16),
        in_specs=[hbm] * 12 + [vm] * 11 + [sm] * 2,
        out_specs=vm,
        scratch_shapes=[chan] * 6 + [
            pltpu.VMEM((8, ROWS), F32), pltpu.VMEM((8, ROWS), F32),
            pltpu.VMEM((ROWS, 128), F32), pltpu.VMEM((ROWS, 128), F32),
            pltpu.VMEM((NBLK, 128, 512), F32), pltpu.VMEM((NBLK, 8, 512), F32),
            pltpu.VMEM((ROWS, 512), F32),
            pltpu.VMEM((4, 16, 256), BF16),
            pltpu.VMEM((128, 512), F32), pltpu.VMEM((8, 128), F32),
            pltpu.VMEM((128, 512), BF16), pltpu.VMEM((128, 512), BF16), pltpu.VMEM((8, 128), F32),
            pltpu.VMEM((64, 512), BF16), pltpu.VMEM((8, 128), F32),
            pltpu.VMEM((3, 64, 512), BF16), pltpu.VMEM((3, 8, 128), F32),
            pltpu.VMEM((64, 512), BF16), pltpu.VMEM((8, 128), F32),
            pltpu.VMEM((3, 64, 512), BF16), pltpu.VMEM((3, 8, 128), F32),
            pltpu.VMEM((64, 512), F32), pltpu.VMEM((128, 512), F32),
            pltpu.VMEM((4, STEPS, OWN, 512), BF16),
            pltpu.VMEM((4, 4, 2, 64, 3 * FF_DEV), BF16), pltpu.VMEM((4, 512, 2048), BF16),
            pltpu.VMEM((ROWS, 2048), BF16), pltpu.VMEM((OWN, 2048), F32), pltpu.VMEM((OWN, 2048), F32),
            pltpu.VMEM((OWN, 2048), BF16), pltpu.VMEM((OWN, FF_DEV), BF16),
            pltpu.VMEM((4, OWN, 2048), BF16),
            pltpu.VMEM((2, 128, 2048), BF16), pltpu.VMEM((2, 128, 2048), BF16),
            pltpu.VMEM((OWN, 2048), BF16), pltpu.VMEM((OWN, 2048), BF16),
            pltpu.VMEM((8, 2048), F32),
            dma((COPIES,)), dma((COPIES,)), dma((12,)),
        ],
        compiler_params=pltpu.CompilerParams(
            collective_id=0, has_side_effects=True, vmem_limit_bytes=67043328
        ),
        cost_estimate=pl.CostEstimate(flops=22_000_000_000, bytes_accessed=30_000_000, transcendentals=0),
    )(*operands)


def local(
    residual, small_heads, large_heads, state_keys, state_queries, small_gate, large_gate,
    small_step, large_step, small_taps, large_taps, key_taps, query_taps, small_decay, large_decay,
    small_gain, large_gain, small_out, large_out, mixer_gain, ffn_in_gain,
    gate_proj, up_proj, down_proj, ffn_out_gain,
):
    return layer(
        residual, small_heads, large_heads, state_keys.reshape(ROWS, 256), state_queries.reshape(ROWS, 256),
        small_gate, large_gate, gate_proj, up_proj, down_proj, small_out, large_out,
        small_step.T, large_step.T, mixer_gain, ffn_in_gain, ffn_out_gain, small_gain, large_gain,
        small_taps, large_taps, key_taps, query_taps, small_decay, large_decay,
    )


def solution(mesh):
    torus = Mesh(mesh.devices.reshape(4, 4, 2, mesh.shape["tp"]), ("sp_0", "sp_1", "sp_2", "tp"))
    in_specs = (
        P(SP, None), P(SP, "tp"), P(SP, "tp"), P(SP, "tp", None), P(SP, "tp", None),
        P(SP, "tp"), P(SP, "tp"), P(SP, "tp"), P(SP, "tp"),
        P(None, "tp"), P(None, "tp"), P(None, "tp", None), P(None, "tp", None),
        P("tp"), P("tp"), P("tp"), P("tp"), P("tp", None), P("tp", None),
        P(), P(), P(SP, "tp"), P(SP, "tp"), P(SP, "tp"), P(),
    )
    return jax.shard_map(local, mesh=torus, in_specs=in_specs, out_specs=P(SP_TP, None), check_vma=False)
```

```python
import functools

import jax
import jax.numpy as jnp
from jax import lax
from jax.experimental import pallas as pl
from jax.experimental.pallas import tpu as pltpu
from jax.sharding import Mesh
from jax.sharding import PartitionSpec as P

BLOCK = 128
ROWS = 1024
NBLK = ROWS // BLOCK
SP = ("sp_0", "sp_1", "sp_2")
SP_TP = ("sp_0", "sp_1", "sp_2", "tp")
EPS = 1e-06
MESH = pl.DeviceIdType.MESH
F32 = jnp.float32
BF16 = jnp.bfloat16


def dot(a, b, contract=((1,), (0,)), precision=None):
    return lax.dot_general(
        a, b, (contract, ((), ())), preferred_element_type=F32, precision=precision
    )


def silu(v):
    return v * jax.nn.sigmoid(v)


def spread(m):
    rows = m.shape[0]
    low = lax.broadcasted_iota(jnp.int32, (rows, 128), 1) < 64
    cols = [jnp.broadcast_to(m[:, h : h + 1], (rows, 128)) for h in range(6)]
    return (
        jnp.where(low, cols[0], cols[1]),
        jnp.where(low, cols[2], cols[3]),
        cols[4],
        cols[5],
    )


def spread_all(m):
    return jnp.concatenate(spread(m), axis=1)


def block_rows(b):
    return pl.ds(pl.multiple_of(b * BLOCK, BLOCK), BLOCK)


OWN = 256
STEPS = 4
PART = OWN // STEPS
MAIN = 192
FF_DEV = 1408
UP_COLS = pl.ds(0, 2 * FF_DEV)
DOWN_COLS = pl.ds(2 * FF_DEV, FF_DEV)


class Net:
    def __init__(self, send_sems, recv_sems):
        self.send_sems, self.recv_sems, self.used = send_sems, recv_sems, 0

    def copy(self, src, dst, peer):
        i = self.used
        self.used += 1
        return pltpu.make_async_remote_copy(
            src_ref=src, dst_ref=dst, send_sem=self.send_sems.at[i], recv_sem=self.recv_sems.at[i],
            device_id=peer, device_id_type=MESH,
        )


class Ring:
    def __init__(self, net, axis, at, view, pieces=(None,)):
        self.net, self.at, self.view = net, at, view
        self.before, self.after = lax.rem(at + 3, 4), lax.rem(at + 1, 4)
        self.up, self.down = {axis: self.after}, {axis: self.before}
        self.ups = [net.copy(view(at, p), view(at, p), self.up) for p in pieces]
        self.downs = [net.copy(view(at, p), view(at, p), self.down) for p in pieces[::-1]]
        self.forwards = []

    def start(self):
        for pair in zip(self.ups, self.downs):
            for copy in pair:
                copy.start()

    def forward(self):
        self.ups[0].wait_recv()
        here = self.view(self.before, 0)
        self.forwards.append(self.net.copy(here, here, self.up))
        self.forwards[-1].start()
        self.downs[0].wait_recv()
        here = self.view(self.after, 1)
        self.forwards.append(self.net.copy(here, here, self.down))
        self.forwards[-1].start()

    def neighbours(self):
        for copy in self.ups[1:] + self.downs[1:]:
            copy.wait_recv()

    def finish(self):
        for copy in self.forwards:
            copy.wait_recv()
        for copy in self.ups + self.downs + self.forwards:
            copy.wait_send()


def layer_kernel(
    residual, sh_in, lh_in, ks_in, qs_in, sg_in, lg_in, gate_in, up_in, down_in, so_in, lo_in,
    small_steps, large_steps, mixer_gain, ffn_in_gain, ffn_out_gain, sgain, lgain, stap, ltap, ktap, qtap, sdec, ldec,
    out,
    xs, xl, kc, qc, sg, lg,
    dtt, ct, ccol, dcol, hloc, eoff, inside,
    halo, mine, mine_tot, sbuf, sib, sib_tot, ysend, ytot_send, yrec, ytot, zsend, ztot_send, zrec, ztot, esend, ebuf,
    chans, weights, projs, res, mix, mixed, rows_in, hidden, parts_out, relay, relay_sum, from_left, from_right,
    params, send_sems, recv_sems, load_sems,
):
    z = lax.axis_index("sp_0")
    y = lax.axis_index("sp_1")
    c = lax.axis_index("sp_2")
    x = lax.axis_index("tp")
    sp = (z * 4 + y) * 2 + c
    nxt = lax.rem(sp + 1, 32)
    prv = lax.rem(sp + 31, 32)
    left, right, across = lax.rem(x + 3, 4), lax.rem(x + 1, 4), lax.rem(x + 2, 4)
    net = Net(send_sems, recv_sems)

    def at_sp(i):
        return {"sp_0": i // 8, "sp_1": lax.rem(i // 2, 4), "sp_2": lax.rem(i, 2)}

    loads = [
        pltpu.make_async_copy(src, dst, load_sems.at[i])
        for i, (src, dst) in enumerate((
            (sh_in, xs), (lh_in, xl), (ks_in, kc), (qs_in, qc),
            (gate_in, weights.at[z, y, c, :, pl.ds(0, FF_DEV)]),
            (up_in, weights.at[z, y, c, :, pl.ds(FF_DEV, FF_DEV)]),
            (down_in, weights.at[z, y, c, :, DOWN_COLS]),
            (so_in, projs.at[x, pl.ds(0, 256)]),
            (lo_in, projs.at[x, pl.ds(256, 256)]),
            (sg_in, sg), (lg_in, lg),
            (residual, res),
        ))
    ]
    for copy in loads:
        copy.start()
    loads_in, loads_own, loads_gate = loads[:4], loads[4:9], loads[9:]

    ypeers = [{"sp_1": lax.rem(y + d, 4)} for d in (1, 2, 3)]
    zpeers = [{"sp_0": lax.rem(z + d, 4)} for d in (1, 2, 3)]
    xpeers = [{"tp": i} for i in (across, right, left)]
    sibling = {"sp_2": 1 - c}
    barrier = pltpu.get_barrier_semaphore()
    peers = [at_sp(nxt), at_sp(prv), sibling] + ypeers + zpeers + xpeers
    for peer in peers:
        pl.semaphore_signal(barrier, inc=1, device_id=peer, device_id_type=MESH)
    pl.semaphore_wait(barrier, len(peers))

    halo_copies = [
        net.copy(src.at[pl.ds(ROWS - 16, 16)], halo.at[i], at_sp(nxt)) for i, src in enumerate((sh_in, lh_in, ks_in, qs_in))
    ]
    for copy in halo_copies:
        copy.start()

    def span(part, size):
        return pl.ds(0, size) if part is None else pl.ds(part * (size // 2), size // 2)

    def y_first(cols):
        return lambda i, p=None: weights.at[z, i, c, span(p, 32), cols]

    def z_first(cols):
        return lambda i, p=None: weights.at[i, y, c, pl.ds(32, 32) if p is None else pl.ds(32 + 16 * p, 16), cols]

    def z_view(cols):
        return lambda i, p=None: weights.at[i, span(p, 4), c, pl.ds(0, 32), cols]

    def y_view(cols):
        return lambda i, p=None: weights.at[span(p, 4), i, c, pl.ds(32, 32), cols]

    def proj_view(i, p=None):
        size = MAIN if p is None else MAIN // 2
        return projs.at[i, pl.ds(pl.multiple_of(c * 256 + (0 if p is None else p * size), 32), size)]

    def slice_view(place, side, i, p=None):
        rows = pl.ds(pl.multiple_of(c * 256 + MAIN + 16 * place, 16), 16)
        return projs.at[i, rows, pl.ds(side * 1024, 1024) if p is None else pl.ds(side * 1024 + 512 * p, 512)]

    for copy in loads_own:
        copy.wait()
    first_rings = [
        Ring(net, axis, at, view(cols))
        for cols in (UP_COLS, DOWN_COLS)
        for axis, at, view in (("sp_1", y, y_first), ("sp_0", z, z_first))
    ]
    proj = Ring(net, "tp", x, proj_view, (0, 1))
    cross_rings = [
        Ring(net, "tp", x, functools.partial(slice_view, place, side)) for side, place in enumerate((y, z))
    ]
    for ring in first_rings + cross_rings + [proj]:
        ring.start()

    for i, gain in enumerate((mixer_gain, ffn_in_gain, ffn_out_gain)):
        params[i : i + 1, :] = gain[...].astype(F32).reshape(1, 2048)
    for i, gain in enumerate((sgain, lgain)):
        params[7:8, i * 256 : i * 256 + 256] = gain[...].astype(F32).reshape(1, 256)
    for i, tap in enumerate((stap, ltap)):
        params[3:7, i * 256 : i * 256 + 256] = tap[...].astype(F32)
    for i, tap in enumerate((ktap, qtap)):
        for g in (0, 1):
            at = 512 + i * 256 + g * 128
            params[3:7, at : at + 128] = tap[:, g, :].astype(F32)

    dtt[...] = jnp.zeros_like(dtt)
    dtt[0:4, :] = jax.nn.softplus(small_steps[...])
    dtt[4:6, :] = jax.nn.softplus(large_steps[...])
    ct[...] = jnp.zeros_like(ct)
    for h in range(6):
        d = sdec[h] if h < 4 else ldec[h - 4]
        rate = jnp.exp(jnp.full((1, ROWS), d, F32))
        ct[h : h + 1, :] = -dtt[h : h + 1, :] * rate
    tr = lax.broadcasted_iota(jnp.int32, (BLOCK, BLOCK), 0)
    tc = lax.broadcasted_iota(jnp.int32, (BLOCK, BLOCK), 1)
    upper = (tr <= tc).astype(F32)
    low = tc < 64
    low_part = low[:PART]
    causal = tc <= tr

    def sums(b, _):
        rows = block_rows(b)
        cum = dot(ct[:, rows], upper, precision=lax.Precision.HIGHEST)
        ct[:, rows] = cum
        pad = jnp.zeros((BLOCK - 8, BLOCK), F32)
        ccol[rows, :] = jnp.concatenate([cum, pad], axis=0).T
        dcol[rows, :] = jnp.concatenate([dtt[:, rows], pad], axis=0).T
        return 0

    lax.fori_loop(0, NBLK, sums, 0, unroll=True)

    taps = [params[3:7, i * 256 : i * 256 + 256] for i in range(4)]
    keep = jnp.where(sp == 0, 0.0, 1.0)

    def conv_of(ext, tap):
        acc = jnp.zeros((BLOCK, 256), F32)
        for k in range(4):
            shifted = ext if k == 3 else pltpu.roll(ext, 3 - k, 0)
            acc = acc + tap[k : k + 1, :] * shifted[16:, :]
        return silu(acc).astype(BF16)

    def convolve(which):
        refs = (xs, xl, kc, qc)

        def conv_block(i, _):
            b = NBLK - 1 - i
            start = pl.multiple_of(b * BLOCK - 16, 16)
            for k in which:
                refs[k][block_rows(b), :] = conv_of(refs[k][pl.ds(start, BLOCK + 16), :].astype(F32), taps[k])
            return 0

        lax.fori_loop(0, NBLK - 1, conv_block, 0)
        for k in which:
            halo_copies[k].wait()
        for k in which:
            ext = jnp.concatenate([halo[k].astype(F32) * keep, refs[k][0:BLOCK, :].astype(F32)], axis=0)
            refs[k][0:BLOCK, :] = conv_of(ext, taps[k])

    for copy in loads_in:
        copy.wait()
    convolve((0, 1, 2))
    for ring in first_rings + cross_rings:
        ring.forward()

    mine[...] = jnp.zeros_like(mine)
    mine_tot[...] = jnp.zeros_like(mine_tot)

    def states(b, _):
        rows = block_rows(b)
        cb = ccol[rows, :]
        last = cb[BLOCK - 1 : BLOCK, :]
        scale = spread(dcol[rows, :] * jnp.exp(last - cb))
        xsb = xs[rows, :].astype(F32)
        xlb = xl[rows, :].astype(F32)
        us = jnp.concatenate([xsb[:, :128] * scale[0], xsb[:, 128:] * scale[1]], axis=1)
        ul = jnp.concatenate([xlb[:, :128] * scale[2], xlb[:, 128:] * scale[3]], axis=1)
        fresh_s = dot(kc[rows, 0:128], us.astype(BF16), ((0,), (0,)))
        fresh_l = dot(kc[rows, 128:256], ul.astype(BF16), ((0,), (0,)))
        state = mine[...]
        tot = mine_tot[...]
        hloc[b] = state
        eoff[b] = jnp.exp(spread_all(tot))
        step = jnp.broadcast_to(last, (8, 128))
        mine[...] = state * jnp.exp(spread_all(step))[0:1, :] + jnp.concatenate([fresh_s, fresh_l], axis=1)
        mine_tot[...] = tot + step
        return 0

    lax.fori_loop(0, NBLK, states, 0, unroll=2)

    sbuf[...] = mine[...].astype(BF16)
    r1 = [net.copy(sbuf, sib, sibling), net.copy(mine_tot, sib_tot, sibling)]
    for copy in r1:
        copy.start()
    convolve((3,))

    def intra(b, _):
        rows = block_rows(b)
        cb = ccol[rows, :]
        parts = []
        for g, vals in ((0, xs), (1, xl)):
            lanes = slice(g * 128, g * 128 + 128)
            scores = dot(qc[rows, lanes], kc[rows, lanes], ((1,), (1,)))
            found = []
            for h in range(4) if g == 0 else range(4, 6):
                gap = jnp.broadcast_to(cb[:, h : h + 1], (BLOCK, BLOCK)) - ct[h : h + 1, rows]
                decay = jnp.exp(jnp.where(causal, gap, -1e30))
                w = (scores * decay * dtt[h : h + 1, rows]).astype(BF16)
                at = (h // 2 if g == 0 else h - 4) * 128
                found.append(dot(w, vals[rows, at : at + 128]))
            if g == 0:
                parts += [jnp.where(low, found[0], found[1]), jnp.where(low, found[2], found[3])]
            else:
                parts += found
        inside[rows, :] = jnp.concatenate(parts, axis=1)
        return 0

    for copy in r1:
        copy.wait()

    half = pl.ds(pl.multiple_of(c * 64, 64), 64)
    my_half = mine[half, :]
    sib_half = sib[half, :].astype(F32)
    first = c == 0
    t_me = mine_tot[...]
    t_sib = sib_tot[...]
    early = jnp.where(first, my_half, sib_half)
    late = jnp.where(first, sib_half, my_half)
    t_late = jnp.where(first, t_sib, t_me)
    chip_tot = t_me + t_sib
    ytot_send[...] = chip_tot
    sides = (slice(0, 256), slice(256, 512))

    def faded(value, tot, k):
        return value * jnp.exp(spread_all(tot))[0:1, sides[k]]

    def to_peers(send, rec, peers_):
        made = [net.copy(send, rec(i), peer) for i, peer in enumerate(peers_)]
        for copy in made:
            copy.start()
        return made

    r2, chip = [], []
    for k in (0, 1):
        chip.append(faded(early[:, sides[k]], t_late, k) + late[:, sides[k]])
        ysend[k] = chip[k].astype(BF16)
        r2.append(to_peers(ysend.at[k], lambda i, k=k: yrec.at[i, k], ypeers))
        if k == 0:
            r2[0] += to_peers(ytot_send, lambda i: ytot.at[i], ypeers)
    lax.fori_loop(0, 4, intra, 0)

    def before_of(pos, rec, tot_rec, k):
        e = jnp.zeros((64, 256), F32)
        for d in (3, 2, 1):
            e = jnp.where(d <= pos, faded(e, tot_rec[d - 1], k) + rec[d - 1, k].astype(F32), e)
        return e

    r3, ey = [], []
    for k in (0, 1):
        for copy in r2[k]:
            copy.wait()
        if k == 0:
            ty = jnp.zeros((8, 128), F32)
            for d in (3, 2, 1):
                ty = jnp.where(d <= y, ty + ytot[d - 1], ty)
            plane_tot = ty + chip_tot
            for e in (1, 2, 3):
                plane_tot = jnp.where(y + e <= 3, plane_tot + ytot[3 - e], plane_tot)
            ztot_send[...] = plane_tot
        ey.append(before_of(y, yrec, ytot, k))
        plane = faded(ey[k], chip_tot, k) + chip[k]
        for e in (1, 2, 3):
            plane = jnp.where(y + e <= 3, faded(plane, ytot[3 - e], k) + yrec[3 - e, k].astype(F32), plane)
        zsend[k] = plane.astype(BF16)
        r3.append(to_peers(zsend.at[k], lambda i, k=k: zrec.at[i, k], zpeers))
        if k == 0:
            r3[0] += to_peers(ztot_send, lambda i: ztot.at[i], zpeers)
    for ring in first_rings + cross_rings:
        ring.finish()
    slice_rings = [
        Ring(net, axis, at, lambda j, p=None, i=i, side=side: slice_view(j, side, i, p))
        for i in (left, right, across)
        for side, (axis, at) in enumerate((("sp_1", y), ("sp_0", z)))
    ]
    for ring in slice_rings:
        ring.start()
    second_rings = [
        Ring(net, axis, at, view(cols), (0, 1))
        for cols in (UP_COLS, DOWN_COLS)
        for axis, at, view in (("sp_0", z, z_view), ("sp_1", y, y_view))
    ]
    shared = [[], []]

    def start_weights(k):
        cols = (UP_COLS, DOWN_COLS)[k]
        second_rings[2 * k].start()
        second_rings[2 * k + 1].start()
        shared[k] += [
            net.copy(z_view(cols)(z), z_view(cols)(z), sibling), net.copy(y_view(cols)(y), y_view(cols)(y), sibling)
        ]
        for copy in shared[k]:
            copy.start()

    start_weights(0)
    proj.forward()
    lax.fori_loop(4, NBLK, intra, 0)
    r4 = []
    for k in (0, 1):
        for copy in r3[k]:
            copy.wait()
        esend[k] = faded(before_of(z, zrec, ztot, k), ty, k) + ey[k]
        r4.append(net.copy(esend.at[k], ebuf.at[k, half], sibling))
        r4[k].start()
    for ring in slice_rings:
        ring.forward()
    for k in (0, 1):
        r4[k].wait()
        own = esend[k]
        enter = jnp.concatenate([jnp.where(c == i, own, ebuf[k, i * 64 : i * 64 + 64, :]) for i in range(2)], axis=0)
        second = faded(enter, t_sib, k) + sib[:, sides[k]].astype(F32)
        mine[:, sides[k]] = jnp.where(first, enter, second)

    for copy in loads_gate:
        copy.wait()

    def share(copies):
        for copy in copies:
            copy.start()
        return copies

    def finish(s, j):
        b = 2 * j + s // 2
        rows = pl.ds(pl.multiple_of(j * OWN + s * PART, PART), PART)
        state = (hloc[b] + eoff[b][0:1, :] * mine[...]).astype(BF16)
        grow = spread(jnp.exp(ccol[rows, :]))
        carried = [dot(qc[rows, g * 128 : g * 128 + 128], state[:, g * 256 : g * 256 + 256]) for g in (0, 1)]
        for i in range(4):
            g, at = i // 2, (i % 2) * 128
            gate_ref = sg if g == 0 else lg
            v = inside[rows, i * 128 : i * 128 + 128] + carried[g][:, at : at + 128] * grow[i]
            v = v * silu(gate_ref[rows, at : at + 128].astype(F32))
            sq = v * v
            if g == 0:
                s0 = jnp.sum(jnp.where(low_part, sq, 0.0), axis=1, keepdims=True)
                s1 = jnp.sum(jnp.where(low_part, 0.0, sq), axis=1, keepdims=True)
                inv = jnp.where(low_part, lax.rsqrt(s0 / 64 + EPS), lax.rsqrt(s1 / 64 + EPS))
            else:
                inv = lax.rsqrt(jnp.sum(sq, axis=1, keepdims=True) / 128 + EPS)
            v = v * inv * params[7:8, i * 128 : i * 128 + 128]
            chans[x, s, pl.ds(pl.multiple_of(j * PART, PART), PART), i * 128 : i * 128 + 128] = v.astype(BF16)
        return 0


    gathers = [
        Ring(net, "tp", x, lambda i, p, s=s: chans.at[i, s, pl.ds(p * 128, 128)], (0, 1)) for s in range(STEPS)
    ]

    def finish_step(s):
        lax.fori_loop(0, 4, lambda j, _: finish(s, j), 0, unroll=True)

    def share_arrived(k, which):
        zr, yr = second_rings[2 * k], second_rings[2 * k + 1]
        cols = (UP_COLS, DOWN_COLS)[k]
        zs = [zr.before, zr.after] if which == 0 else [lax.rem(z + 2, 4)]
        ys = [yr.before, yr.after] if which == 0 else [lax.rem(y + 2, 4)]
        return share(
            [net.copy(z_view(cols)(i), z_view(cols)(i), sibling) for i in zs]
            + [net.copy(y_view(cols)(i), y_view(cols)(i), sibling) for i in ys]
        )

    def forward_weights(k):
        second_rings[2 * k].forward()
        second_rings[2 * k + 1].forward()

    def share_weights(k):
        second_rings[2 * k].neighbours()
        second_rings[2 * k + 1].neighbours()
        shared[k] += share_arrived(k, 0)

    def wait_weights(k):
        second_rings[2 * k].finish()
        second_rings[2 * k + 1].finish()
        for copy in shared[k] + share_arrived(k, 1):
            copy.wait()

    def project(s):
        def tile(n, _):
            cols = pl.ds(pl.multiple_of(n * 256, 256), 256)
            acc = dot(chans[0, s], projs[0, :, cols])
            for i in range(1, 4):
                acc = acc + dot(chans[i, s], projs[i, :, cols])
            mix[:, cols] = acc
            return 0

        lax.fori_loop(0, 8, tile, 0, unroll=True)

        def norms(r, _):
            rows = pl.ds(pl.multiple_of(r * 32, 32), 32)
            v = mix[rows, :]
            v = v * lax.rsqrt(jnp.mean(v * v, axis=1, keepdims=True) + EPS)
            at = (r // 2) * OWN + lax.rem(r, 2) * 32 + s * PART
            v = res[pl.ds(pl.multiple_of(at, 32), 32), :].astype(F32) + v * params[0:1, :]
            mix[rows, :] = v
            v = v * lax.rsqrt(jnp.mean(v * v, axis=1, keepdims=True) + EPS)
            rows_in[rows, :] = (v * params[1:2, :]).astype(BF16)
            return 0

        lax.fori_loop(0, OWN // 32, norms, 0, unroll=4)
        mixed[s * PART : s * PART + PART, :] = mix[pl.ds(pl.multiple_of(x * PART, PART), PART), :]

    def gate_up():
        def tile(n, _):
            g_cols = pl.ds(pl.multiple_of(n * 128, 128), 128)
            u_cols = pl.ds(pl.multiple_of(FF_DEV + n * 128, 128), 128)
            w = jnp.concatenate(
                [weights[:, :, :, :, g_cols].reshape(2048, 128), weights[:, :, :, :, u_cols].reshape(2048, 128)], axis=1
            )
            both = dot(rows_in[...], w)
            hidden[:, g_cols] = (silu(both[:, :128]) * both[:, 128:]).astype(BF16)
            return 0

        lax.fori_loop(0, FF_DEV // 128, tile, 0, unroll=True)

    def down(s, first_tile=0, tiles=8):
        def tile(n, _):
            w = weights[n // 2, pl.ds(lax.rem(n, 2) * 2, 2), :, :, DOWN_COLS].reshape(256, FF_DEV)
            part = dot(hidden[...], w, ((1,), (1,))).astype(BF16).reshape(4, PART, 256)
            parts_out[:, s * PART : s * PART + PART, pl.ds(pl.multiple_of(n * 256, 256), 256)] = part
            return 0

        lax.fori_loop(first_tile, first_tile + tiles, tile, 0, unroll=True)

    to_left, to_right = {"tp": left}, {"tp": right}
    relays, sends = [[] for _ in range(STEPS)], [[] for _ in range(STEPS)]

    def halves(s):
        return pl.ds(s * PART, PART // 2), pl.ds(s * PART + PART // 2, PART // 2)

    def send_parts(s, cols):
        h0, h1 = halves(s)
        kept = pl.ds(s * (PART // 2), PART // 2)
        relays[s] += [(cols, share([
            net.copy(parts_out.at[across, h0, cols], relay.at[0, kept, cols], to_right),
            net.copy(parts_out.at[across, h1, cols], relay.at[1, kept, cols], to_left),
        ]))]
        sends[s] += share([
            net.copy(parts_out.at[left, h0, cols], from_right.at[h0, cols], to_left),
            net.copy(parts_out.at[right, h1, cols], from_left.at[h1, cols], to_right),
        ])

    def send_sums(s):
        h0, h1 = halves(s)
        kept = pl.ds(s * (PART // 2), PART // 2)
        for cols, pair in relays[s]:
            for k, (peer, rows, dst, to) in enumerate(((right, h0, from_left, to_right), (left, h1, from_right, to_left))):
                pair[k].wait_recv()
                total = parts_out[peer, rows, cols].astype(F32) + relay[k, kept, cols].astype(F32)
                relay_sum[k, kept, cols] = total.astype(BF16)
                sends[s] += share([net.copy(relay_sum.at[k, kept, cols], dst.at[rows, cols], to)])

    def last(s):
        for _, pair in relays[s]:
            for copy in pair:
                copy.wait_send()
        for copy in sends[s]:
            copy.wait()

        def rows_of(r, _):
            rows = pl.ds(pl.multiple_of(s * PART + r * 32, 32), 32)
            v = parts_out[x, rows, :].astype(F32) + from_left[rows, :].astype(F32) + from_right[rows, :].astype(F32)
            v = v * lax.rsqrt(jnp.mean(v * v, axis=1, keepdims=True) + EPS)
            out[rows, :] = (mixed[rows, :] + 0.5 * v * params[2:3, :]).astype(BF16)
            return 0

        lax.fori_loop(0, PART // 32, rows_of, 0)

    finish_step(0)
    gathers[0].start()
    finish_step(1)
    gathers[1].start()
    finish_step(2)
    finish_step(3)
    forward_weights(0)
    start_weights(1)
    proj.neighbours()
    shared_proj = share([net.copy(proj_view(i), proj_view(i), sibling) for i in (left, right)])
    proj.finish()
    shared_proj += share([net.copy(proj_view(across), proj_view(across), sibling)])
    gathers[0].forward()
    gathers[2].start()
    for ring in slice_rings:
        ring.finish()
    for i in (left, right, across):
        here = projs.at[i, pl.ds(pl.multiple_of(c * 256 + MAIN, 32), 256 - MAIN)]
        shared_proj += share([net.copy(here, here, sibling)])
    gathers[1].forward()
    gathers[3].start()
    share_weights(0)
    for copy in shared_proj:
        copy.wait()
    def project_step(s):
        gathers[s].neighbours()
        gathers[s].finish()
        project(s)

    project_step(0)
    gathers[2].forward()
    for s in range(STEPS):
        if s == 0:
            wait_weights(0)
            forward_weights(1)
        elif s > 1:
            project_step(s)
        gate_up()
        if s == 0:
            gathers[3].forward()
            share_weights(1)
            project_step(1)
            wait_weights(1)
        else:
            send_sums(s - 1)
        if s + 1 < STEPS:
            down(s)
            send_parts(s, pl.ds(0, 2048))
        else:
            for k in (0, 1):
                down(s, 4 * k, 4)
                send_parts(s, pl.ds(1024 * k, 1024))
    for s in range(STEPS - 1):
        last(s)
    send_sums(STEPS - 1)
    last(STEPS - 1)


COPIES = 200


def layer(*operands):
    vm = pl.BlockSpec(memory_space=pltpu.VMEM)
    sm = pl.BlockSpec(memory_space=pltpu.SMEM)
    hbm = pl.BlockSpec(memory_space=pl.ANY)
    dma = pltpu.SemaphoreType.DMA
    chan = pltpu.VMEM((ROWS, 256), BF16)
    return pl.pallas_call(
        layer_kernel,
        name="layer",
        out_shape=jax.ShapeDtypeStruct((OWN, 2048), BF16),
        in_specs=[hbm] * 12 + [vm] * 11 + [sm] * 2,
        out_specs=vm,
        scratch_shapes=[chan] * 6 + [
            pltpu.VMEM((8, ROWS), F32), pltpu.VMEM((8, ROWS), F32),
            pltpu.VMEM((ROWS, 128), F32), pltpu.VMEM((ROWS, 128), F32),
            pltpu.VMEM((NBLK, 128, 512), F32), pltpu.VMEM((NBLK, 8, 512), F32),
            pltpu.VMEM((ROWS, 512), F32),
            pltpu.VMEM((4, 16, 256), BF16),
            pltpu.VMEM((128, 512), F32), pltpu.VMEM((8, 128), F32),
            pltpu.VMEM((128, 512), BF16), pltpu.VMEM((128, 512), BF16), pltpu.VMEM((8, 128), F32),
            pltpu.VMEM((2, 64, 256), BF16), pltpu.VMEM((8, 128), F32),
            pltpu.VMEM((3, 2, 64, 256), BF16), pltpu.VMEM((3, 8, 128), F32),
            pltpu.VMEM((2, 64, 256), BF16), pltpu.VMEM((8, 128), F32),
            pltpu.VMEM((3, 2, 64, 256), BF16), pltpu.VMEM((3, 8, 128), F32),
            pltpu.VMEM((2, 64, 256), F32), pltpu.VMEM((2, 128, 256), F32),
            pltpu.VMEM((4, STEPS, OWN, 512), BF16),
            pltpu.VMEM((4, 4, 2, 64, 3 * FF_DEV), BF16), pltpu.VMEM((4, 512, 2048), BF16),
            pltpu.VMEM((ROWS, 2048), BF16), pltpu.VMEM((OWN, 2048), F32), pltpu.VMEM((OWN, 2048), F32),
            pltpu.VMEM((OWN, 2048), BF16), pltpu.VMEM((OWN, FF_DEV), BF16),
            pltpu.VMEM((4, OWN, 2048), BF16),
            pltpu.VMEM((2, 128, 2048), BF16), pltpu.VMEM((2, 128, 2048), BF16),
            pltpu.VMEM((OWN, 2048), BF16), pltpu.VMEM((OWN, 2048), BF16),
            pltpu.VMEM((8, 2048), F32),
            dma((COPIES,)), dma((COPIES,)), dma((12,)),
        ],
        compiler_params=pltpu.CompilerParams(
            collective_id=0, has_side_effects=True, vmem_limit_bytes=67043328
        ),
        cost_estimate=pl.CostEstimate(flops=22_000_000_000, bytes_accessed=30_000_000, transcendentals=0),
    )(*operands)


def local(
    residual, small_heads, large_heads, state_keys, state_queries, small_gate, large_gate,
    small_step, large_step, small_taps, large_taps, key_taps, query_taps, small_decay, large_decay,
    small_gain, large_gain, small_out, large_out, mixer_gain, ffn_in_gain,
    gate_proj, up_proj, down_proj, ffn_out_gain,
):
    return layer(
        residual, small_heads, large_heads, state_keys.reshape(ROWS, 256), state_queries.reshape(ROWS, 256),
        small_gate, large_gate, gate_proj, up_proj, down_proj, small_out, large_out,
        small_step.T, large_step.T, mixer_gain, ffn_in_gain, ffn_out_gain, small_gain, large_gain,
        small_taps, large_taps, key_taps, query_taps, small_decay, large_decay,
    )


def solution(mesh):
    torus = Mesh(mesh.devices.reshape(4, 4, 2, mesh.shape["tp"]), ("sp_0", "sp_1", "sp_2", "tp"))
    in_specs = (
        P(SP, None), P(SP, "tp"), P(SP, "tp"), P(SP, "tp", None), P(SP, "tp", None),
        P(SP, "tp"), P(SP, "tp"), P(SP, "tp"), P(SP, "tp"),
        P(None, "tp"), P(None, "tp"), P(None, "tp", None), P(None, "tp", None),
        P("tp"), P("tp"), P("tp"), P("tp"), P("tp", None), P("tp", None),
        P(), P(), P(SP, "tp"), P(SP, "tp"), P(SP, "tp"), P(),
    )
    return jax.shard_map(local, mesh=torus, in_specs=in_specs, out_specs=P(SP_TP, None), check_vma=False)
```

```python
import functools

import jax
import jax.numpy as jnp
from jax import lax
from jax.experimental import pallas as pl
from jax.experimental.pallas import tpu as pltpu
from jax.sharding import Mesh
from jax.sharding import PartitionSpec as P

BLOCK = 128
ROWS = 1024
NBLK = ROWS // BLOCK
SP = ("sp_0", "sp_1", "sp_2")
SP_TP = ("sp_0", "sp_1", "sp_2", "tp")
EPS = 1e-06
MESH = pl.DeviceIdType.MESH
F32 = jnp.float32
BF16 = jnp.bfloat16


def dot(a, b, contract=((1,), (0,)), precision=None):
    return lax.dot_general(
        a, b, (contract, ((), ())), preferred_element_type=F32, precision=precision
    )


def silu(v):
    return v * jax.nn.sigmoid(v)


def spread(m):
    rows = m.shape[0]
    low = lax.broadcasted_iota(jnp.int32, (rows, 128), 1) < 64
    cols = [jnp.broadcast_to(m[:, h : h + 1], (rows, 128)) for h in range(6)]
    return (
        jnp.where(low, cols[0], cols[1]),
        jnp.where(low, cols[2], cols[3]),
        cols[4],
        cols[5],
    )


def spread_all(m):
    return jnp.concatenate(spread(m), axis=1)


def block_rows(b):
    return pl.ds(pl.multiple_of(b * BLOCK, BLOCK), BLOCK)


OWN = 256
STEPS = 4
PART = OWN // STEPS
MAIN = 192
FF_DEV = 1408
UP_COLS = pl.ds(0, 2 * FF_DEV)
DOWN_COLS = pl.ds(2 * FF_DEV, FF_DEV)


class Net:
    def __init__(self, send_sems, recv_sems):
        self.send_sems, self.recv_sems, self.used = send_sems, recv_sems, 0

    def copy(self, src, dst, peer):
        i = self.used
        self.used += 1
        return pltpu.make_async_remote_copy(
            src_ref=src, dst_ref=dst, send_sem=self.send_sems.at[i], recv_sem=self.recv_sems.at[i],
            device_id=peer, device_id_type=MESH,
        )


class Ring:
    def __init__(self, net, axis, at, view, pieces=(None,)):
        self.net, self.at, self.view = net, at, view
        self.before, self.after = lax.rem(at + 3, 4), lax.rem(at + 1, 4)
        self.up, self.down = {axis: self.after}, {axis: self.before}
        self.ups = [net.copy(view(at, p), view(at, p), self.up) for p in pieces]
        self.downs = [net.copy(view(at, p), view(at, p), self.down) for p in pieces[::-1]]
        self.forwards = []

    def start(self):
        for pair in zip(self.ups, self.downs):
            for copy in pair:
                copy.start()

    def forward(self):
        self.ups[0].wait_recv()
        here = self.view(self.before, 0)
        self.forwards.append(self.net.copy(here, here, self.up))
        self.forwards[-1].start()
        self.downs[0].wait_recv()
        here = self.view(self.after, 1)
        self.forwards.append(self.net.copy(here, here, self.down))
        self.forwards[-1].start()

    def neighbours(self):
        for copy in self.ups[1:] + self.downs[1:]:
            copy.wait_recv()

    def finish(self):
        for copy in self.forwards:
            copy.wait_recv()
        for copy in self.ups + self.downs + self.forwards:
            copy.wait_send()


def layer_kernel(
    residual, sh_in, lh_in, ks_in, qs_in, sg_in, lg_in, gate_in, up_in, down_in, so_in, lo_in,
    small_steps, large_steps, mixer_gain, ffn_in_gain, ffn_out_gain, sgain, lgain, stap, ltap, ktap, qtap, sdec, ldec,
    out,
    xs, xl, kc, qc, sg, lg,
    dtt, ct, ccol, dcol, hloc, eoff, inside,
    halo, mine, mine_tot, sbuf, sib, sib_tot, ysend, ytot_send, yrec, ytot, zsend, ztot_send, zrec, ztot, esend, ebuf,
    chans, weights, projs, res, mix, mixed, rows_in, hidden, parts_out, relay, relay_sum, from_left, from_right,
    params, send_sems, recv_sems, load_sems,
):
    z = lax.axis_index("sp_0")
    y = lax.axis_index("sp_1")
    c = lax.axis_index("sp_2")
    x = lax.axis_index("tp")
    sp = (z * 4 + y) * 2 + c
    nxt = lax.rem(sp + 1, 32)
    prv = lax.rem(sp + 31, 32)
    left, right, across = lax.rem(x + 3, 4), lax.rem(x + 1, 4), lax.rem(x + 2, 4)
    net = Net(send_sems, recv_sems)

    def at_sp(i):
        return {"sp_0": i // 8, "sp_1": lax.rem(i // 2, 4), "sp_2": lax.rem(i, 2)}

    loads = [
        pltpu.make_async_copy(src, dst, load_sems.at[i])
        for i, (src, dst) in enumerate((
            (sh_in, xs), (lh_in, xl), (ks_in, kc), (qs_in, qc),
            (gate_in, weights.at[z, y, c, :, pl.ds(0, FF_DEV)]),
            (up_in, weights.at[z, y, c, :, pl.ds(FF_DEV, FF_DEV)]),
            (down_in, weights.at[z, y, c, :, DOWN_COLS]),
            (so_in, projs.at[x, pl.ds(0, 256)]),
            (lo_in, projs.at[x, pl.ds(256, 256)]),
            (sg_in, sg), (lg_in, lg),
            (residual, res),
        ))
    ]
    for copy in loads:
        copy.start()
    loads_in, loads_own, loads_gate = loads[:4], loads[4:9], loads[9:]

    ypeers = [{"sp_1": lax.rem(y + d, 4)} for d in (1, 2, 3)]
    zpeers = [{"sp_0": lax.rem(z + d, 4)} for d in (1, 2, 3)]
    xpeers = [{"tp": i} for i in (across, right, left)]
    sibling = {"sp_2": 1 - c}
    barrier = pltpu.get_barrier_semaphore()
    peers = [at_sp(nxt), at_sp(prv), sibling] + ypeers + zpeers + xpeers
    for peer in peers:
        pl.semaphore_signal(barrier, inc=1, device_id=peer, device_id_type=MESH)
    pl.semaphore_wait(barrier, len(peers))

    halo_copies = [
        net.copy(src.at[pl.ds(ROWS - 16, 16)], halo.at[i], at_sp(nxt)) for i, src in enumerate((sh_in, lh_in, ks_in, qs_in))
    ]
    for copy in halo_copies:
        copy.start()

    def span(part, size):
        return pl.ds(0, size) if part is None else pl.ds(part * (size // 2), size // 2)

    def y_first(cols):
        return lambda i, p=None: weights.at[z, i, c, span(p, 32), cols]

    def z_first(cols):
        return lambda i, p=None: weights.at[i, y, c, pl.ds(32, 32) if p is None else pl.ds(32 + 16 * p, 16), cols]

    def z_view(cols):
        return lambda i, p=None: weights.at[i, span(p, 4), c, pl.ds(0, 32), cols]

    def y_view(cols):
        return lambda i, p=None: weights.at[span(p, 4), i, c, pl.ds(32, 32), cols]

    def proj_view(i, p=None):
        size = MAIN if p is None else MAIN // 2
        return projs.at[i, pl.ds(pl.multiple_of(c * 256 + (0 if p is None else p * size), 32), size)]

    def slice_view(place, side, i, p=None):
        rows = pl.ds(pl.multiple_of(c * 256 + MAIN + 16 * place, 16), 16)
        return projs.at[i, rows, pl.ds(side * 1024, 1024) if p is None else pl.ds(side * 1024 + 512 * p, 512)]

    for copy in loads_own:
        copy.wait()
    first_rings = [
        Ring(net, axis, at, view(cols))
        for cols in (UP_COLS, DOWN_COLS)
        for axis, at, view in (("sp_1", y, y_first), ("sp_0", z, z_first))
    ]
    proj = Ring(net, "tp", x, proj_view, (0, 1))
    cross_rings = [
        Ring(net, "tp", x, functools.partial(slice_view, place, side)) for side, place in enumerate((y, z))
    ]
    for ring in first_rings + cross_rings + [proj]:
        ring.start()

    for i, gain in enumerate((mixer_gain, ffn_in_gain, ffn_out_gain)):
        params[i : i + 1, :] = gain[...].astype(F32).reshape(1, 2048)
    for i, gain in enumerate((sgain, lgain)):
        params[7:8, i * 256 : i * 256 + 256] = gain[...].astype(F32).reshape(1, 256)
    for i, tap in enumerate((stap, ltap)):
        params[3:7, i * 256 : i * 256 + 256] = tap[...].astype(F32)
    for i, tap in enumerate((ktap, qtap)):
        for g in (0, 1):
            at = 512 + i * 256 + g * 128
            params[3:7, at : at + 128] = tap[:, g, :].astype(F32)

    dtt[...] = jnp.zeros_like(dtt)
    dtt[0:4, :] = jax.nn.softplus(small_steps[...])
    dtt[4:6, :] = jax.nn.softplus(large_steps[...])
    ct[...] = jnp.zeros_like(ct)
    for h in range(6):
        d = sdec[h] if h < 4 else ldec[h - 4]
        rate = jnp.exp(jnp.full((1, ROWS), d, F32))
        ct[h : h + 1, :] = -dtt[h : h + 1, :] * rate
    tr = lax.broadcasted_iota(jnp.int32, (BLOCK, BLOCK), 0)
    tc = lax.broadcasted_iota(jnp.int32, (BLOCK, BLOCK), 1)
    upper = (tr <= tc).astype(F32)
    low = tc < 64
    low_part = low[:PART]
    causal = tc <= tr

    def sums(b, _):
        rows = block_rows(b)
        cum = dot(ct[:, rows], upper, precision=lax.Precision.HIGHEST)
        ct[:, rows] = cum
        pad = jnp.zeros((BLOCK - 8, BLOCK), F32)
        ccol[rows, :] = jnp.concatenate([cum, pad], axis=0).T
        dcol[rows, :] = jnp.concatenate([dtt[:, rows], pad], axis=0).T
        return 0

    lax.fori_loop(0, NBLK, sums, 0, unroll=True)

    taps = [params[3:7, i * 256 : i * 256 + 256] for i in range(4)]
    keep = jnp.where(sp == 0, 0.0, 1.0)

    def conv_of(ext, tap):
        acc = jnp.zeros((BLOCK, 256), F32)
        for k in range(4):
            shifted = ext if k == 3 else pltpu.roll(ext, 3 - k, 0)
            acc = acc + tap[k : k + 1, :] * shifted[16:, :]
        return silu(acc).astype(BF16)

    def convolve(which):
        refs = (xs, xl, kc, qc)

        def conv_block(i, _):
            b = NBLK - 1 - i
            start = pl.multiple_of(b * BLOCK - 16, 16)
            for k in which:
                refs[k][block_rows(b), :] = conv_of(refs[k][pl.ds(start, BLOCK + 16), :].astype(F32), taps[k])
            return 0

        lax.fori_loop(0, NBLK - 1, conv_block, 0)
        for k in which:
            halo_copies[k].wait()
        for k in which:
            ext = jnp.concatenate([halo[k].astype(F32) * keep, refs[k][0:BLOCK, :].astype(F32)], axis=0)
            refs[k][0:BLOCK, :] = conv_of(ext, taps[k])

    for copy in loads_in:
        copy.wait()
    convolve((0, 1, 2))
    for ring in first_rings + cross_rings:
        ring.forward()

    mine[...] = jnp.zeros_like(mine)
    mine_tot[...] = jnp.zeros_like(mine_tot)

    def states(b, _):
        rows = block_rows(b)
        cb = ccol[rows, :]
        last = cb[BLOCK - 1 : BLOCK, :]
        scale = spread(dcol[rows, :] * jnp.exp(last - cb))
        xsb = xs[rows, :].astype(F32)
        xlb = xl[rows, :].astype(F32)
        us = jnp.concatenate([xsb[:, :128] * scale[0], xsb[:, 128:] * scale[1]], axis=1)
        ul = jnp.concatenate([xlb[:, :128] * scale[2], xlb[:, 128:] * scale[3]], axis=1)
        fresh_s = dot(kc[rows, 0:128], us.astype(BF16), ((0,), (0,)))
        fresh_l = dot(kc[rows, 128:256], ul.astype(BF16), ((0,), (0,)))
        state = mine[...]
        tot = mine_tot[...]
        hloc[b] = state
        eoff[b] = jnp.exp(spread_all(tot))
        step = jnp.broadcast_to(last, (8, 128))
        mine[...] = state * jnp.exp(spread_all(step))[0:1, :] + jnp.concatenate([fresh_s, fresh_l], axis=1)
        mine_tot[...] = tot + step
        return 0

    lax.fori_loop(0, NBLK, states, 0, unroll=2)

    sbuf[...] = mine[...].astype(BF16)
    r1 = [net.copy(sbuf, sib, sibling), net.copy(mine_tot, sib_tot, sibling)]
    for copy in r1:
        copy.start()
    convolve((3,))

    def intra(b, _):
        rows = block_rows(b)
        cb = ccol[rows, :]
        parts = []
        for g, vals in ((0, xs), (1, xl)):
            lanes = slice(g * 128, g * 128 + 128)
            scores = dot(qc[rows, lanes], kc[rows, lanes], ((1,), (1,)))
            found = []
            for h in range(4) if g == 0 else range(4, 6):
                gap = jnp.broadcast_to(cb[:, h : h + 1], (BLOCK, BLOCK)) - ct[h : h + 1, rows]
                decay = jnp.exp(jnp.where(causal, gap, -1e30))
                w = (scores * decay * dtt[h : h + 1, rows]).astype(BF16)
                at = (h // 2 if g == 0 else h - 4) * 128
                found.append(dot(w, vals[rows, at : at + 128]))
            if g == 0:
                parts += [jnp.where(low, found[0], found[1]), jnp.where(low, found[2], found[3])]
            else:
                parts += found
        inside[rows, :] = jnp.concatenate(parts, axis=1)
        return 0

    for copy in r1:
        copy.wait()

    half = pl.ds(pl.multiple_of(c * 64, 64), 64)
    my_half = mine[half, :]
    sib_half = sib[half, :].astype(F32)
    first = c == 0
    t_me = mine_tot[...]
    t_sib = sib_tot[...]
    early = jnp.where(first, my_half, sib_half)
    late = jnp.where(first, sib_half, my_half)
    t_late = jnp.where(first, t_sib, t_me)
    chip_tot = t_me + t_sib
    ytot_send[...] = chip_tot
    sides = (slice(0, 256), slice(256, 512))

    def faded(value, tot, k):
        return value * jnp.exp(spread_all(tot))[0:1, sides[k]]

    def to_peers(send, rec, peers_):
        made = [net.copy(send, rec(i), peer) for i, peer in enumerate(peers_)]
        for copy in made:
            copy.start()
        return made

    r2, chip = [], []
    for k in (0, 1):
        chip.append(faded(early[:, sides[k]], t_late, k) + late[:, sides[k]])
        ysend[k] = chip[k].astype(BF16)
        r2.append(to_peers(ysend.at[k], lambda i, k=k: yrec.at[i, k], ypeers))
        if k == 0:
            r2[0] += to_peers(ytot_send, lambda i: ytot.at[i], ypeers)
    lax.fori_loop(0, 4, intra, 0)

    def before_of(pos, rec, tot_rec, k):
        e = jnp.zeros((64, 256), F32)
        for d in (3, 2, 1):
            e = jnp.where(d <= pos, faded(e, tot_rec[d - 1], k) + rec[d - 1, k].astype(F32), e)
        return e

    r3, ey = [], []
    for k in (0, 1):
        for copy in r2[k]:
            copy.wait()
        if k == 0:
            ty = jnp.zeros((8, 128), F32)
            for d in (3, 2, 1):
                ty = jnp.where(d <= y, ty + ytot[d - 1], ty)
            plane_tot = ty + chip_tot
            for e in (1, 2, 3):
                plane_tot = jnp.where(y + e <= 3, plane_tot + ytot[3 - e], plane_tot)
            ztot_send[...] = plane_tot
        ey.append(before_of(y, yrec, ytot, k))
        plane = faded(ey[k], chip_tot, k) + chip[k]
        for e in (1, 2, 3):
            plane = jnp.where(y + e <= 3, faded(plane, ytot[3 - e], k) + yrec[3 - e, k].astype(F32), plane)
        zsend[k] = plane.astype(BF16)
        r3.append(to_peers(zsend.at[k], lambda i, k=k: zrec.at[i, k], zpeers))
        if k == 0:
            r3[0] += to_peers(ztot_send, lambda i: ztot.at[i], zpeers)
    for ring in first_rings + cross_rings:
        ring.finish()
    slice_rings = [
        Ring(net, axis, at, lambda j, p=None, i=i, side=side: slice_view(j, side, i, p))
        for i in (left, right, across)
        for side, (axis, at) in enumerate((("sp_1", y), ("sp_0", z)))
    ]
    for ring in slice_rings:
        ring.start()
    second_rings = [
        Ring(net, axis, at, view(cols), (0, 1))
        for cols in (UP_COLS, DOWN_COLS)
        for axis, at, view in (("sp_0", z, z_view), ("sp_1", y, y_view))
    ]
    shared = [[], []]

    def start_weights(k):
        cols = (UP_COLS, DOWN_COLS)[k]
        second_rings[2 * k].start()
        second_rings[2 * k + 1].start()
        shared[k] += [
            net.copy(z_view(cols)(z), z_view(cols)(z), sibling), net.copy(y_view(cols)(y), y_view(cols)(y), sibling)
        ]
        for copy in shared[k]:
            copy.start()

    start_weights(0)
    proj.forward()
    lax.fori_loop(4, NBLK, intra, 0)
    r4 = []
    for k in (0, 1):
        for copy in r3[k]:
            copy.wait()
        esend[k] = faded(before_of(z, zrec, ztot, k), ty, k) + ey[k]
        r4.append(net.copy(esend.at[k], ebuf.at[k, half], sibling))
        r4[k].start()
    for ring in slice_rings:
        ring.forward()
    for k in (0, 1):
        r4[k].wait()
        own = esend[k]
        enter = jnp.concatenate([jnp.where(c == i, own, ebuf[k, i * 64 : i * 64 + 64, :]) for i in range(2)], axis=0)
        second = faded(enter, t_sib, k) + sib[:, sides[k]].astype(F32)
        mine[:, sides[k]] = jnp.where(first, enter, second)

    for copy in loads_gate:
        copy.wait()

    def share(copies):
        for copy in copies:
            copy.start()
        return copies

    def finish(s, j):
        b = 2 * j + s // 2
        rows = pl.ds(pl.multiple_of(j * OWN + s * PART, PART), PART)
        state = (hloc[b] + eoff[b][0:1, :] * mine[...]).astype(BF16)
        grow = spread(jnp.exp(ccol[rows, :]))
        carried = [dot(qc[rows, g * 128 : g * 128 + 128], state[:, g * 256 : g * 256 + 256]) for g in (0, 1)]
        for i in range(4):
            g, at = i // 2, (i % 2) * 128
            gate_ref = sg if g == 0 else lg
            v = inside[rows, i * 128 : i * 128 + 128] + carried[g][:, at : at + 128] * grow[i]
            v = v * silu(gate_ref[rows, at : at + 128].astype(F32))
            sq = v * v
            if g == 0:
                s0 = jnp.sum(jnp.where(low_part, sq, 0.0), axis=1, keepdims=True)
                s1 = jnp.sum(jnp.where(low_part, 0.0, sq), axis=1, keepdims=True)
                inv = jnp.where(low_part, lax.rsqrt(s0 / 64 + EPS), lax.rsqrt(s1 / 64 + EPS))
            else:
                inv = lax.rsqrt(jnp.sum(sq, axis=1, keepdims=True) / 128 + EPS)
            v = v * inv * params[7:8, i * 128 : i * 128 + 128]
            chans[x, s, pl.ds(pl.multiple_of(j * PART, PART), PART), i * 128 : i * 128 + 128] = v.astype(BF16)
        return 0


    gathers = [
        Ring(net, "tp", x, lambda i, p, s=s: chans.at[i, s, pl.ds(p * 128, 128)], (0, 1)) for s in range(STEPS)
    ]

    def finish_step(s):
        lax.fori_loop(0, 4, lambda j, _: finish(s, j), 0, unroll=True)

    def share_arrived(k, which):
        zr, yr = second_rings[2 * k], second_rings[2 * k + 1]
        cols = (UP_COLS, DOWN_COLS)[k]
        zs = [zr.before, zr.after] if which == 0 else [lax.rem(z + 2, 4)]
        ys = [yr.before, yr.after] if which == 0 else [lax.rem(y + 2, 4)]
        return share(
            [net.copy(z_view(cols)(i), z_view(cols)(i), sibling) for i in zs]
            + [net.copy(y_view(cols)(i), y_view(cols)(i), sibling) for i in ys]
        )

    def forward_weights(k):
        second_rings[2 * k].forward()
        second_rings[2 * k + 1].forward()

    def share_weights(k):
        second_rings[2 * k].neighbours()
        second_rings[2 * k + 1].neighbours()
        shared[k] += share_arrived(k, 0)

    def wait_weights(k):
        second_rings[2 * k].finish()
        second_rings[2 * k + 1].finish()
        for copy in shared[k] + share_arrived(k, 1):
            copy.wait()

    def project(s):
        def tile(n, _):
            cols = pl.ds(pl.multiple_of(n * 256, 256), 256)
            acc = dot(chans[0, s], projs[0, :, cols])
            for i in range(1, 4):
                acc = acc + dot(chans[i, s], projs[i, :, cols])
            mix[:, cols] = acc
            return 0

        lax.fori_loop(0, 8, tile, 0, unroll=True)

        def norms(r, _):
            rows = pl.ds(pl.multiple_of(r * 32, 32), 32)
            v = mix[rows, :]
            v = v * lax.rsqrt(jnp.mean(v * v, axis=1, keepdims=True) + EPS)
            at = (r // 2) * OWN + lax.rem(r, 2) * 32 + s * PART
            v = res[pl.ds(pl.multiple_of(at, 32), 32), :].astype(F32) + v * params[0:1, :]
            mix[rows, :] = v
            v = v * lax.rsqrt(jnp.mean(v * v, axis=1, keepdims=True) + EPS)
            rows_in[rows, :] = (v * params[1:2, :]).astype(BF16)
            return 0

        lax.fori_loop(0, OWN // 32, norms, 0, unroll=True)
        mixed[s * PART : s * PART + PART, :] = mix[pl.ds(pl.multiple_of(x * PART, PART), PART), :]

    def gate_up():
        def tile(n, _):
            g_cols = pl.ds(pl.multiple_of(n * 128, 128), 128)
            u_cols = pl.ds(pl.multiple_of(FF_DEV + n * 128, 128), 128)
            w = jnp.concatenate(
                [weights[:, :, :, :, g_cols].reshape(2048, 128), weights[:, :, :, :, u_cols].reshape(2048, 128)], axis=1
            )
            both = dot(rows_in[...], w)
            hidden[:, g_cols] = (silu(both[:, :128]) * both[:, 128:]).astype(BF16)
            return 0

        lax.fori_loop(0, FF_DEV // 128, tile, 0, unroll=True)

    def down(s, first_tile=0, tiles=8):
        def tile(n, _):
            w = weights[n // 2, pl.ds(lax.rem(n, 2) * 2, 2), :, :, DOWN_COLS].reshape(256, FF_DEV)
            part = dot(hidden[...], w, ((1,), (1,))).astype(BF16).reshape(4, PART, 256)
            parts_out[:, s * PART : s * PART + PART, pl.ds(pl.multiple_of(n * 256, 256), 256)] = part
            return 0

        lax.fori_loop(first_tile, first_tile + tiles, tile, 0, unroll=True)

    to_left, to_right = {"tp": left}, {"tp": right}
    relays, sends = [[] for _ in range(STEPS)], [[] for _ in range(STEPS)]

    def halves(s):
        return pl.ds(s * PART, PART // 2), pl.ds(s * PART + PART // 2, PART // 2)

    def send_parts(s, cols):
        h0, h1 = halves(s)
        kept = pl.ds(s * (PART // 2), PART // 2)
        relays[s] += [(cols, share([
            net.copy(parts_out.at[across, h0, cols], relay.at[0, kept, cols], to_right),
            net.copy(parts_out.at[across, h1, cols], relay.at[1, kept, cols], to_left),
        ]))]
        sends[s] += share([
            net.copy(parts_out.at[left, h0, cols], from_right.at[h0, cols], to_left),
            net.copy(parts_out.at[right, h1, cols], from_left.at[h1, cols], to_right),
        ])

    def send_sums(s):
        h0, h1 = halves(s)
        kept = pl.ds(s * (PART // 2), PART // 2)
        for cols, pair in relays[s]:
            for k, (peer, rows, dst, to) in enumerate(((right, h0, from_left, to_right), (left, h1, from_right, to_left))):
                pair[k].wait_recv()
                total = parts_out[peer, rows, cols].astype(F32) + relay[k, kept, cols].astype(F32)
                relay_sum[k, kept, cols] = total.astype(BF16)
                sends[s] += share([net.copy(relay_sum.at[k, kept, cols], dst.at[rows, cols], to)])

    def last(s):
        for _, pair in relays[s]:
            for copy in pair:
                copy.wait_send()
        for copy in sends[s]:
            copy.wait()

        def rows_of(r, _):
            rows = pl.ds(pl.multiple_of(s * PART + r * 32, 32), 32)
            v = parts_out[x, rows, :].astype(F32) + from_left[rows, :].astype(F32) + from_right[rows, :].astype(F32)
            v = v * lax.rsqrt(jnp.mean(v * v, axis=1, keepdims=True) + EPS)
            out[rows, :] = (mixed[rows, :] + 0.5 * v * params[2:3, :]).astype(BF16)
            return 0

        lax.fori_loop(0, PART // 32, rows_of, 0)

    finish_step(0)
    gathers[0].start()
    finish_step(1)
    gathers[1].start()
    finish_step(2)
    finish_step(3)
    forward_weights(0)
    start_weights(1)
    proj.neighbours()
    shared_proj = share([net.copy(proj_view(i), proj_view(i), sibling) for i in (left, right)])
    proj.finish()
    shared_proj += share([net.copy(proj_view(across), proj_view(across), sibling)])
    gathers[0].forward()
    gathers[2].start()
    for ring in slice_rings:
        ring.finish()
    for i in (left, right, across):
        here = projs.at[i, pl.ds(pl.multiple_of(c * 256 + MAIN, 32), 256 - MAIN)]
        shared_proj += share([net.copy(here, here, sibling)])
    gathers[1].forward()
    gathers[3].start()
    share_weights(0)
    for copy in shared_proj:
        copy.wait()
    def project_step(s):
        gathers[s].neighbours()
        gathers[s].finish()
        project(s)

    project_step(0)
    gathers[2].forward()
    for s in range(STEPS):
        if s == 0:
            wait_weights(0)
            forward_weights(1)
        elif s > 1:
            project_step(s)
        gate_up()
        if s == 0:
            gathers[3].forward()
            share_weights(1)
            project_step(1)
            wait_weights(1)
        else:
            send_sums(s - 1)
        if s + 1 < STEPS:
            down(s)
            send_parts(s, pl.ds(0, 2048))
        else:
            for k in (0, 1):
                down(s, 4 * k, 4)
                send_parts(s, pl.ds(1024 * k, 1024))
    for s in range(STEPS - 1):
        last(s)
    send_sums(STEPS - 1)
    last(STEPS - 1)


COPIES = 200


def layer(*operands):
    vm = pl.BlockSpec(memory_space=pltpu.VMEM)
    sm = pl.BlockSpec(memory_space=pltpu.SMEM)
    hbm = pl.BlockSpec(memory_space=pl.ANY)
    dma = pltpu.SemaphoreType.DMA
    chan = pltpu.VMEM((ROWS, 256), BF16)
    return pl.pallas_call(
        layer_kernel,
        name="layer",
        out_shape=jax.ShapeDtypeStruct((OWN, 2048), BF16),
        in_specs=[hbm] * 12 + [vm] * 11 + [sm] * 2,
        out_specs=vm,
        scratch_shapes=[chan] * 6 + [
            pltpu.VMEM((8, ROWS), F32), pltpu.VMEM((8, ROWS), F32),
            pltpu.VMEM((ROWS, 128), F32), pltpu.VMEM((ROWS, 128), F32),
            pltpu.VMEM((NBLK, 128, 512), F32), pltpu.VMEM((NBLK, 8, 512), F32),
            pltpu.VMEM((ROWS, 512), F32),
            pltpu.VMEM((4, 16, 256), BF16),
            pltpu.VMEM((128, 512), F32), pltpu.VMEM((8, 128), F32),
            pltpu.VMEM((128, 512), BF16), pltpu.VMEM((128, 512), BF16), pltpu.VMEM((8, 128), F32),
            pltpu.VMEM((2, 64, 256), BF16), pltpu.VMEM((8, 128), F32),
            pltpu.VMEM((3, 2, 64, 256), BF16), pltpu.VMEM((3, 8, 128), F32),
            pltpu.VMEM((2, 64, 256), BF16), pltpu.VMEM((8, 128), F32),
            pltpu.VMEM((3, 2, 64, 256), BF16), pltpu.VMEM((3, 8, 128), F32),
            pltpu.VMEM((2, 64, 256), F32), pltpu.VMEM((2, 128, 256), F32),
            pltpu.VMEM((4, STEPS, OWN, 512), BF16),
            pltpu.VMEM((4, 4, 2, 64, 3 * FF_DEV), BF16), pltpu.VMEM((4, 512, 2048), BF16),
            pltpu.VMEM((ROWS, 2048), BF16), pltpu.VMEM((OWN, 2048), F32), pltpu.VMEM((OWN, 2048), F32),
            pltpu.VMEM((OWN, 2048), BF16), pltpu.VMEM((OWN, FF_DEV), BF16),
            pltpu.VMEM((4, OWN, 2048), BF16),
            pltpu.VMEM((2, 128, 2048), BF16), pltpu.VMEM((2, 128, 2048), BF16),
            pltpu.VMEM((OWN, 2048), BF16), pltpu.VMEM((OWN, 2048), BF16),
            pltpu.VMEM((8, 2048), F32),
            dma((COPIES,)), dma((COPIES,)), dma((12,)),
        ],
        compiler_params=pltpu.CompilerParams(
            collective_id=0, has_side_effects=True, vmem_limit_bytes=67043328
        ),
        cost_estimate=pl.CostEstimate(flops=22_000_000_000, bytes_accessed=30_000_000, transcendentals=0),
    )(*operands)


def local(
    residual, small_heads, large_heads, state_keys, state_queries, small_gate, large_gate,
    small_step, large_step, small_taps, large_taps, key_taps, query_taps, small_decay, large_decay,
    small_gain, large_gain, small_out, large_out, mixer_gain, ffn_in_gain,
    gate_proj, up_proj, down_proj, ffn_out_gain,
):
    return layer(
        residual, small_heads, large_heads, state_keys.reshape(ROWS, 256), state_queries.reshape(ROWS, 256),
        small_gate, large_gate, gate_proj, up_proj, down_proj, small_out, large_out,
        small_step.T, large_step.T, mixer_gain, ffn_in_gain, ffn_out_gain, small_gain, large_gain,
        small_taps, large_taps, key_taps, query_taps, small_decay, large_decay,
    )


def solution(mesh):
    torus = Mesh(mesh.devices.reshape(4, 4, 2, mesh.shape["tp"]), ("sp_0", "sp_1", "sp_2", "tp"))
    in_specs = (
        P(SP, None), P(SP, "tp"), P(SP, "tp"), P(SP, "tp", None), P(SP, "tp", None),
        P(SP, "tp"), P(SP, "tp"), P(SP, "tp"), P(SP, "tp"),
        P(None, "tp"), P(None, "tp"), P(None, "tp", None), P(None, "tp", None),
        P("tp"), P("tp"), P("tp"), P("tp"), P("tp", None), P("tp", None),
        P(), P(), P(SP, "tp"), P(SP, "tp"), P(SP, "tp"), P(),
    )
    return jax.shard_map(local, mesh=torus, in_specs=in_specs, out_specs=P(SP_TP, None), check_vma=False)
```
